256 devices in a mesh: ep: 32 (over z, x), tp: 8 (over y, core).
Axes of the slice: x: 4, y: 4, z: 8, core: 2. Of those that a mesh axis runs over, the one named last changes fastest.
Arguments:
- tokens: bfloat16 [1536, 2048], P('ep'), may hold values from -6 to 6
- state: float32 [1536, 8, 128, 128], P('ep', 'tp'), may hold values from -4 to 4
- norm_gain: float32 [2048], replicated, may hold values from 0.1 to 1.9
- w_query: bfloat16 [2048, 1024], P('ep', 'tp'), may hold values from -0.125 to 0.125
- w_forget: bfloat16 [2048, 1024], P('ep', 'tp'), may hold values from -0.125 to 0.125
- w_input: bfloat16 [2048, 1024], P('ep', 'tp'), may hold values from -0.125 to 0.125
- w_outgate: bfloat16 [2048, 1024], P('ep', 'tp'), may hold values from -0.125 to 0.125
- lower_bound: float32 [1024], P('tp'), may hold values from 0 to 0.9
- head_gain: float32 [1024], P('tp'), may hold values from 0.1 to 1.9
- w_output: bfloat16 [1024, 2048], P('tp'), may hold values from -0.1875 to 0.1875
- ffn_gain: float32 [2048], replicated, may hold values from 0.1 to 1.9
- route_ids: int32 [1536, 4], P('ep'), may hold values from 0 to 63, all different within a row; in each aligned block of 48 rows (0 to 47, 48 to 95, ...) at most 6 rows name the same one
- route_weight: float32 [1536, 4], P('ep'), may hold values from 0.2 to 1
- expert_gate: bfloat16 [64, 2048, 1024], P('ep', None, 'tp'), may hold values from -0.125 to 0.125
- expert_up: bfloat16 [64, 2048, 1024], P('ep', None, 'tp'), may hold values from -0.125 to 0.125
- expert_down: bfloat16 [64, 1024, 2048], P('ep', 'tp'), may hold values from -0.1875 to 0.1875
- shared_gate: bfloat16 [2048, 1024], P(None, 'tp'), may hold values from -0.125 to 0.125
- shared_up: bfloat16 [2048, 1024], P(None, 'tp'), may hold values from -0.125 to 0.125
- shared_down: bfloat16 [1024, 2048], P('tp'), may hold values from -0.1875 to 0.1875
- dense_gate: bfloat16 [2048, 8192], P('tp', 'ep'), may hold values from -0.125 to 0.125
- dense_up: bfloat16 [2048, 8192], P('tp', 'ep'), may hold values from -0.125 to 0.125
- dense_down: bfloat16 [8192, 2048], P('ep', 'tp'), may hold values from -0.0625 to 0.0625
- dense_mix: float32 [2048], P('tp'), may hold values from -6 to 6
Outputs:
- mixed: bfloat16 [1536, 2048], P('ep', 'tp')
- new_state: float32 [1536, 8, 128, 128], P('ep', 'tp')
The draws below stay inside these ranges and needn't reach their ends.
Inputs may be any that keep to these rules, and one draw needn't show every extreme that they name: `route_ids`: each row names 4 different experts. Among the rows of one device no expert is named more than 6 times, and in every draw some expert is named exactly 6 times by some device's rows.
All inputs are finite; a program needn't handle non-finite values.
Results may differ from the reference program's by a relative error of at most 0.025.
Values may be sent and summed in bfloat16 or wider, within the bound.
A program may use at most 64 MiB of HBM per device.

```python
import math
import jax
import jax.numpy as jnp
import numpy as np
from jax import lax

WIDTH = 2048
HEADS = 8
HEAD_DIM = 128
MIX_WIDTH = 1024
EXPERTS = 64
TOPK = 4
EXPERT_FF = 1024
SHARED_FF = 1024
DENSE_FF = 8192
SEQ_DEV = 48
BATCH = 1536
CAP = 6
N_EP = 32
N_TP = 8


def shard_levels(rng, extent, cuts, smallest, largest):
    level = 1.0
    for axis_at, blocks in cuts:
        steps = jax.random.uniform(jax.random.fold_in(jax.random.fold_in(rng, 6), axis_at), (blocks,), jnp.float32, smallest / len(cuts), largest / len(cuts))
        level = level * jnp.repeat(jnp.exp(steps), extent[axis_at] // blocks).reshape((-1,) + (1,) * (len(extent) - 1 - axis_at))
    return level


def assign_block(key, own, number, rows, amount, top, limit, skew):
    order = jax.random.permutation(key, amount)
    crowded, usual = portions_of(amount, rows * top, limit, skew, True), portions_of(amount, rows * top, limit, skew, False)
    places = jnp.arange(amount)

    def named(tallies, turn):
        used = int((tallies > 0).sum())
        fixed = max(1, used // 4)
        moved = fixed + (places - fixed + turn * (used - fixed)) % max(1, amount - fixed)
        return jnp.zeros((amount,), jnp.int32).at[order[jnp.where(places < fixed, places, moved)]].set(jnp.asarray(tallies, jnp.int32))

    tallies = jnp.where(number % 4 == 0, named(crowded, number // 4), named(usual, number - number // 4 - 1))
    mixed = jax.random.permutation(jax.random.fold_in(own, 3), amount)
    giver, taker = mixed[0:amount // 2 * 2:2], mixed[1:amount // 2 * 2:2]
    room = jnp.minimum(tallies[giver] - 1, limit - tallies[taker]) // 2
    room = jnp.where((giver == order[0]) | (taker == order[0]) | (tallies[taker] == 0), 0, jnp.maximum(room, 0))
    moved = jax.random.randint(jax.random.fold_in(own, 4), (amount // 2,), 0, 1 << 20) % (room + 1)
    tallies = tallies.at[giver].add(-moved).at[taker].add(moved)
    members = jnp.searchsorted(jnp.cumsum(tallies), jnp.arange(rows * top), side="right").astype(jnp.int32)
    listing = members.reshape(top, rows).T
    listing = listing[jax.random.permutation(jax.random.fold_in(own, 1), rows)]
    turn = jax.random.randint(jax.random.fold_in(own, 2), (rows, 1), 0, top)
    return jnp.take_along_axis(listing, (jnp.arange(top)[None, :] + turn) % top, axis=1)


def portions_of(count, total, reach, skew, full):
    loads = [(1 << 20) // math.isqrt(rank ** skew) + 1 for rank in range(1, count + 1)]
    largest = reach if full else min(reach, max(-(-total // count), total * loads[0] // sum(loads)))
    least = 1 if total - largest >= count - 1 else 0
    holding, rest = [largest] + [least] * (count - 1), total - largest - least * (count - 1)
    while rest > 0:
        movable = [i for i in range(1, count) if holding[i] < largest] or [i for i in range(1, count) if holding[i] < reach]
        whole, remaining = sum([loads[i] for i in movable]), rest
        for i in movable:
            more = min(reach - holding[i], max(1, remaining * loads[i] // whole), rest)
            holding[i] = holding[i] + more
            rest = rest - more
    return np.array(holding)


def bell_draw(stream_key, shape, deviation, bound, cuts=(), held_as=jnp.bfloat16):
    result = deviation * jax.random.normal(stream_key, shape, jnp.float32)
    if cuts:
        result = result * shard_levels(stream_key, shape, cuts, -0.22, 0.18)
    return jnp.clip(result, -bound, bound).astype(held_as)


def setup_inputs(seed: int = 0) -> dict:
    keys = jax.random.split(jax.random.key(seed), 24)
    tokens = bell_draw(keys[0], (BATCH, WIDTH), 1.0, 6.0, ((0, 32),))
    state = bell_draw(keys[1], (BATCH, HEADS, HEAD_DIM, HEAD_DIM), 0.5, 4.0, ((0, 32), (1, 8)), jnp.float32)
    norm_gain = jnp.clip(1.0 + 0.18 * jax.random.normal(keys[2], (WIDTH,), jnp.float32), 0.1, 1.9)
    w_query = bell_draw(keys[3], (WIDTH, MIX_WIDTH), WIDTH ** -0.5, 0.125, ((0, 32), (1, 8)))
    w_forget = bell_draw(keys[4], (WIDTH, MIX_WIDTH), WIDTH ** -0.5, 0.125, ((0, 32), (1, 8)))
    w_input = bell_draw(keys[5], (WIDTH, MIX_WIDTH), WIDTH ** -0.5, 0.125, ((0, 32), (1, 8)))
    w_outgate = bell_draw(keys[6], (WIDTH, MIX_WIDTH), WIDTH ** -0.5, 0.125, ((0, 32), (1, 8)))
    lower_bound = jnp.clip(0.9 * jax.random.uniform(keys[7], (MIX_WIDTH,), jnp.float32) ** shard_levels(keys[7], (MIX_WIDTH,), ((0, 8),), -0.2, 0.2), 0.0, 0.9)
    head_gain = jnp.clip(1.0 + 0.18 * jax.random.normal(keys[8], (MIX_WIDTH,), jnp.float32), 0.1, 1.9)
    w_output = bell_draw(keys[9], (MIX_WIDTH, WIDTH), MIX_WIDTH ** -0.5, 0.1875, ((0, 8),))
    ffn_gain = jnp.clip(1.0 + 0.18 * jax.random.normal(keys[10], (WIDTH,), jnp.float32), 0.1, 1.9)
    route_ids_keys = jax.random.split(jax.random.fold_in(keys[11], 1), BATCH // SEQ_DEV)
    route_ids_turns = jax.random.permutation(jax.random.fold_in(keys[11], 3), BATCH // SEQ_DEV)
    route_ids = jax.vmap(lambda own, number: assign_block(jax.random.fold_in(keys[11], 2), own, number, SEQ_DEV, EXPERTS, TOPK, CAP, 2))(route_ids_keys, route_ids_turns).reshape((BATCH, TOPK))
    route_weight = jnp.clip(0.2 + 0.8 * jax.random.uniform(keys[12], (BATCH, TOPK), jnp.float32) ** shard_levels(keys[12], (BATCH, TOPK), ((0, 32),), -0.2, 0.2), 0.2, 1.0)
    expert_gate = bell_draw(keys[13], (EXPERTS, WIDTH, EXPERT_FF), WIDTH ** -0.5, 0.125, ((0, 32), (2, 8)))
    expert_up = bell_draw(keys[14], (EXPERTS, WIDTH, EXPERT_FF), WIDTH ** -0.5, 0.125, ((0, 32), (2, 8)))
    expert_down = bell_draw(keys[15], (EXPERTS, EXPERT_FF, WIDTH), EXPERT_FF ** -0.5, 0.1875, ((0, 32), (1, 8)))
    shared_gate = bell_draw(keys[16], (WIDTH, SHARED_FF), WIDTH ** -0.5, 0.125, ((1, 8),))
    shared_up = bell_draw(keys[17], (WIDTH, SHARED_FF), WIDTH ** -0.5, 0.125, ((1, 8),))
    shared_down = bell_draw(keys[18], (SHARED_FF, WIDTH), SHARED_FF ** -0.5, 0.1875, ((0, 8),))
    dense_gate = bell_draw(keys[19], (WIDTH, DENSE_FF), WIDTH ** -0.5, 0.125, ((0, 8), (1, 32)))
    dense_up = bell_draw(keys[20], (WIDTH, DENSE_FF), WIDTH ** -0.5, 0.125, ((0, 8), (1, 32)))
    dense_down = bell_draw(keys[21], (DENSE_FF, WIDTH), DENSE_FF ** -0.5, 0.0625, ((0, 32), (1, 8)))
    dense_mix = bell_draw(keys[22], (WIDTH,), 1.5, 6.0, ((0, 8),), jnp.float32)
    return dict(tokens=tokens, state=state, norm_gain=norm_gain, w_query=w_query, w_forget=w_forget, w_input=w_input, w_outgate=w_outgate, lower_bound=lower_bound, head_gain=head_gain, w_output=w_output, ffn_gain=ffn_gain, route_ids=route_ids, route_weight=route_weight, expert_gate=expert_gate, expert_up=expert_up, expert_down=expert_down, shared_gate=shared_gate, shared_up=shared_up, shared_down=shared_down, dense_gate=dense_gate, dense_up=dense_up, dense_down=dense_down, dense_mix=dense_mix)


EPS = 1e-06

def rms_scale(values, gain):
    values = values.astype(jnp.float32)
    return values * lax.rsqrt(lax.optimization_barrier(jnp.mean(values * values, axis=-1, keepdims=True)) + EPS) * gain

def rounded(values):
    return lax.optimization_barrier(values.astype(jnp.bfloat16)).astype(jnp.float32)

def blocked_sum(left, right, pieces):
    inner = left.shape[1] // pieces
    total = jnp.zeros((left.shape[0], right.shape[1]), jnp.float32)
    for index in range(pieces):
        part = jnp.dot(left[:, index * inner:(index + 1) * inner], right[index * inner:(index + 1) * inner], preferred_element_type=jnp.float32)
        total = total + rounded(part)
    return total

def reference(tokens, state, norm_gain, w_query, w_forget, w_input, w_outgate, lower_bound, head_gain, w_output, ffn_gain, route_ids, route_weight, expert_gate, expert_up, expert_down, shared_gate, shared_up, shared_down, dense_gate, dense_up, dense_down, dense_mix):
    batch = tokens.shape[0]
    normed = rms_scale(tokens, norm_gain).astype(jnp.bfloat16)

    def project(weight):
        return rounded(jnp.dot(normed, weight, preferred_element_type=jnp.float32))
    query, forget_pre, values, out_gate = [project(w) for w in (w_query, w_forget, w_input, w_outgate)]
    forget_sig = jax.nn.sigmoid(forget_pre)
    shape = (batch, HEADS, HEAD_DIM)
    decay = (lower_bound + (1.0 - lower_bound) * forget_sig).reshape(shape)
    keygate = ((1.0 - lower_bound) * (1.0 - forget_sig)).reshape(shape)
    new_state = decay[..., None] * state + keygate[..., None] * values.reshape(shape)[:, :, None, :]
    readout = jnp.einsum('bhk,bhkv->bhv', query.reshape(shape), new_state, precision=lax.Precision.HIGHEST)
    readout = readout * lax.rsqrt(lax.optimization_barrier(jnp.mean(readout * readout, axis=-1, keepdims=True)) + EPS)
    head_out = (readout.reshape(batch, MIX_WIDTH) * head_gain * jax.nn.silu(out_gate)).astype(jnp.bfloat16)
    resid = tokens.astype(jnp.float32) + blocked_sum(head_out, w_output, N_TP)
    moe_in = rms_scale(resid, ffn_gain).astype(jnp.bfloat16)
    flat_ids = route_ids.reshape(N_EP, SEQ_DEV * TOPK)
    onehot = (flat_ids[..., None] == jnp.arange(EXPERTS, dtype=jnp.int32)).astype(jnp.int32)
    slot_rank = lax.optimization_barrier(jnp.sum((jnp.cumsum(onehot, axis=1) - onehot) * onehot, axis=-1))
    device = jnp.arange(N_EP, dtype=jnp.int32)[:, None]
    slot_index = ((flat_ids * N_EP + device) * CAP + slot_rank).reshape(-1).astype(jnp.int32)
    token_index = jnp.repeat(jnp.arange(batch, dtype=jnp.int32), TOPK)
    table = jnp.full((EXPERTS * N_EP * CAP,), batch, jnp.int32).at[slot_index].set(token_index)
    padded = jnp.concatenate([moe_in, jnp.zeros((1, WIDTH), jnp.bfloat16)], axis=0)
    gathered = padded[table].reshape(EXPERTS, N_EP * CAP, WIDTH)

    def one_expert(args):
        rows_in, gate_weight, up_weight, down_weight = args
        gate_pre = jnp.dot(rows_in, gate_weight, preferred_element_type=jnp.float32)
        up_pre = jnp.dot(rows_in, up_weight, preferred_element_type=jnp.float32)
        hidden = (jax.nn.silu(gate_pre) * up_pre).astype(jnp.bfloat16)
        return blocked_sum(hidden, down_weight, N_TP).astype(jnp.bfloat16)
    outputs = lax.map(one_expert, (gathered, expert_gate, expert_up, expert_down)).reshape(-1, WIDTH)
    picked = outputs[slot_index].reshape(batch, TOPK, WIDTH).astype(jnp.float32)
    routed = lax.optimization_barrier(jnp.sum(route_weight[..., None] * picked, axis=1))
    shared_hidden = (jax.nn.silu(jnp.dot(moe_in, shared_gate, preferred_element_type=jnp.float32)) * jnp.dot(moe_in, shared_up, preferred_element_type=jnp.float32)).astype(jnp.bfloat16)
    shared_out = blocked_sum(shared_hidden, shared_down, N_TP)
    dense_pre_gate = blocked_sum(moe_in, dense_gate, N_TP)
    dense_pre_up = blocked_sum(moe_in, dense_up, N_TP)
    dense_hidden = (jax.nn.silu(dense_pre_gate) * dense_pre_up).astype(jnp.bfloat16)
    dense_out = jnp.dot(dense_hidden, dense_down, preferred_element_type=jnp.float32)
    mixed = (resid + routed + shared_out + jax.nn.sigmoid(dense_mix) * dense_out).astype(jnp.bfloat16)
    return (mixed, new_state)
```

```python
import functools

import jax
import jax.numpy as jnp
from jax import lax
from jax.experimental import pallas as pl
from jax.experimental.pallas import tpu as pltpu
from jax.sharding import Mesh
from jax.sharding import PartitionSpec as P

EP = ("z", "x")
TP = ("y", "c")
NZ, NX, NY, NC = 8, 4, 4, 2
NE, NT = NZ * NX, NY * NC
MESH = pl.DeviceIdType.MESH
EPS = 1e-06

Z_ORDER = (1, 7, 2, 6, 3, 5, 4)
Y_ORDER = (1, 3, 2)


def whole(ref, index):
    return ref.at[index]


def lanes(width):
    def view(ref, index):
        start = pl.multiple_of(index * width, width)
        return ref.at[(slice(None),) * (len(ref.shape) - 1) + (pl.ds(start, width),)]

    return view


class Links:
    def __init__(self, send_sem, recv_sem):
        self.send_sem, self.recv_sem = send_sem, recv_sem
        self.sent = self.received = 0
        self.z, self.x = lax.axis_index("z"), lax.axis_index("x")
        self.y, self.c = lax.axis_index("y"), lax.axis_index("c")
        self.e = self.z * NX + self.x
        self.t = self.y * NC + self.c
        self.copies = []

    def reserve(self, number):
        first = self.received
        self.received += number
        return first

    def send(self, src, dst, slot, **device):
        copy = pltpu.make_async_remote_copy(
            src_ref=src,
            dst_ref=dst,
            send_sem=self.send_sem.at[self.sent],
            recv_sem=self.recv_sem.at[slot],
            device_id=device,
            device_id_type=MESH,
        )
        self.sent += 1
        copy.start()
        self.copies.append(copy)

    def wait(self, dst, slot):
        pltpu.make_async_remote_copy(
            src_ref=dst,
            dst_ref=dst,
            send_sem=self.send_sem.at[0],
            recv_sem=self.recv_sem.at[slot],
            device_id={"c": 1 - self.c},
            device_id_type=MESH,
        ).wait_recv()

    def finish(self):
        for copy in self.copies:
            copy.wait_send()


class GatherEp:
    peers = "zx"
    sends, receives = 7 + 3 * 8, 32

    def __init__(self, dst_view=whole):
        self.view = dst_view

    def begin(self, n, src, dst):
        self.base = n.reserve(32)
        mine = self.view(dst, n.e)
        for dz in Z_ORDER:
            n.send(src, mine, self.base + n.e, z=(n.z + dz) % NZ)
        for dx in (1, 3, 2):
            n.send(src, mine, self.base + n.e, x=(n.x + dx) % NX)
        mine[...] = src[...]

    def stages(self, n, src, dst):
        for dz in Z_ORDER:
            e = ((n.z + dz) % NZ) * NX + n.x
            block = self.view(dst, e)
            n.wait(block, self.base + e)
            for dx in (1, 3, 2):
                n.send(block, block, self.base + e, x=(n.x + dx) % NX)
            yield
        for dz in (0,) + Z_ORDER:
            for dx in (1, 3, 2):
                e = ((n.z + dz) % NZ) * NX + (n.x + dx) % NX
                n.wait(self.view(dst, e), self.base + e)


class GatherTp:
    peers = "yc"
    sends, receives = 3 + 1 + 3, 8

    def __init__(self, dst_view=whole):
        self.view = dst_view

    def begin(self, n, src, dst):
        self.base = n.reserve(8)
        mine = self.view(dst, n.t)
        for dy in Y_ORDER:
            n.send(src, mine, self.base + n.t, y=(n.y + dy) % NY)
        n.send(src, mine, self.base + n.t, c=1 - n.c)
        mine[...] = src[...]

    def stages(self, n, src, dst):
        for dy in Y_ORDER:
            t = ((n.y + dy) % NY) * NC + n.c
            block = self.view(dst, t)
            n.wait(block, self.base + t)
            n.send(block, block, self.base + t, c=1 - n.c)
            yield
        for dy in (0,) + Y_ORDER:
            t = ((n.y + dy) % NY) * NC + 1 - n.c
            n.wait(self.view(dst, t), self.base + t)


class SwapTp:
    peers = "yct"
    sends, receives = 7, 8

    def __init__(self, src_view=whole, dst_view=whole):
        self.src_view, self.view = src_view, dst_view

    def begin(self, n, src, dst):
        self.base = n.reserve(8)
        mine = self.view(dst, n.t)
        for dy in Y_ORDER:
            for dc in (0, 1):
                y, c = (n.y + dy) % NY, (n.c + dc) % NC
                n.send(self.src_view(src, y * NC + c), mine, self.base + n.t, y=y, c=c)
        other = n.y * NC + 1 - n.c
        n.send(self.src_view(src, other), mine, self.base + n.t, c=1 - n.c)
        mine[...] = self.src_view(src, n.t)[...]

    def stages(self, n, src, dst):
        yield
        for dy in (0,) + Y_ORDER:
            for dc in (0, 1):
                if dy or dc:
                    t = ((n.y + dy) % NY) * NC + (n.c + dc) % NC
                    n.wait(self.view(dst, t), self.base + t)


class SwapEp:
    peers = "e"
    sends, receives = 31, 32

    def begin(self, n, src, dst):
        self.base = n.reserve(32)
        for dz in (4, 3, 5, 2, 6, 1, 7, 0):
            for dx in (2, 1, 3, 0):
                if dz or dx:
                    z, x = (n.z + dz) % NZ, (n.x + dx) % NX
                    n.send(src.at[z * NX + x], dst.at[n.e], self.base + n.e, z=z, x=x)
        dst.at[n.e][...] = src.at[n.e][...]

    def stages(self, n, src, dst):
        yield
        for dz in range(NZ):
            for dx in range(NX):
                if dz or dx:
                    e = ((n.z + dz) % NZ) * NX + (n.x + dx) % NX
                    n.wait(dst.at[e], self.base + e)


def greet(n, kinds):
    barrier = pltpu.get_barrier_semaphore()
    peers = []
    if "e" in kinds:
        for dz in range(NZ):
            for dx in range(NX):
                if dz or dx:
                    peers.append(dict(z=(n.z + dz) % NZ, x=(n.x + dx) % NX))
    elif "z" in kinds:
        peers += [dict(z=(n.z + dz) % NZ) for dz in range(1, NZ)]
        peers += [dict(x=(n.x + dx) % NX) for dx in range(1, NX)]
    if "t" in kinds:
        for dy in range(1, NY):
            for dc in (0, 1):
                peers.append(dict(y=(n.y + dy) % NY, c=(n.c + dc) % NC))
    elif "y" in kinds:
        peers += [dict(y=(n.y + dy) % NY) for dy in range(1, NY)]
    if "c" in kinds:
        peers.append(dict(c=1 - n.c))
    for peer in peers:
        pl.semaphore_signal(barrier, inc=1, device_id=peer, device_id_type=MESH)
    pl.semaphore_wait(barrier, len(peers))


def mover(plans, *refs):
    count = len(plans)
    srcs, dsts = refs[:count], refs[count : 2 * count]
    n = Links(*refs[2 * count :])
    greet(n, "".join(plan.peers for plan in plans))
    for plan, src, dst in zip(plans, srcs, dsts):
        plan.begin(n, src, dst)
    running = [plan.stages(n, src, dst) for plan, src, dst in zip(plans, srcs, dsts)]
    while running:
        running = [stage for stage in running if next(stage, running) is not running]
    n.finish()


def move(ident, name, *jobs):
    plans = [job[0] for job in jobs]
    arrays = [job[1] for job in jobs]
    shapes = [jax.ShapeDtypeStruct(job[2], job[1].dtype) for job in jobs]
    vmem = pl.BlockSpec(memory_space=pltpu.VMEM)
    return pl.pallas_call(
        functools.partial(mover, plans),
        out_shape=shapes,
        in_specs=[vmem] * len(jobs),
        out_specs=[vmem] * len(jobs),
        scratch_shapes=[
            pltpu.SemaphoreType.DMA((sum(plan.sends for plan in plans),)),
            pltpu.SemaphoreType.DMA((sum(plan.receives for plan in plans),)),
        ],
        compiler_params=pltpu.CompilerParams(collective_id=ident, has_side_effects=True),
        name=name,
    )(*arrays)


def rms_scale(values, gain):
    values = values.astype(jnp.float32)
    return values * lax.rsqrt(jnp.mean(values * values, axis=-1, keepdims=True) + EPS) * gain


def rounded(values):
    return lax.optimization_barrier(values.astype(jnp.bfloat16)).astype(jnp.float32)


def dot(left, right):
    return jnp.dot(left, right, preferred_element_type=jnp.float32)


def local(
    tokens,
    state,
    norm_gain,
    w_query,
    w_forget,
    w_input,
    w_outgate,
    lower_bound,
    head_gain,
    w_output,
    ffn_gain,
    route_ids,
    route_weight,
    expert_gate,
    expert_up,
    expert_down,
    shared_gate,
    shared_up,
    shared_down,
    dense_gate,
    dense_up,
    dense_down,
    dense_mix,
):
    bf16, f32 = jnp.bfloat16, jnp.float32
    seq, width = tokens.shape
    batch = seq * NE
    wide = width // NT
    topk = route_ids.shape[1]
    exp_local = expert_gate.shape[0]
    capacity = max(2, 2 * seq * topk // (exp_local * NE))
    slots = NE * capacity
    e_index = lax.axis_index(EP)
    t_index = lax.axis_index(TP)

    joined = jnp.concatenate((w_query, w_forget, w_input, w_outgate), axis=1)
    dense_joined = jnp.concatenate((dense_gate, dense_up), axis=1)
    routes = jnp.stack([route_ids.astype(f32).T, route_weight.T]).reshape(2 * topk, seq)
    routes = jnp.pad(routes, ((0, 0), (0, 128 - seq)))
    down_blocks = expert_down.reshape(exp_local * expert_down.shape[1], width)
    w_all, routes_all, dense_all, down_all = move(
        0,
        "gather_weights",
        (GatherEp(), joined, (NE, *joined.shape)),
        (GatherEp(), routes, (NE, *routes.shape)),
        (GatherTp(), dense_joined, (NT, *dense_joined.shape)),
        (SwapTp(lanes(wide)), down_blocks, (NT, down_blocks.shape[0], wide)),
    )

    normed = rms_scale(tokens, norm_gain).astype(bf16)
    projected = rounded(dot(normed, w_all.reshape(width, -1)))
    query, forget_pre, values, out_gate = jnp.split(projected, 4, axis=1)
    shape = (seq, 1, query.shape[1])
    forget_sig = jax.nn.sigmoid(forget_pre)
    decay = (lower_bound + (1.0 - lower_bound) * forget_sig).reshape(shape)
    keygate = ((1.0 - lower_bound) * (1.0 - forget_sig)).reshape(shape)
    new_state = decay[..., None] * state + keygate[..., None] * values.reshape(shape)[:, :, None, :]
    readout = jnp.einsum("bhk,bhkv->bhv", query.reshape(shape), new_state)
    readout = readout * lax.rsqrt(jnp.mean(readout * readout, axis=-1, keepdims=True) + EPS)
    head_out = (readout.reshape(seq, -1) * head_gain * jax.nn.silu(out_gate)).astype(bf16)
    head_part = dot(head_out, w_output).astype(bf16)

    (head_parts,) = move(1, "swap_heads", (SwapTp(lanes(wide)), head_part, (NT, seq, wide)))
    own_tokens = lax.dynamic_slice_in_dim(tokens, t_index * wide, wide, 1)
    own_resid = own_tokens.astype(f32) + head_parts.astype(f32).sum(axis=0)
    resid_cols = own_resid.astype(bf16)

    cols_all, resid_rows = move(
        2,
        "gather_resid",
        (GatherEp(), resid_cols, (NE, seq, wide)),
        (GatherTp(lanes(wide)), resid_cols, (seq, width)),
    )
    cols_all = cols_all.reshape(batch, wide)

    ids = routes_all[:, :topk, :seq].astype(jnp.int32)
    weights = routes_all[:, topk:, :seq]
    experts = e_index * exp_local + jnp.arange(exp_local, dtype=jnp.int32)
    named = ids[None] == experts[:, None, None, None]
    token_weight = jnp.sum(jnp.where(named, weights[None], 0.0), axis=2)
    hit = jnp.any(named, axis=2)
    earlier = jnp.triu(jnp.ones((seq, seq), bf16), 1)
    rank = jnp.einsum("jeb,bc->jec", hit.astype(bf16), earlier, preferred_element_type=f32)
    slot = jnp.arange(NE, dtype=jnp.int32)[None, :, None] * capacity + rank.astype(jnp.int32)
    slot = jnp.where(hit, slot, -1).reshape(exp_local, 1, batch)
    pick = (slot == jnp.arange(slots, dtype=jnp.int32)[None, :, None]).astype(bf16)
    chosen = dot(pick.reshape(exp_local * slots, batch), cols_all).astype(bf16)

    dense_rows, chosen_rows = move(
        3,
        "swap_rows",
        (SwapTp(dst_view=lanes(wide)), cols_all.reshape(NT, batch // NT, wide), (batch // NT, width)),
        (GatherTp(lanes(wide)), chosen, (exp_local * slots, width)),
    )

    dense_in = rms_scale(dense_rows, ffn_gain).astype(bf16)
    dense_pre = dot(dense_in, dense_all.reshape(width, -1))
    dense_gate_pre, dense_up_pre = jnp.split(dense_pre, 2, axis=1)
    dense_hidden = (jax.nn.silu(dense_gate_pre) * dense_up_pre).astype(bf16)

    expert_in = rms_scale(chosen_rows, ffn_gain).astype(bf16).reshape(exp_local, slots, width)
    gate_pre = jnp.einsum("jsd,jdf->jsf", expert_in, expert_gate, preferred_element_type=f32)
    up_pre = jnp.einsum("jsd,jdf->jsf", expert_in, expert_up, preferred_element_type=f32)
    hidden = (jax.nn.silu(gate_pre) * up_pre).astype(bf16).reshape(exp_local * slots, -1)

    shared_in = rms_scale(resid_rows, ffn_gain).astype(bf16)
    shared_hidden = (jax.nn.silu(dot(shared_in, shared_gate)) * dot(shared_in, shared_up)).astype(bf16)
    shared_part = dot(shared_hidden, shared_down).astype(bf16)

    dense_hidden_all, hidden_all, shared_parts = move(
        4,
        "gather_hidden",
        (GatherTp(), dense_hidden, (NT, *dense_hidden.shape)),
        (GatherTp(lanes(hidden.shape[1])), hidden, (hidden.shape[0], NT * hidden.shape[1])),
        (SwapTp(lanes(wide)), shared_part, (NT, seq, wide)),
    )
    shared_out = shared_parts.astype(f32).sum(axis=0)
    dense_out = dot(dense_hidden_all.reshape(batch, -1), dense_down) * jax.nn.sigmoid(dense_mix)
    hidden_all = hidden_all.reshape(exp_local, slots, -1)
    down = down_all.reshape(NT, exp_local, -1, wide).transpose(1, 0, 2, 3)
    down = down.reshape(exp_local, -1, wide)
    expert_out = jnp.einsum("jsf,jfd->jsd", hidden_all, down, preferred_element_type=f32)
    expert_out = expert_out.astype(bf16)
    back = jnp.einsum("jsb,jsd->jbd", pick, expert_out, preferred_element_type=f32)
    routed = jnp.sum(back * token_weight.reshape(exp_local, batch, 1), axis=0)
    partial = (dense_out + routed).astype(bf16).reshape(NE, seq, wide)

    (partials,) = move(5, "swap_partials", (SwapEp(), partial, (NE, seq, wide)))
    mixed = own_resid + shared_out + partials.astype(f32).sum(axis=0)
    return mixed.astype(bf16), new_state


def solution(mesh):
    torus = Mesh(mesh.devices.reshape(NZ, NX, NY, NC), ("z", "x", "y", "c"))
    return jax.shard_map(
        local,
        mesh=torus,
        in_specs=(
            P(EP, None),
            P(EP, TP, None, None),
            P(),
            P(EP, TP),
            P(EP, TP),
            P(EP, TP),
            P(EP, TP),
            P(TP),
            P(TP),
            P(TP, None),
            P(),
            P(EP, None),
            P(EP, None),
            P(EP, None, TP),
            P(EP, None, TP),
            P(EP, TP, None),
            P(None, TP),
            P(None, TP),
            P(TP, None),
            P(TP, EP),
            P(TP, EP),
            P(EP, TP),
            P(TP),
        ),
        out_specs=(P(EP, TP), P(EP, TP, None, None)),
        check_vma=False,
    )
```

```python
import jax
import jax.numpy as jnp
from jax import lax
from jax.experimental import pallas as pl
from jax.experimental.pallas import tpu as pltpu
from jax.sharding import Mesh
from jax.sharding import PartitionSpec as P

EP = ("z", "x")
TP = ("y", "c")
NZ, NX, NY, NC = 8, 4, 4, 2
NE, NT = NZ * NX, NY * NC
MESH = pl.DeviceIdType.MESH
EPS = 1e-06
SEQ, WIDTH, HEAD, WIDE, TOPK = 48, 2048, 128, 256, 4
PAIR, CAP, PAD = 2, 6, 16
SLOTS, PADDED = NE * CAP, NE * PAD
ROWS = SEQ * NE // NT
FF = 128

BF, F32 = jnp.bfloat16, jnp.float32
Z_ORDER = (1, 7, 2, 6, 3, 5, 4)
Y_ORDER = (1, 3, 2)
X_ORDER = (1, 3, 2)
SENDS, ARRIVALS, LOCALS = 119, 134, 20


def cols_at(ref, index, width):
    start = pl.multiple_of(index * width, width)
    return ref.at[(slice(None),) * (len(ref.shape) - 1) + (pl.ds(start, width),)]


def dot(left, right):
    return jnp.dot(left, right, preferred_element_type=F32)


def iota(shape, dim):
    return lax.broadcasted_iota(jnp.int32, shape, dim)


def scaled(values, gain):
    values = values.astype(F32)
    return values * lax.rsqrt(jnp.mean(values * values, axis=-1, keepdims=True) + EPS) * gain


class Links:
    def __init__(self, send_sem, recv_sem, local_sem):
        self.send_sem, self.recv_sem, self.local_sem = send_sem, recv_sem, local_sem
        self.sent = self.received = self.locals = 0
        self.z, self.x = lax.axis_index("z"), lax.axis_index("x")
        self.y, self.c = lax.axis_index("y"), lax.axis_index("c")
        self.e = self.z * NX + self.x
        self.t = self.y * NC + self.c
        self.pending = []

    def load(self, src, dst):
        copy = pltpu.make_async_copy(src, dst, self.local_sem.at[self.locals])
        self.locals += 1
        copy.start()
        return copy

    def reserve(self, number):
        first = self.received
        self.received += number
        return first

    def new_send(self):
        self.sent += 1
        return self.sent - 1

    def copy(self, src, dst, sent, slot, **device):
        return pltpu.make_async_remote_copy(
            src_ref=src,
            dst_ref=dst,
            send_sem=self.send_sem.at[sent],
            recv_sem=self.recv_sem.at[slot],
            device_id=device,
            device_id_type=MESH,
        )

    def send(self, src, dst, slot, **device):
        copy = self.copy(src, dst, self.new_send(), slot, **device)
        copy.start()
        self.pending.append(copy)

    def wait(self, dst, slot):
        self.copy(dst, dst, 0, slot, c=1 - self.c).wait_recv()

    def finish(self):
        for copy in self.pending:
            copy.wait_send()
        assert (self.sent, self.received, self.locals) == (SENDS, ARRIVALS, LOCALS)

    def greet(self):
        barrier = pltpu.get_barrier_semaphore()
        peers = []
        for dz in range(NZ):
            for dx in range(NX):
                if dz or dx:
                    peers.append(dict(z=(self.z + dz) % NZ, x=(self.x + dx) % NX))
        for dy in range(NY):
            for dc in range(NC):
                if dy or dc:
                    peers.append(dict(y=(self.y + dy) % NY, c=(self.c + dc) % NC))
        for peer in peers:
            pl.semaphore_signal(barrier, inc=1, device_id=peer, device_id_type=MESH)
        return lambda: pl.semaphore_wait(barrier, len(peers))

    def gather_tp(self, view):
        base = self.reserve(NT)
        mine = view(self.t)
        for dy in Y_ORDER:
            self.send(mine, mine, base + self.t, y=(self.y + dy) % NY)
        self.send(mine, mine, base + self.t, c=1 - self.c)

        def relay():
            for dy in Y_ORDER:
                t = ((self.y + dy) % NY) * NC + self.c
                block = view(t)
                self.wait(block, base + t)
                self.send(block, block, base + t, c=1 - self.c)

        def rest():
            for dy in (0,) + Y_ORDER:
                t = ((self.y + dy) % NY) * NC + 1 - self.c
                self.wait(view(t), base + t)

        return relay, rest

    def swap_tp(self, src_view, dst_view):
        base = self.reserve(NT)
        mine = dst_view(self.t)
        others = []
        for dy in Y_ORDER + (0,):
            for dc in range(NC):
                if dy or dc:
                    others.append(((self.y + dy) % NY, (self.c + dc) % NC))
        for y, c in others:
            self.send(src_view(y * NC + c), mine, base + self.t, y=y, c=c)

        def rest():
            for y, c in others:
                t = y * NC + c
                self.wait(dst_view(t), base + t)

        return rest

    def swap_ep(self, src, dst):
        slot, sent = self.reserve(1), self.new_send()
        for dz in (4, 3, 5, 2, 6, 1, 7, 0):
            for dx in (2, 1, 3, 0):
                if dz or dx:
                    z, x = (self.z + dz) % NZ, (self.x + dx) % NX
                    self.copy(src.at[z * NX + x], dst.at[self.e], sent, slot, z=z, x=x).start()
        self.pending.append(self.copy(src.at[pl.ds(0, NE - 1)], dst.at[pl.ds(0, NE - 1)], sent, slot, c=1 - self.c))
        return lambda: self.wait(dst.at[pl.ds(0, NE - 1)], slot)


def layer(
    tokens,
    state,
    norm_gain,
    w_query,
    w_forget,
    w_input,
    w_outgate,
    lower_bound,
    head_gain,
    w_output,
    ffn_gain,
    route_ids,
    route_weight,
    expert_gate,
    expert_up,
    expert_down,
    shared_gate,
    shared_up,
    shared_down,
    dense_gate,
    dense_up,
    dense_down,
    dense_mix,
    mixed,
    new_state,
    tok,
    wz,
    dense_w,
    down_own,
    down_all,
    held,
    expert_w,
    shared_w,
    shared_d,
    out_w,
    dense_d,
    tok_out,
    tok_in,
    part_out,
    part_in,
    head_part,
    head_in,
    cols,
    resid_rows,
    slot_out,
    slot_in,
    chosen,
    chosen_in,
    dense_rows,
    dense_in,
    dense_hidden,
    hidden,
    shared_part,
    shared_in,
    sum_out,
    sum_in,
    sum2_out,
    sum2_in,
    back_out,
    back_in,
    readout,
    combine,
    dispatch,
    squeeze,
    expand,
    decay_t,
    keygate_t,
    value_f,
    resid,
    send_sem,
    recv_sem,
    local_sem,
):
    n = Links(send_sem, recv_sem, local_sem)
    met = n.greet()
    own_down = cols_at(expert_down, n.t, WIDE)
    load_tok = n.load(tokens, tok)
    load_w = [
        n.load(w, wz.at[n.z, :, pl.ds(i * HEAD, HEAD)])
        for i, w in enumerate((w_query, w_forget, w_input, w_outgate))
    ]
    load_dense = [
        n.load(w, dense_w.at[n.t, :, pl.ds(i * WIDE, WIDE)]) for i, w in enumerate((dense_gate, dense_up))
    ]
    load_down = n.load(expert_down, down_own)
    load_mine = n.load(own_down, down_all.at[:, n.t])
    load_state = n.load(state, held)
    load_out = n.load(w_output, out_w)
    load_shared = [
        n.load(shared_gate, shared_w.at[:, pl.ds(0, FF)]),
        n.load(shared_up, shared_w.at[:, pl.ds(FF, FF)]),
        n.load(shared_down, shared_d),
    ]
    load_expert = [
        n.load(w.at[j], expert_w.at[:, pl.ds((2 * j + i) * FF, FF)])
        for j in range(PAIR)
        for i, w in enumerate((expert_gate, expert_up))
    ]
    load_dense_d = n.load(dense_down, dense_d)

    load_tok.wait()
    normed = scaled(tok[...], norm_gain[...]).astype(BF)
    for x in range(NX):
        for z in range(NZ):
            start = (z * NX + x) * 64
            tok_out[x, :, z * 64 : (z + 1) * 64] = normed[:, start : start + 64]
    tok_in[pl.ds(n.x, 1)] = tok_out[pl.ds(n.x, 1)]

    met()
    for copy in load_w:
        copy.wait()
    base_w = n.reserve(NZ)
    for dz in Z_ORDER:
        n.send(wz.at[n.z], wz.at[n.z], base_w + n.z, z=(n.z + dz) % NZ)
    base_t = n.reserve(NX)
    for dx in X_ORDER:
        x = (n.x + dx) % NX
        n.send(tok_out.at[x], tok_in.at[n.x], base_t + n.x, x=x)
    for copy in load_dense:
        copy.wait()
    dense_relay, dense_rest = n.gather_tp(lambda t: dense_w.at[t])
    load_down.wait()
    down_rest = n.swap_tp(lambda t: cols_at(down_own, t, WIDE), lambda t: down_all.at[:, t])

    lane = iota((SEQ, 128), 1)
    named = [route_ids[:, k : k + 1] for k in range(TOPK)]
    equal = [(lane == ids).astype(F32) for ids in named]
    earlier = (iota((SEQ, SEQ), 1) < iota((SEQ, SEQ), 0)).astype(BF)
    rank = dot(earlier, sum(equal).astype(BF))
    places = []
    for ids, same in zip(named, equal):
        first = (ids // 2) * PAD + (ids % 2) * CAP
        places.append(first.astype(F32) + jnp.sum(same * rank, axis=1, keepdims=True))
    slot_lane = iota((SEQ, PADDED), 1).astype(F32)
    total = jnp.zeros((SEQ, PADDED), F32)
    table = jnp.full((SEQ, 128), -1.0, F32)
    for k, place in enumerate(places):
        total = total + jnp.where(slot_lane == place, route_weight[:, k : k + 1], 0.0)
        table = jnp.where(lane == k, place, table)
    combine[...] = total
    table = table.T
    slot_row = iota((PADDED, SEQ), 0).astype(F32)
    picked = jnp.zeros((PADDED, SEQ), F32)
    for k in range(TOPK):
        picked = picked + (slot_row == table[k : k + 1, :]).astype(F32)
    dispatch[...] = picked.astype(BF)

    def row_of(slot):
        inside = slot % PAD
        second = (inside >= CAP).astype(jnp.int32)
        row = second * SLOTS + (slot // PAD) * CAP + inside - second * CAP
        return jnp.where(inside < PAIR * CAP, row, -1)

    squeeze[...] = (iota((PAIR * SLOTS, PADDED), 0) == row_of(iota((1, PADDED), 1))).astype(F32).astype(BF)
    expand[...] = (iota((PADDED, PAIR * SLOTS), 1) == row_of(iota((PADDED, 1), 0))).astype(F32).astype(BF)

    for dx in X_ORDER:
        x = (n.x + dx) % NX
        n.wait(tok_in.at[x], base_t + x)
    for dz in Z_ORDER:
        z = (n.z + dz) % NZ
        n.wait(wz.at[z], base_w + z)
    part = dot(tok_in[...].reshape(NX * SEQ, 512), wz[...].reshape(512, 512))
    part_out[...] = part.astype(BF).reshape(NX, SEQ, 512)
    base_p = n.reserve(NX)
    for dx in X_ORDER:
        x = (n.x + dx) % NX
        n.send(part_out.at[x], part_in.at[n.x], base_p + n.x, x=x)
    part_in[pl.ds(n.x, 1)] = part_out[pl.ds(n.x, 1)]
    dense_relay()
    for dx in X_ORDER:
        x = (n.x + dx) % NX
        n.wait(part_in.at[x], base_p + x)
    projected = part_in[0].astype(F32)
    for x in range(1, NX):
        projected = projected + part_in[x].astype(F32)
    projected = projected.astype(BF).astype(F32)
    query, forget_pre = projected[:, :HEAD], projected[:, HEAD : 2 * HEAD]
    values, out_gate = projected[:, 2 * HEAD : 3 * HEAD], projected[:, 3 * HEAD :]
    low = lower_bound[...]
    forget_sig = jax.nn.sigmoid(forget_pre)
    decay = low + (1.0 - low) * forget_sig
    keygate = (1.0 - low) * (1.0 - forget_sig)
    mixed_q = (query * decay).T
    decay_t[...] = decay.T
    keygate_t[...] = keygate.T
    value_f[...] = values
    load_state.wait()
    for b in range(SEQ):
        readout[b : b + 1, :] = jnp.sum(mixed_q[:, b : b + 1] * held[b, 0], axis=0, keepdims=True)
    read = readout[...] + jnp.sum(query * keygate, axis=1, keepdims=True) * values
    read = read * lax.rsqrt(jnp.mean(read * read, axis=-1, keepdims=True) + EPS)
    head_out = (read * head_gain[...] * jax.nn.silu(out_gate)).astype(BF)
    load_out.wait()
    head_part[...] = dot(head_out, out_w[...]).astype(BF)
    head_rest = n.swap_tp(lambda t: cols_at(head_part, t, WIDE), lambda t: head_in.at[t])
    head_in[pl.ds(n.t, 1)] = cols_at(head_part, n.t, WIDE)[...][None]
    head_rest()
    own = cols_at(tok, n.t, WIDE)[...].astype(F32)
    for t in range(NT):
        own = own + head_in[t].astype(F32)
    resid[...] = own
    own_cols = own.astype(BF)
    cols[pl.ds(n.e, 1)] = own_cols[None]

    base_c = n.reserve(NE)
    mine = cols.at[n.e]
    for dz in Z_ORDER:
        n.send(mine, mine, base_c + n.e, z=(n.z + dz) % NZ)
    for dx in X_ORDER:
        n.send(mine, mine, base_c + n.e, x=(n.x + dx) % NX)
    cols_at(resid_rows, n.t, WIDE)[...] = own_cols
    rows_relay, rows_rest = n.gather_tp(lambda t: cols_at(resid_rows, t, WIDE))
    slot_out[...] = dot(dispatch[...], own_cols).astype(BF).reshape(NE, PAD, WIDE)
    slots_rest = n.swap_ep(slot_out, slot_in)
    slot_in[pl.ds(n.e, 1)] = slot_out[pl.ds(n.e, 1)]
    for dz in Z_ORDER:
        e = ((n.z + dz) % NZ) * NX + n.x
        n.wait(cols.at[e], base_c + e)
        for dx in X_ORDER:
            n.send(cols.at[e], cols.at[e], base_c + e, x=(n.x + dx) % NX)
    rows_relay()

    slots_rest()
    picked_rows = dot(squeeze[...], slot_in[...].reshape(PADDED, WIDE)).astype(BF)
    cols_at(chosen, n.t, WIDE)[...] = picked_rows
    chosen_relay, chosen_rest = n.gather_tp(lambda t: cols_at(chosen, t, WIDE))

    for b in range(SEQ):
        held[b, 0] = decay_t[:, b : b + 1] * held[b, 0] + keygate_t[:, b : b + 1] * value_f[b : b + 1, :]
    store_state = n.load(held, new_state)

    for dz in (0,) + Z_ORDER:
        for dx in X_ORDER:
            e = ((n.z + dz) % NZ) * NX + (n.x + dx) % NX
            n.wait(cols.at[e], base_c + e)
    per = NE // NT
    dense_swap = n.swap_tp(
        lambda t: cols.at[pl.ds(t * per, per)],
        lambda t: dense_rows.at[:, :, pl.ds(pl.multiple_of(t * WIDE, WIDE), WIDE)],
    )
    dense_rows[:, :, pl.ds(pl.multiple_of(n.t * WIDE, WIDE), WIDE)] = cols[pl.ds(n.t * per, per)]

    rows_rest()
    for copy in load_shared:
        copy.wait()
    shared_x = scaled(resid_rows[...], ffn_gain[...]).astype(BF)
    shared_pre = dot(shared_x, shared_w[...])
    shared_hidden = (jax.nn.silu(shared_pre[:, :FF]) * shared_pre[:, FF:]).astype(BF)
    shared_part[...] = dot(shared_hidden, shared_d[...]).astype(BF)
    shared_rest = n.swap_tp(lambda t: cols_at(shared_part, t, WIDE), lambda t: shared_in.at[t])
    shared_in[pl.ds(n.t, 1)] = cols_at(shared_part, n.t, WIDE)[...][None]

    chosen_relay()
    chosen_rest()
    for copy in load_expert:
        copy.wait()
    gain = ffn_gain[...]
    for j in range(PAIR):
        for i in range(4):
            rows = pl.ds(j * SLOTS + i * SEQ, SEQ)
            chosen_in[rows] = scaled(chosen[rows], gain).astype(BF)
        pre = dot(chosen_in[pl.ds(j * SLOTS, SLOTS)], expert_w[:, 2 * j * FF : 2 * (j + 1) * FF])
        unit = (jax.nn.silu(pre[:, :FF]) * pre[:, FF:]).astype(BF)
        cols_at(hidden, n.t, FF).at[pl.ds(j * SLOTS, SLOTS)][...] = unit
    hidden_relay, hidden_rest = n.gather_tp(lambda t: cols_at(hidden, t, FF))

    dense_rest()
    dense_swap()
    for i in range(per):
        dense_in[pl.ds(i * SEQ, SEQ)] = scaled(dense_rows[i], gain).astype(BF)
    pre = dot(dense_in[...], dense_w[...].reshape(WIDTH, 2 * WIDE))
    dense_hidden[pl.ds(n.t, 1)] = (jax.nn.silu(pre[:, :WIDE]) * pre[:, WIDE:]).astype(BF)[None]
    units_relay, units_rest = n.gather_tp(lambda t: dense_hidden.at[t])

    hidden_relay()
    units_relay()
    down_rest()
    load_mine.wait()
    hidden_rest()
    outs = [
        dot(hidden[pl.ds(j * SLOTS, SLOTS)], down_all[j].reshape(NT * FF, WIDE)).astype(BF) for j in range(PAIR)
    ]
    spread = dot(expand[:, :SLOTS], outs[0]) + dot(expand[:, SLOTS:], outs[1])
    back_out[...] = spread.astype(BF).reshape(NE, PAD, WIDE)
    back_rest = n.swap_ep(back_out, back_in)
    back_in[pl.ds(n.e, 1)] = back_out[pl.ds(n.e, 1)]

    units_rest()
    load_dense_d.wait()
    scale = jax.nn.sigmoid(dense_mix[...])
    for t in range(NT):
        block = dot(dense_hidden[t], dense_d[...]) * scale
        sum_out[t] = block.astype(BF).reshape(NX, SEQ, WIDE)
    base_x = n.reserve(NX)
    for dx in X_ORDER:
        x = (n.x + dx) % NX
        n.send(sum_out.at[:, x], sum_in.at[n.x], base_x + n.x, x=x)
    back_rest()
    shared_rest()
    result = resid[...] + jnp.dot(
        combine[...],
        back_in[...].reshape(PADDED, WIDE).astype(F32),
        preferred_element_type=F32,
        precision=lax.Precision.HIGHEST,
    )
    for t in range(NT):
        result = result + shared_in[t].astype(F32)
    resid[...] = result
    for dx in X_ORDER:
        x = (n.x + dx) % NX
        n.wait(sum_in.at[x], base_x + x)
    for z in range(NZ):
        block = sum_out[z, pl.ds(n.x, 1)][0].astype(F32)
        for dx in X_ORDER:
            block = block + sum_in[pl.ds((n.x + dx) % NX, 1), z][0].astype(F32)
        sum2_out[z] = block.astype(BF)
    base_z = n.reserve(NZ)
    for dz in (4, 3, 5, 2, 6, 1, 7):
        z = (n.z + dz) % NZ
        n.send(sum2_out.at[z], sum2_in.at[n.z], base_z + n.z, z=z)
    sum2_in[pl.ds(n.z, 1)] = sum2_out[pl.ds(n.z, 1)]
    for dz in Z_ORDER:
        z = (n.z + dz) % NZ
        n.wait(sum2_in.at[z], base_z + z)
    result = resid[...]
    for z in range(NZ):
        result = result + sum2_in[z].astype(F32)
    mixed[...] = result.astype(BF)
    store_state.wait()
    n.finish()


def local(*args):
    args = list(args)
    for i in (2, 7, 8, 10, 22):
        args[i] = args[i].reshape(1, -1)
    vmem = pl.BlockSpec(memory_space=pltpu.VMEM)
    hbm = pl.BlockSpec(memory_space=pl.ANY)
    small = (2, 7, 8, 10, 11, 12, 22)
    scratch = [
        ((SEQ, WIDTH), BF),
        ((NZ, 64, 512), BF),
        ((NT, WIDE, 2 * WIDE), BF),
        ((PAIR, FF, WIDTH), BF),
        ((PAIR, NT, FF, WIDE), BF),
        ((SEQ, 1, HEAD, HEAD), F32),
        ((WIDTH, 2 * PAIR * FF), BF),
        ((WIDTH, 2 * FF), BF),
        ((FF, WIDTH), BF),
        ((HEAD, WIDTH), BF),
        ((WIDE, WIDE), BF),
        ((NX, SEQ, 512), BF),
        ((NX, SEQ, 512), BF),
        ((NX, SEQ, 512), BF),
        ((NX, SEQ, 512), BF),
        ((SEQ, WIDTH), BF),
        ((NT, SEQ, WIDE), BF),
        ((NE, SEQ, WIDE), BF),
        ((SEQ, WIDTH), BF),
        ((NE, PAD, WIDE), BF),
        ((NE, PAD, WIDE), BF),
        ((PAIR * SLOTS, WIDTH), BF),
        ((PAIR * SLOTS, WIDTH), BF),
        ((NE // NT, SEQ, WIDTH), BF),
        ((ROWS, WIDTH), BF),
        ((NT, ROWS, WIDE), BF),
        ((PAIR * SLOTS, NT * FF), BF),
        ((SEQ, WIDTH), BF),
        ((NT, SEQ, WIDE), BF),
        ((NZ, NX, SEQ, WIDE), BF),
        ((NX, NZ, SEQ, WIDE), BF),
        ((NZ, SEQ, WIDE), BF),
        ((NZ, SEQ, WIDE), BF),
        ((NE, PAD, WIDE), BF),
        ((NE, PAD, WIDE), BF),
        ((SEQ, HEAD), F32),
        ((SEQ, PADDED), F32),
        ((PADDED, SEQ), BF),
        ((PAIR * SLOTS, PADDED), BF),
        ((PADDED, PAIR * SLOTS), BF),
        ((HEAD, SEQ), F32),
        ((HEAD, SEQ), F32),
        ((SEQ, HEAD), F32),
        ((SEQ, WIDE), F32),
    ]
    return pl.pallas_call(
        layer,
        out_shape=[
            jax.ShapeDtypeStruct((SEQ, WIDE), BF),
            jax.ShapeDtypeStruct((SEQ, 1, HEAD, HEAD), F32),
        ],
        in_specs=[vmem if i in small else hbm for i in range(len(args))],
        out_specs=[vmem, hbm],
        scratch_shapes=[pltpu.VMEM(shape, kind) for shape, kind in scratch]
        + [
            pltpu.SemaphoreType.DMA((SENDS,)),
            pltpu.SemaphoreType.DMA((ARRIVALS,)),
            pltpu.SemaphoreType.DMA((LOCALS,)),
        ],
        compiler_params=pltpu.CompilerParams(collective_id=0, has_side_effects=True),
        name="layer",
    )(*args)


def solution(mesh):
    torus = Mesh(mesh.devices.reshape(NZ, NX, NY, NC), ("z", "x", "y", "c"))
    return jax.shard_map(
        local,
        mesh=torus,
        in_specs=(
            P(EP, None),
            P(EP, TP, None, None),
            P(),
            P(EP, TP),
            P(EP, TP),
            P(EP, TP),
            P(EP, TP),
            P(TP),
            P(TP),
            P(TP, None),
            P(),
            P(EP, None),
            P(EP, None),
            P(EP, None, TP),
            P(EP, None, TP),
            P(EP, TP, None),
            P(None, TP),
            P(None, TP),
            P(TP, None),
            P(TP, EP),
            P(TP, EP),
            P(EP, TP),
            P(TP),
        ),
        out_specs=(P(EP, TP), P(EP, TP, None, None)),
        check_vma=False,
    )
```

```python
import jax
import jax.numpy as jnp
from jax import lax
from jax.experimental import pallas as pl
from jax.experimental.pallas import tpu as pltpu
from jax.sharding import Mesh
from jax.sharding import PartitionSpec as P

EP = ("z", "x")
TP = ("y", "c")
NZ, NX, NY, NC = 8, 4, 4, 2
NE, NT = NZ * NX, NY * NC
MESH = pl.DeviceIdType.MESH
EPS = 1e-06
SEQ, WIDTH, HEAD, WIDE, TOPK = 48, 2048, 128, 256, 4
PAIR, CAP, PAD = 2, 6, 16
SLOTS, PADDED = NE * CAP, NE * PAD
ROWS = SEQ * NE // NT
FF = 128
OWN = SEQ // NT
TILE = OWN * WIDTH // 128

BF, F32 = jnp.bfloat16, jnp.float32
Z_ORDER = (1, 7, 2, 6, 3, 5, 4)
Y_ORDER = (1, 3, 2)
X_ORDER = (1, 3, 2)
FAR_ORDER = (4, 3, 5, 2, 6, 1, 7, 0)
SENDS, ARRIVALS, LOCALS = 140, 162, 19
STRIPS = 6
scope = jax.named_scope


def cols_at(ref, index, width):
    start = pl.multiple_of(index * width, width)
    return ref.at[(slice(None),) * (len(ref.shape) - 1) + (pl.ds(start, width),)]


def dot(left, right):
    return jnp.dot(left, right, preferred_element_type=F32)


def iota(shape, dim):
    return lax.broadcasted_iota(jnp.int32, shape, dim)


def scaled(values, gain):
    values = values.astype(F32)
    return values * lax.rsqrt(jnp.mean(values * values, axis=-1, keepdims=True) + EPS) * gain


class Links:
    def __init__(self, send_sem, recv_sem, local_sem):
        self.send_sem, self.recv_sem, self.local_sem = send_sem, recv_sem, local_sem
        self.sent = self.received = self.locals = 0
        self.z, self.x = lax.axis_index("z"), lax.axis_index("x")
        self.y, self.c = lax.axis_index("y"), lax.axis_index("c")
        self.e = self.z * NX + self.x
        self.t = self.y * NC + self.c
        self.pending = []

    def load(self, src, dst):
        copy = pltpu.make_async_copy(src, dst, self.local_sem.at[self.locals])
        self.locals += 1
        copy.start()
        return copy

    def reserve(self, number):
        first = self.received
        self.received += number
        return first

    def new_send(self):
        self.sent += 1
        return self.sent - 1

    def copy(self, src, dst, sent, slot, **device):
        return pltpu.make_async_remote_copy(
            src_ref=src,
            dst_ref=dst,
            send_sem=self.send_sem.at[sent],
            recv_sem=self.recv_sem.at[slot],
            device_id=device,
            device_id_type=MESH,
        )

    def send(self, src, dst, slot, **device):
        copy = self.copy(src, dst, self.new_send(), slot, **device)
        copy.start()
        self.pending.append(copy)

    def wait(self, dst, slot):
        self.copy(dst, dst, 0, slot, c=1 - self.c).wait_recv()

    def finish(self):
        for copy in self.pending:
            copy.wait_send()
        assert (self.sent, self.received, self.locals) == (SENDS, ARRIVALS, LOCALS)

    def greet(self):
        barrier = pltpu.get_barrier_semaphore()
        peers = []
        for dz in range(NZ):
            for dx in range(NX):
                if dz or dx:
                    peers.append(dict(z=(self.z + dz) % NZ, x=(self.x + dx) % NX))
        for dy in range(NY):
            for dc in range(NC):
                if dy or dc:
                    peers.append(dict(y=(self.y + dy) % NY, c=(self.c + dc) % NC))
        for peer in peers:
            pl.semaphore_signal(barrier, inc=1, device_id=peer, device_id_type=MESH)
        return lambda: pl.semaphore_wait(barrier, len(peers))

    def gather_tp(self, view):
        base = self.reserve(NT)
        mine = view(self.t)
        for dy in Y_ORDER:
            self.send(mine, mine, base + self.t, y=(self.y + dy) % NY)
        self.send(mine, mine, base + self.t, c=1 - self.c)

        def relay():
            for dy in Y_ORDER:
                t = ((self.y + dy) % NY) * NC + self.c
                block = view(t)
                self.wait(block, base + t)
                self.send(block, block, base + t, c=1 - self.c)

        def rest():
            for dy in (0,) + Y_ORDER:
                t = ((self.y + dy) % NY) * NC + 1 - self.c
                self.wait(view(t), base + t)

        return relay, rest

    def swap_tp(self, src_view, dst_view):
        base = self.reserve(NT)
        mine = dst_view(self.t)
        others = []
        for dy in Y_ORDER + (0,):
            for dc in range(NC):
                if dy or dc:
                    others.append(((self.y + dy) % NY, (self.c + dc) % NC))
        for y, c in others:
            self.send(src_view(y * NC + c), mine, base + self.t, y=y, c=c)

        def rest():
            for y, c in others:
                t = y * NC + c
                self.wait(dst_view(t), base + t)

        return rest

    def swap_ep(self, src, dst):
        slot, sent = self.reserve(1), self.new_send()
        for dz in (4, 3, 5, 2, 6, 1, 7, 0):
            for dx in (2, 1, 3, 0):
                if dz or dx:
                    z, x = (self.z + dz) % NZ, (self.x + dx) % NX
                    self.copy(src.at[z * NX + x], dst.at[self.e], sent, slot, z=z, x=x).start()
        self.pending.append(self.copy(src.at[pl.ds(0, NE - 1)], dst.at[pl.ds(0, NE - 1)], sent, slot, c=1 - self.c))
        return lambda: self.wait(dst.at[pl.ds(0, NE - 1)], slot)


def layer(
    tokens,
    state,
    norm_gain,
    w_query,
    w_forget,
    w_input,
    w_outgate,
    lower_bound,
    head_gain,
    w_output,
    ffn_gain,
    route_ids,
    route_weight,
    expert_gate,
    expert_up,
    expert_down,
    shared_gate,
    shared_up,
    shared_down,
    dense_gate,
    dense_up,
    dense_down,
    dense_mix,
    mixed,
    gates,
    tok,
    wz,
    dense_w,
    down_own,
    down_all,
    held,
    expert_w,
    shared_w,
    shared_d,
    out_w,
    dense_d,
    tok_out,
    tok_in,
    part_out,
    part_in,
    head_part,
    head_in,
    rows,
    flat,
    tok_rows,
    row_out,
    row_in,
    pack,
    unpack,
    order,
    unit_rows,
    dense_raw,
    resid_rows,
    slot_out,
    slot_in,
    chosen,
    chosen_in,
    dense_in,
    dense_hidden,
    hidden,
    shared_part,
    shared_in,
    sum_out,
    sum_in,
    sum2_out,
    sum2_in,
    back_out,
    back_in,
    readout,
    combine,
    dispatch,
    squeeze,
    expand,
    resid,
    send_sem,
    recv_sem,
    local_sem,
):
    n = Links(send_sem, recv_sem, local_sem)
    met = n.greet()
    own_down = cols_at(expert_down, n.t, WIDE)
    load_tok = n.load(tokens, tok)
    load_w = [
        n.load(w, wz.at[n.z, :, pl.ds(i * HEAD, HEAD)])
        for i, w in enumerate((w_query, w_forget, w_input, w_outgate))
    ]
    load_dense = [
        n.load(w, dense_w.at[n.t, :, pl.ds(i * WIDE, WIDE)]) for i, w in enumerate((dense_gate, dense_up))
    ]
    load_down = n.load(expert_down, down_own)
    load_mine = n.load(own_down, down_all.at[:, n.t])
    load_state = n.load(state, held)
    load_out = n.load(w_output, out_w)
    load_shared = [
        n.load(shared_gate, shared_w.at[:, pl.ds(0, FF)]),
        n.load(shared_up, shared_w.at[:, pl.ds(FF, FF)]),
        n.load(shared_down, shared_d),
    ]
    load_expert = [
        n.load(w.at[j], expert_w.at[:, pl.ds((2 * j + i) * FF, FF)])
        for j in range(PAIR)
        for i, w in enumerate((expert_gate, expert_up))
    ]
    load_dense_d = n.load(dense_down, dense_d)

    load_tok.wait()
    normed = scaled(tok[...], norm_gain[...]).astype(BF)
    for x in range(NX):
        for z in range(NZ):
            start = (z * NX + x) * 64
            tok_out[x, :, z * 64 : (z + 1) * 64] = normed[:, start : start + 64]
    tok_in[pl.ds(n.x, 1)] = tok_out[pl.ds(n.x, 1)]

    met()
    for copy in load_w:
        copy.wait()
    base_w = n.reserve(NZ)
    for dz in Z_ORDER:
        n.send(wz.at[n.z], wz.at[n.z], base_w + n.z, z=(n.z + dz) % NZ)
    base_t = n.reserve(NX)
    for dx in X_ORDER:
        x = (n.x + dx) % NX
        n.send(tok_out.at[x], tok_in.at[n.x], base_t + n.x, x=x)
    for copy in load_dense:
        copy.wait()
    dense_relay, dense_rest = n.gather_tp(lambda t: dense_w.at[t])

    with scope("routes"):
        expert_row = iota((128, SEQ), 0)
        named = [route_ids[k : k + 1, :] for k in range(TOPK)]
        equal = [(expert_row == ids).astype(F32) for ids in named]
        earlier = (iota((SEQ, SEQ), 0) < iota((SEQ, SEQ), 1)).astype(BF)
        rank = dot(sum(equal).astype(BF), earlier)
        slot_row = iota((PADDED, SEQ), 0).astype(F32)
        total = jnp.zeros((PADDED, SEQ), F32)
        picked = jnp.zeros((PADDED, SEQ), F32)
        for k in range(TOPK):
            ids = named[k]
            first = (ids // 2) * PAD + (ids % 2) * CAP
            place = first.astype(F32) + jnp.sum(equal[k] * rank, axis=0, keepdims=True)
            here = slot_row == place
            total = total + jnp.where(here, route_weight[k : k + 1, :], 0.0)
            picked = picked + here.astype(F32)
        dispatch[...] = picked.astype(BF)
        combine[...] = total.T

    def row_of(slot):
        inside = slot % PAD
        second = (inside >= CAP).astype(jnp.int32)
        row = second * SLOTS + (slot // PAD) * CAP + inside - second * CAP
        return jnp.where(inside < PAIR * CAP, row, -1)

    squeeze[...] = (iota((PAIR * SLOTS, PADDED), 0) == row_of(iota((1, PADDED), 1))).astype(F32).astype(BF)
    expand[...] = (iota((PADDED, PAIR * SLOTS), 1) == row_of(iota((PADDED, 1), 0))).astype(F32).astype(BF)

    def packed_row(row):
        inside = row % SEQ
        return (inside // OWN) * TILE + (row // SEQ) * OWN + inside % OWN

    def ordered_row(row):
        inside = row % SEQ
        return (inside // OWN) * SEQ + (row // SEQ) * OWN + inside % OWN

    many, few = NT * TILE, NT * SEQ
    pack[...] = (iota((many, many), 0) == packed_row(iota((1, many), 1))).astype(F32).astype(BF)
    unpack[...] = (iota((many, many), 1) == packed_row(iota((many, 1), 0))).astype(F32).astype(BF)
    order[...] = (iota((few, few), 0) == ordered_row(iota((1, few), 1))).astype(F32).astype(BF)
    for k in range(WIDTH // 128):
        flat[k * SEQ : (k + 1) * SEQ, :] = tok[:, k * 128 : (k + 1) * 128]
    tok_rows[...] = dot(pack[...], flat[...]).astype(BF).reshape(NT, TILE, 128)

    for dx in X_ORDER:
        x = (n.x + dx) % NX
        n.wait(tok_in.at[x], base_t + x)
    for dz in Z_ORDER:
        z = (n.z + dz) % NZ
        n.wait(wz.at[z], base_w + z)
    part = dot(tok_in[...].reshape(NX * SEQ, 512), wz[...].reshape(512, 512))
    part_out[...] = part.astype(BF).reshape(NX, SEQ, 512)
    base_p = n.reserve(NX)
    for dx in X_ORDER:
        x = (n.x + dx) % NX
        n.send(part_out.at[x], part_in.at[n.x], base_p + n.x, x=x)
    part_in[pl.ds(n.x, 1)] = part_out[pl.ds(n.x, 1)]
    for dx in X_ORDER:
        x = (n.x + dx) % NX
        n.wait(part_in.at[x], base_p + x)
    projected = part_in[0].astype(F32)
    for x in range(1, NX):
        projected = projected + part_in[x].astype(F32)
    projected = projected.astype(BF).astype(F32)
    query, forget_pre = projected[:, :HEAD], projected[:, HEAD : 2 * HEAD]
    values, out_gate = projected[:, 2 * HEAD : 3 * HEAD], projected[:, 3 * HEAD :]
    low = lower_bound[...]
    forget_sig = jax.nn.sigmoid(forget_pre)
    decay = low + (1.0 - low) * forget_sig
    keygate = (1.0 - low) * (1.0 - forget_sig)
    mixed_q = (query * decay).T
    gates[0], gates[1], gates[2] = decay, keygate, values
    load_state.wait()
    for b in range(SEQ):
        readout[b : b + 1, :] = jnp.sum(mixed_q[:, b : b + 1] * held[b, 0], axis=0, keepdims=True)
    read = readout[...] + jnp.sum(query * keygate, axis=1, keepdims=True) * values
    read = read * lax.rsqrt(jnp.mean(read * read, axis=-1, keepdims=True) + EPS)
    head_out = (read * head_gain[...] * jax.nn.silu(out_gate)).astype(BF)
    load_out.wait()
    whole = dot(head_out, out_w[...]).astype(BF)
    for k in range(WIDTH // 128):
        flat[k * SEQ : (k + 1) * SEQ, :] = whole[:, k * 128 : (k + 1) * 128]
    row_out[...] = dot(pack[...], flat[...]).astype(BF).reshape(NT, TILE, 128)
    row_rest = n.swap_tp(lambda t: row_out.at[t], lambda t: row_in.at[t])
    head_part[...] = whole
    head_rest = n.swap_tp(lambda t: cols_at(head_part, t, WIDE), lambda t: head_in.at[t])
    row_in[pl.ds(n.t, 1)] = row_out[pl.ds(n.t, 1)]
    head_in[pl.ds(n.t, 1)] = cols_at(head_part, n.t, WIDE)[...][None]
    row_rest()
    own = tok_rows[pl.ds(n.t, 1)][0].astype(F32)
    for t in range(NT):
        own = own + row_in[t].astype(F32)
    rows[pl.ds(n.e, 1)] = own.astype(BF)[None]

    base_c = n.reserve(NE)
    mine = rows.at[n.e]
    for dz in Z_ORDER:
        n.send(mine, mine, base_c + n.e, z=(n.z + dz) % NZ)
    for dx in X_ORDER:
        n.send(mine, mine, base_c + n.e, x=(n.x + dx) % NX)
    head_rest()
    own = cols_at(tok, n.t, WIDE)[...].astype(F32)
    for t in range(NT):
        own = own + head_in[t].astype(F32)
    resid[...] = own
    own_cols = own.astype(BF)
    slot_out[...] = dot(dispatch[...], own_cols).astype(BF).reshape(NE, PAD, WIDE)
    slots_rest = n.swap_ep(slot_out, slot_in)
    slot_in[pl.ds(n.e, 1)] = slot_out[pl.ds(n.e, 1)]
    cols_at(resid_rows, n.t, WIDE)[...] = own_cols
    rows_relay, rows_rest = n.gather_tp(lambda t: cols_at(resid_rows, t, WIDE))
    load_down.wait()
    down_rest = n.swap_tp(lambda t: cols_at(down_own, t, WIDE), lambda t: down_all.at[:, t])
    for dz in Z_ORDER:
        e = ((n.z + dz) % NZ) * NX + n.x
        n.wait(rows.at[e], base_c + e)
        for dx in X_ORDER:
            n.send(rows.at[e], rows.at[e], base_c + e, x=(n.x + dx) % NX)
    rows_relay()
    dense_relay()

    slots_rest()
    picked_rows = dot(squeeze[...], slot_in[...].reshape(PADDED, WIDE)).astype(BF)
    cols_at(chosen, n.t, WIDE)[...] = picked_rows
    chosen_relay, chosen_rest = n.gather_tp(lambda t: cols_at(chosen, t, WIDE))

    for dz in (0,) + Z_ORDER:
        for dx in X_ORDER:
            e = ((n.z + dz) % NZ) * NX + (n.x + dx) % NX
            n.wait(rows.at[e], base_c + e)
    gain = ffn_gain[...]
    for g in range(NE // NT):
        group = dot(unpack[...], rows[g * NT : (g + 1) * NT].reshape(NT * TILE, 128))
        for k in range(WIDTH // 128):
            dense_raw[:, k * 128 : (k + 1) * 128] = group[k * SEQ : (k + 1) * SEQ, :]
        dense_in[g * SEQ : (g + 1) * SEQ, :] = scaled(dense_raw[...], gain).astype(BF)
    dense_rest()
    pre = dot(dense_in[...], dense_w[...].reshape(WIDTH, 2 * WIDE))
    dense_hidden[pl.ds(n.t, 1)] = (jax.nn.silu(pre[:, :WIDE]) * pre[:, WIDE:]).astype(BF)[None]
    units_relay, units_rest = n.gather_tp(lambda t: dense_hidden.at[t])

    chosen_relay()
    chosen_rest()
    for copy in load_expert:
        copy.wait()
    for j in range(PAIR):
        for i in range(4):
            part = pl.ds(j * SLOTS + i * SEQ, SEQ)
            chosen_in[part] = scaled(chosen[part], gain).astype(BF)
        pre = dot(chosen_in[pl.ds(j * SLOTS, SLOTS)], expert_w[:, 2 * j * FF : 2 * (j + 1) * FF])
        unit = (jax.nn.silu(pre[:, :FF]) * pre[:, FF:]).astype(BF)
        cols_at(hidden, n.t, FF).at[pl.ds(j * SLOTS, SLOTS)][...] = unit
    hidden_relay, hidden_rest = n.gather_tp(lambda t: cols_at(hidden, t, FF))

    rows_rest()
    for copy in load_shared:
        copy.wait()
    shared_x = scaled(resid_rows[...], ffn_gain[...]).astype(BF)
    shared_pre = dot(shared_x, shared_w[...])
    shared_hidden = (jax.nn.silu(shared_pre[:, :FF]) * shared_pre[:, FF:]).astype(BF)
    shared_part[...] = dot(shared_hidden, shared_d[...]).astype(BF)
    shared_rest = n.swap_tp(lambda t: cols_at(shared_part, t, WIDE), lambda t: shared_in.at[t])
    shared_in[pl.ds(n.t, 1)] = cols_at(shared_part, n.t, WIDE)[...][None]

    units_relay()
    units_rest()
    load_dense_d.wait()
    scale = jax.nn.sigmoid(dense_mix[...])
    for g in range(NE // NT):
        for t in range(NT):
            unit_rows[t * SEQ : (t + 1) * SEQ, :] = dense_hidden[t, g * SEQ : (g + 1) * SEQ, :]
        inner = dot(order[...], unit_rows[...]).astype(BF)
        block = dot(inner, dense_d[...]) * scale
        sum_out[2 * g : 2 * g + 2] = block.astype(BF).reshape(2, NX, SEQ, WIDE)
    base_x = n.reserve(NX * NZ)
    for dz in FAR_ORDER:
        z = (n.z + dz) % NZ
        for dx in X_ORDER:
            x = (n.x + dx) % NX
            n.send(sum_out.at[z, x], sum_in.at[n.x, z], base_x + n.x * NZ + z, x=x)

    hidden_relay()
    down_rest()
    load_mine.wait()
    hidden_rest()
    outs = [
        dot(hidden[pl.ds(j * SLOTS, SLOTS)], down_all[j].reshape(NT * FF, WIDE)).astype(BF) for j in range(PAIR)
    ]
    spread = dot(expand[:, :SLOTS], outs[0]) + dot(expand[:, SLOTS:], outs[1])
    back_out[...] = spread.astype(BF).reshape(NE, PAD, WIDE)
    back_rest = n.swap_ep(back_out, back_in)
    back_in[pl.ds(n.e, 1)] = back_out[pl.ds(n.e, 1)]

    base_z = n.reserve(NZ)
    for dz in FAR_ORDER:
        z = (n.z + dz) % NZ
        block = sum_out[pl.ds(z, 1), n.x][0].astype(F32)
        for dx in X_ORDER:
            x = (n.x + dx) % NX
            n.wait(sum_in.at[x, z], base_x + x * NZ + z)
            block = block + sum_in[x, pl.ds(z, 1)][0].astype(F32)
        if dz:
            sum2_out[pl.ds(z, 1)] = block.astype(BF)[None]
            n.send(sum2_out.at[z], sum2_in.at[n.z], base_z + n.z, z=z)
        else:
            sum2_in[pl.ds(n.z, 1)] = block.astype(BF)[None]
    back_rest()
    shared_rest()
    result = resid[...] + jnp.dot(
        combine[...],
        back_in[...].reshape(PADDED, WIDE).astype(F32),
        preferred_element_type=F32,
        precision=lax.Precision.HIGHEST,
    )
    for t in range(NT):
        result = result + shared_in[t].astype(F32)
    for dz in Z_ORDER:
        z = (n.z + dz) % NZ
        n.wait(sum2_in.at[z], base_z + z)
    for z in range(NZ):
        result = result + sum2_in[z].astype(F32)
    mixed[...] = result
    n.finish()


def closing(result, gates, state, mixed, new_state, held, sem):
    rows = SEQ // STRIPS
    strips = [pl.ds(i * rows, rows) for i in range(STRIPS)]
    loads = [pltpu.make_async_copy(state.at[r], held.at[r], sem.at[i]) for i, r in enumerate(strips)]
    stores = [
        pltpu.make_async_copy(held.at[r], new_state.at[r], sem.at[STRIPS + i]) for i, r in enumerate(strips)
    ]
    for copy in loads:
        copy.start()
    mixed[...] = result[...].astype(BF)
    decay, keygate = gates[0].T, gates[1].T
    for i in range(STRIPS):
        loads[i].wait()
        for b in range(i * rows, (i + 1) * rows):
            held[b, 0] = decay[:, b : b + 1] * held[b, 0] + keygate[:, b : b + 1] * gates[2, b : b + 1, :]
        stores[i].start()
    for copy in stores:
        copy.wait()


def local(*args):
    args = list(args)
    state = args[1]
    for i in (2, 7, 8, 10, 22):
        args[i] = args[i].reshape(1, -1)
    for i in (11, 12):
        args[i] = args[i].T
    vmem = pl.BlockSpec(memory_space=pltpu.VMEM)
    hbm = pl.BlockSpec(memory_space=pl.ANY)
    small = (2, 7, 8, 10, 11, 12, 22)
    scratch = [
        ((SEQ, WIDTH), BF),
        ((NZ, 64, 512), BF),
        ((NT, WIDE, 2 * WIDE), BF),
        ((PAIR, FF, WIDTH), BF),
        ((PAIR, NT, FF, WIDE), BF),
        ((SEQ, 1, HEAD, HEAD), F32),
        ((WIDTH, 2 * PAIR * FF), BF),
        ((WIDTH, 2 * FF), BF),
        ((FF, WIDTH), BF),
        ((HEAD, WIDTH), BF),
        ((WIDE, WIDE), BF),
        ((NX, SEQ, 512), BF),
        ((NX, SEQ, 512), BF),
        ((NX, SEQ, 512), BF),
        ((NX, SEQ, 512), BF),
        ((SEQ, WIDTH), BF),
        ((NT, SEQ, WIDE), BF),
        ((NE, TILE, 128), BF),
        ((NT * TILE, 128), BF),
        ((NT, TILE, 128), BF),
        ((NT, TILE, 128), BF),
        ((NT, TILE, 128), BF),
        ((NT * TILE, NT * TILE), BF),
        ((NT * TILE, NT * TILE), BF),
        ((NT * SEQ, NT * SEQ), BF),
        ((NT * SEQ, WIDE), BF),
        ((SEQ, WIDTH), F32),
        ((SEQ, WIDTH), BF),
        ((NE, PAD, WIDE), BF),
        ((NE, PAD, WIDE), BF),
        ((PAIR * SLOTS, WIDTH), BF),
        ((PAIR * SLOTS, WIDTH), BF),
        ((ROWS, WIDTH), BF),
        ((NT, ROWS, WIDE), BF),
        ((PAIR * SLOTS, NT * FF), BF),
        ((SEQ, WIDTH), BF),
        ((NT, SEQ, WIDE), BF),
        ((NZ, NX, SEQ, WIDE), BF),
        ((NX, NZ, SEQ, WIDE), BF),
        ((NZ, SEQ, WIDE), BF),
        ((NZ, SEQ, WIDE), BF),
        ((NE, PAD, WIDE), BF),
        ((NE, PAD, WIDE), BF),
        ((SEQ, HEAD), F32),
        ((SEQ, PADDED), F32),
        ((PADDED, SEQ), BF),
        ((PAIR * SLOTS, PADDED), BF),
        ((PADDED, PAIR * SLOTS), BF),
        ((SEQ, WIDE), F32),
    ]
    result, gates = pl.pallas_call(
        layer,
        out_shape=[
            jax.ShapeDtypeStruct((SEQ, WIDE), F32),
            jax.ShapeDtypeStruct((3, SEQ, HEAD), F32),
        ],
        in_specs=[vmem if i in small else hbm for i in range(len(args))],
        out_specs=[vmem, vmem],
        scratch_shapes=[pltpu.VMEM(shape, kind) for shape, kind in scratch]
        + [
            pltpu.SemaphoreType.DMA((SENDS,)),
            pltpu.SemaphoreType.DMA((ARRIVALS,)),
            pltpu.SemaphoreType.DMA((LOCALS,)),
        ],
        compiler_params=pltpu.CompilerParams(collective_id=0, has_side_effects=True),
        name="layer",
    )(*args)
    return pl.pallas_call(
        closing,
        out_shape=[
            jax.ShapeDtypeStruct((SEQ, WIDE), BF),
            jax.ShapeDtypeStruct((SEQ, 1, HEAD, HEAD), F32),
        ],
        in_specs=[vmem, vmem, hbm],
        out_specs=[vmem, hbm],
        scratch_shapes=[
            pltpu.VMEM((SEQ, 1, HEAD, HEAD), F32),
            pltpu.SemaphoreType.DMA((2 * STRIPS,)),
        ],
        name="closing",
    )(result, gates, state)


def solution(mesh):
    torus = Mesh(mesh.devices.reshape(NZ, NX, NY, NC), ("z", "x", "y", "c"))
    return jax.shard_map(
        local,
        mesh=torus,
        in_specs=(
            P(EP, None),
            P(EP, TP, None, None),
            P(),
            P(EP, TP),
            P(EP, TP),
            P(EP, TP),
            P(EP, TP),
            P(TP),
            P(TP),
            P(TP, None),
            P(),
            P(EP, None),
            P(EP, None),
            P(EP, None, TP),
            P(EP, None, TP),
            P(EP, TP, None),
            P(None, TP),
            P(None, TP),
            P(TP, None),
            P(TP, EP),
            P(TP, EP),
            P(EP, TP),
            P(TP),
        ),
        out_specs=(P(EP, TP), P(EP, TP, None, None)),
        check_vma=False,
    )
```

```python
import jax
import jax.numpy as jnp
from jax import lax
from jax.experimental import pallas as pl
from jax.experimental.pallas import tpu as pltpu
from jax.sharding import Mesh
from jax.sharding import PartitionSpec as P

EP = ("z", "x")
TP = ("y", "c")
NZ, NX, NY, NC = 8, 4, 4, 2
NE, NT = NZ * NX, NY * NC
MESH = pl.DeviceIdType.MESH
EPS = 1e-06
SEQ, WIDTH, HEAD, WIDE, TOPK = 48, 2048, 128, 256, 4
PAIR, CAP, PAD = 2, 6, 16
SLOTS, PADDED = NE * CAP, NE * PAD
ROWS = SEQ * NE // NT
FF = 128
OWN = SEQ // NT
TILE = OWN * WIDTH // 128

BF, F32 = jnp.bfloat16, jnp.float32
Z_ORDER = (1, 7, 2, 6, 3, 5, 4)
Y_ORDER = (1, 3, 2)
X_ORDER = (1, 3, 2)
FAR_ORDER = (4, 3, 5, 2, 6, 1, 7, 0)
SENDS, ARRIVALS, LOCALS = 18, 62, 19
scope = jax.named_scope


def cols_at(ref, index, width):
    start = pl.multiple_of(index * width, width)
    return ref.at[(slice(None),) * (len(ref.shape) - 1) + (pl.ds(start, width),)]


def dot(left, right):
    return jnp.dot(left, right, preferred_element_type=F32)


def iota(shape, dim):
    return lax.broadcasted_iota(jnp.int32, shape, dim)


def scaled(values, gain):
    values = values.astype(F32)
    return values * lax.rsqrt(jnp.mean(values * values, axis=-1, keepdims=True) + EPS) * gain


class Links:
    def __init__(self, send_sem, recv_sem, local_sem):
        self.send_sem, self.recv_sem, self.local_sem = send_sem, recv_sem, local_sem
        self.sent = self.received = self.locals = 0
        self.z, self.x = lax.axis_index("z"), lax.axis_index("x")
        self.y, self.c = lax.axis_index("y"), lax.axis_index("c")
        self.e = self.z * NX + self.x
        self.t = self.y * NC + self.c
        self.pending = []

    def load(self, src, dst):
        copy = pltpu.make_async_copy(src, dst, self.local_sem.at[self.locals])
        self.locals += 1
        copy.start()
        return copy

    def reserve(self, number):
        first = self.received
        self.received += number
        return first

    def new_send(self):
        self.sent += 1
        return self.sent - 1

    def copy(self, src, dst, sent, slot, **device):
        return pltpu.make_async_remote_copy(
            src_ref=src,
            dst_ref=dst,
            send_sem=self.send_sem.at[sent],
            recv_sem=self.recv_sem.at[slot],
            device_id=device,
            device_id_type=MESH,
        )

    def stage(self, total):
        sent = self.new_send()
        self.pending.append(self.copy(total, total, sent, 0, c=1 - self.c))

        def send(src, dst, slot, **device):
            self.copy(src, dst, sent, slot, **device).start()

        return send

    def wait(self, dst, slot):
        self.copy(dst, dst, 0, slot, c=1 - self.c).wait_recv()

    def finish(self):
        for copy in self.pending:
            copy.wait_send()
        assert (self.sent, self.received, self.locals) == (SENDS, ARRIVALS, LOCALS)

    def greet(self):
        barrier = pltpu.get_barrier_semaphore()
        peers = []
        for dz in range(NZ):
            for dx in range(NX):
                if dz or dx:
                    peers.append(dict(z=(self.z + dz) % NZ, x=(self.x + dx) % NX))
        for dy in range(NY):
            for dc in range(NC):
                if dy or dc:
                    peers.append(dict(y=(self.y + dy) % NY, c=(self.c + dc) % NC))
        for peer in peers:
            pl.semaphore_signal(barrier, inc=1, device_id=peer, device_id_type=MESH)
        return lambda: pl.semaphore_wait(barrier, len(peers))

    def gather_tp(self, view, seven, four):
        base = self.reserve(7)
        send = self.stage(seven)
        up, down = (self.y + 1) % NY, (self.y + NY - 1) % NY
        far = (self.y + 2) % NY

        def half(y, i):
            block = view(y * NC + self.c)
            size = block.shape[0] // 2
            return block.at[(pl.ds(i * size, size),) + (slice(None),) * (len(block.shape) - 1)]

        for i in range(2):
            send(half(self.y, i), half(self.y, i), base + i, y=up)
            send(half(self.y, 1 - i), half(self.y, 1 - i), base + 2 + i, y=down)
        mine = view(self.t)
        send(mine, mine, base + 6, c=1 - self.c)

        def onward():
            self.wait(half(down, 0), base)
            send(half(down, 0), half(down, 0), base + 4, y=up)
            self.wait(half(up, 1), base + 2)
            send(half(up, 1), half(up, 1), base + 5, y=down)

        def relay():
            self.wait(half(down, 1), base + 1)
            block = view(down * NC + self.c)
            send(block, block, base + 6, c=1 - self.c)
            self.wait(half(up, 0), base + 3)
            block = view(up * NC + self.c)
            send(block, block, base + 6, c=1 - self.c)
            self.wait(half(far, 0), base + 4)
            self.wait(half(far, 1), base + 5)
            block = view(far * NC + self.c)
            send(block, block, base + 6, c=1 - self.c)

        def rest():
            self.wait(four, base + 6)

        return onward, relay, rest

    def swap_tp(self, src_view, dst_view, seven):
        base = self.reserve(1)
        send = self.stage(seven)
        mine = dst_view(self.t)
        for dy in Y_ORDER + (0,):
            for dc in range(NC):
                if dy or dc:
                    y, c = (self.y + dy) % NY, (self.c + dc) % NC
                    send(src_view(y * NC + c), mine, base, y=y, c=c)
        return lambda: self.wait(seven, base)

    def swap_ep(self, src, dst):
        slot, sent = self.reserve(1), self.new_send()
        for dz in (4, 3, 5, 2, 6, 1, 7, 0):
            for dx in (2, 1, 3, 0):
                if dz or dx:
                    z, x = (self.z + dz) % NZ, (self.x + dx) % NX
                    self.copy(src.at[z * NX + x], dst.at[self.e], sent, slot, z=z, x=x).start()
        self.pending.append(self.copy(src.at[pl.ds(0, NE - 1)], dst.at[pl.ds(0, NE - 1)], sent, slot, c=1 - self.c))
        return lambda: self.wait(dst.at[pl.ds(0, NE - 1)], slot)


def layer(
    tokens,
    state,
    norm_gain,
    w_query,
    w_forget,
    w_input,
    w_outgate,
    lower_bound,
    head_gain,
    w_output,
    ffn_gain,
    route_ids,
    route_weight,
    expert_gate,
    expert_up,
    expert_down,
    shared_gate,
    shared_up,
    shared_down,
    dense_gate,
    dense_up,
    dense_down,
    dense_mix,
    mixed,
    held,
    tok,
    wz,
    dense_w,
    down_own,
    down_all,
    gates,
    expert_w,
    shared_w,
    shared_d,
    out_w,
    dense_d,
    tok_out,
    tok_in,
    part_out,
    part_in,
    head_part,
    head_in,
    rows,
    flat,
    tok_rows,
    row_out,
    row_in,
    pack,
    unpack,
    order,
    unit_rows,
    dense_raw,
    resid_rows,
    slot_out,
    slot_in,
    chosen,
    chosen_in,
    dense_in,
    dense_hidden,
    hidden,
    shared_part,
    shared_in,
    sum_out,
    sum_in,
    sum2_out,
    sum2_in,
    back_out,
    back_in,
    readout,
    combine,
    dispatch,
    squeeze,
    expand,
    resid,
    send_sem,
    recv_sem,
    local_sem,
):
    n = Links(send_sem, recv_sem, local_sem)
    met = n.greet()
    own_down = cols_at(expert_down, n.t, WIDE)
    load_tok = n.load(tokens, tok)
    load_w = [
        n.load(w, wz.at[n.z, :, pl.ds(i * HEAD, HEAD)])
        for i, w in enumerate((w_query, w_forget, w_input, w_outgate))
    ]
    load_dense = [
        n.load(w, dense_w.at[n.t, :, pl.ds(i * WIDE, WIDE)]) for i, w in enumerate((dense_gate, dense_up))
    ]
    load_down = n.load(expert_down, down_own)
    load_mine = n.load(own_down, down_all.at[:, n.t])
    load_state = n.load(state, held)
    load_out = n.load(w_output, out_w)
    load_shared = [
        n.load(shared_gate, shared_w.at[:, pl.ds(0, FF)]),
        n.load(shared_up, shared_w.at[:, pl.ds(FF, FF)]),
        n.load(shared_down, shared_d),
    ]
    load_expert = [
        n.load(w.at[j], expert_w.at[:, pl.ds((2 * j + i) * FF, FF)])
        for j in range(PAIR)
        for i, w in enumerate((expert_gate, expert_up))
    ]
    load_dense_d = n.load(dense_down, dense_d)

    load_tok.wait()
    normed = scaled(tok[...], norm_gain[...]).astype(BF)
    for x in range(NX):
        for z in range(NZ):
            start = (z * NX + x) * 64
            tok_out[x, :, z * 64 : (z + 1) * 64] = normed[:, start : start + 64]
    tok_in[pl.ds(n.x, 1)] = tok_out[pl.ds(n.x, 1)]

    met()
    for copy in load_w:
        copy.wait()
    base_w = n.reserve(7)
    send_w = n.stage(wz.at[pl.ds(0, 7)])
    z_at = [(n.z + dz) % NZ for dz in range(NZ)]
    for dz, slot in ((2, 0), (6, 1), (1, 2), (7, 2)):
        send_w(wz.at[n.z], wz.at[n.z], base_w + slot, z=z_at[dz])
    base_t = n.reserve(1)
    send_t = n.stage(tok_in.at[pl.ds(0, 3)])
    for dx in X_ORDER:
        x = (n.x + dx) % NX
        send_t(tok_out.at[x], tok_in.at[n.x], base_t, x=x)
    for copy in load_dense:
        copy.wait()
    dense_onward, dense_relay, dense_rest = n.gather_tp(
        lambda t: dense_w.at[t], dense_w.at[pl.ds(0, 7)], dense_w.at[pl.ds(0, 4)]
    )

    with scope("routes"):
        expert_row = iota((128, SEQ), 0)
        named = [route_ids[k : k + 1, :] for k in range(TOPK)]
        equal = [(expert_row == ids).astype(F32) for ids in named]
        earlier = (iota((SEQ, SEQ), 0) < iota((SEQ, SEQ), 1)).astype(BF)
        rank = dot(sum(equal).astype(BF), earlier)
        slot_row = iota((PADDED, SEQ), 0).astype(F32)
        total = jnp.zeros((PADDED, SEQ), F32)
        picked = jnp.zeros((PADDED, SEQ), F32)
        for k in range(TOPK):
            ids = named[k]
            first = (ids // 2) * PAD + (ids % 2) * CAP
            place = first.astype(F32) + jnp.sum(equal[k] * rank, axis=0, keepdims=True)
            here = slot_row == place
            total = total + jnp.where(here, route_weight[k : k + 1, :], 0.0)
            picked = picked + here.astype(F32)
        dispatch[...] = picked.astype(BF)
        combine[...] = total.T

    def row_of(slot):
        inside = slot % PAD
        second = (inside >= CAP).astype(jnp.int32)
        row = second * SLOTS + (slot // PAD) * CAP + inside - second * CAP
        return jnp.where(inside < PAIR * CAP, row, -1)

    squeeze[...] = (iota((PAIR * SLOTS, PADDED), 0) == row_of(iota((1, PADDED), 1))).astype(F32).astype(BF)
    expand[...] = (iota((PADDED, PAIR * SLOTS), 1) == row_of(iota((PADDED, 1), 0))).astype(F32).astype(BF)

    def packed_row(row):
        inside = row % SEQ
        return (inside // OWN) * TILE + (row // SEQ) * OWN + inside % OWN

    def ordered_row(row):
        inside = row % SEQ
        return (inside // OWN) * SEQ + (row // SEQ) * OWN + inside % OWN

    many, few = NT * TILE, NT * SEQ
    pack[...] = (iota((many, many), 0) == packed_row(iota((1, many), 1))).astype(F32).astype(BF)
    unpack[...] = (iota((many, many), 1) == packed_row(iota((many, 1), 0))).astype(F32).astype(BF)
    order[...] = (iota((few, few), 0) == ordered_row(iota((1, few), 1))).astype(F32).astype(BF)
    for k in range(WIDTH // 128):
        flat[k * SEQ : (k + 1) * SEQ, :] = tok[:, k * 128 : (k + 1) * 128]
    tok_rows[...] = dot(pack[...], flat[...]).astype(BF).reshape(NT, TILE, 128)

    for source, near, far, row, slot in ((6, 1, 2, 0, 0), (2, 7, 6, 32, 1)):
        block = wz.at[z_at[source]]
        n.wait(block, base_w + slot)
        send_w(block, block, base_w + 3 + slot, z=z_at[near])
        block = wz.at[z_at[source], pl.ds(row, 32)]
        send_w(block, block, base_w + 5 + slot, z=z_at[far])
    dense_onward()
    load_down.wait()
    down_rest = [
        n.swap_tp(lambda t: cols_at(down_own.at[0], t, WIDE), lambda t: down_all.at[0, t], down_all.at[0, pl.ds(0, 7)])
    ]
    n.wait(tok_in.at[pl.ds(0, 3)], base_t)
    n.wait(wz.at[pl.ds(0, 2)], base_w + 2)
    for slot in range(2):
        n.wait(wz.at[0], base_w + 3 + slot)
        n.wait(wz.at[0, pl.ds(0, 32)], base_w + 5 + slot)
    part = dot(tok_in[...].reshape(NX * SEQ, 512), wz[...].reshape(512, 512))
    part_out[...] = part.astype(BF).reshape(NX, SEQ, 512)
    base_p = n.reserve(1)
    send_p = n.stage(part_in.at[pl.ds(0, 3)])
    for dx in X_ORDER:
        x = (n.x + dx) % NX
        send_p(part_out.at[x], part_in.at[n.x], base_p, x=x)
    part_in[pl.ds(n.x, 1)] = part_out[pl.ds(n.x, 1)]
    n.wait(part_in.at[pl.ds(0, 3)], base_p)
    projected = part_in[0].astype(F32)
    for x in range(1, NX):
        projected = projected + part_in[x].astype(F32)
    projected = projected.astype(BF).astype(F32)
    query, forget_pre = projected[:, :HEAD], projected[:, HEAD : 2 * HEAD]
    values, out_gate = projected[:, 2 * HEAD : 3 * HEAD], projected[:, 3 * HEAD :]
    low = lower_bound[...]
    forget_sig = jax.nn.sigmoid(forget_pre)
    decay = low + (1.0 - low) * forget_sig
    keygate = (1.0 - low) * (1.0 - forget_sig)
    mixed_q = (query * decay).T
    gates[0, :, :], gates[1, :, :], gates[2, :, :] = decay, keygate, values
    load_state.wait()
    for b in range(SEQ):
        readout[b : b + 1, :] = jnp.sum(mixed_q[:, b : b + 1] * held[b, 0], axis=0, keepdims=True)
    read = readout[...] + jnp.sum(query * keygate, axis=1, keepdims=True) * values
    read = read * lax.rsqrt(jnp.mean(read * read, axis=-1, keepdims=True) + EPS)
    head_out = (read * head_gain[...] * jax.nn.silu(out_gate)).astype(BF)
    load_out.wait()
    whole = dot(head_out, out_w[...]).astype(BF)
    for k in range(WIDTH // 128):
        flat[k * SEQ : (k + 1) * SEQ, :] = whole[:, k * 128 : (k + 1) * 128]
    row_out[...] = dot(pack[...], flat[...]).astype(BF).reshape(NT, TILE, 128)
    row_rest = n.swap_tp(lambda t: row_out.at[t], lambda t: row_in.at[t], row_in.at[pl.ds(0, 7)])
    head_part[...] = whole
    head_rest = n.swap_tp(lambda t: cols_at(head_part, t, WIDE), lambda t: head_in.at[t], head_in.at[pl.ds(0, 7)])
    row_in[pl.ds(n.t, 1)] = row_out[pl.ds(n.t, 1)]
    head_in[pl.ds(n.t, 1)] = cols_at(head_part, n.t, WIDE)[...][None]
    row_rest()
    own = tok_rows[pl.ds(n.t, 1)][0].astype(F32)
    for t in range(NT):
        own = own + row_in[t].astype(F32)
    rows[pl.ds(n.e, 1)] = own.astype(BF)[None]

    base_c = n.reserve(NZ)
    send_c = n.stage(rows.at[pl.ds(0, NE - 1)])
    mine = rows.at[n.e]
    for i, dz in enumerate(Z_ORDER):
        send_c(mine, mine, base_c + i, z=z_at[dz])
    for dx in X_ORDER:
        send_c(mine, mine, base_c + 7, x=(n.x + dx) % NX)
    head_rest()
    own = cols_at(tok, n.t, WIDE)[...].astype(F32)
    for t in range(NT):
        own = own + head_in[t].astype(F32)
    resid[...] = own
    own_cols = own.astype(BF)
    slot_out[...] = dot(dispatch[...], own_cols).astype(BF).reshape(NE, PAD, WIDE)
    slots_rest = n.swap_ep(slot_out, slot_in)
    slot_in[pl.ds(n.e, 1)] = slot_out[pl.ds(n.e, 1)]
    cols_at(resid_rows, n.t, WIDE)[...] = own_cols
    rows_mine = cols_at(resid_rows, n.t, WIDE)
    rows_seven = resid_rows.at[:, pl.ds(0, 7 * WIDE)]
    rows_rest = n.swap_tp(lambda t: rows_mine, lambda t: cols_at(resid_rows, t, WIDE), rows_seven)
    down_rest.append(
        n.swap_tp(lambda t: cols_at(down_own.at[1], t, WIDE), lambda t: down_all.at[1, t], down_all.at[1, pl.ds(0, 7)])
    )
    dense_relay()
    for i, dz in enumerate(Z_ORDER):
        e = z_at[(NZ - dz) % NZ] * NX + n.x
        n.wait(rows.at[e], base_c + i)
        for dx in X_ORDER:
            send_c(rows.at[e], rows.at[e], base_c + 7, x=(n.x + dx) % NX)

    gain = ffn_gain[...]
    rows_rest()
    for copy in load_shared:
        copy.wait()
    shared_x = scaled(resid_rows[...], gain).astype(BF)
    shared_pre = dot(shared_x, shared_w[...])
    shared_hidden = (jax.nn.silu(shared_pre[:, :FF]) * shared_pre[:, FF:]).astype(BF)
    shared_part[...] = dot(shared_hidden, shared_d[...]).astype(BF)
    shared_rest = n.swap_tp(lambda t: cols_at(shared_part, t, WIDE), lambda t: shared_in.at[t], shared_in.at[pl.ds(0, 7)])
    shared_in[pl.ds(n.t, 1)] = cols_at(shared_part, n.t, WIDE)[...][None]

    slots_rest()
    picked_rows = dot(squeeze[...], slot_in[...].reshape(PADDED, WIDE)).astype(BF)
    cols_at(chosen, n.t, WIDE)[...] = picked_rows
    chosen_onward, chosen_relay, chosen_rest = n.gather_tp(
        lambda t: cols_at(chosen, t, WIDE), chosen.at[:, pl.ds(0, 7 * WIDE)], chosen.at[:, pl.ds(0, 4 * WIDE)]
    )

    n.wait(rows.at[pl.ds(0, 24)], base_c + 7)
    for g in range(NE // NT):
        group = dot(unpack[...], rows[g * NT : (g + 1) * NT].reshape(NT * TILE, 128))
        for k in range(WIDTH // 128):
            dense_raw[:, k * 128 : (k + 1) * 128] = group[k * SEQ : (k + 1) * SEQ, :]
        dense_in[g * SEQ : (g + 1) * SEQ, :] = scaled(dense_raw[...], gain).astype(BF)
    dense_rest()
    pre = dot(dense_in[...], dense_w[...].reshape(WIDTH, 2 * WIDE))
    dense_hidden[pl.ds(n.t, 1)] = (jax.nn.silu(pre[:, :WIDE]) * pre[:, WIDE:]).astype(BF)[None]
    chosen_onward()
    units_onward, units_relay, units_rest = n.gather_tp(
        lambda t: dense_hidden.at[t], dense_hidden.at[pl.ds(0, 7)], dense_hidden.at[pl.ds(0, 4)]
    )

    decay, keygate = gates[0].T, gates[1].T
    for b in range(SEQ):
        held[b, 0] = decay[:, b : b + 1] * held[b, 0] + keygate[:, b : b + 1] * gates[2, b : b + 1, :]

    chosen_relay()
    units_onward()
    chosen_rest()
    for copy in load_expert:
        copy.wait()
    for j in range(PAIR):
        for i in range(4):
            part = pl.ds(j * SLOTS + i * SEQ, SEQ)
            chosen_in[part] = scaled(chosen[part], gain).astype(BF)
        pre = dot(chosen_in[pl.ds(j * SLOTS, SLOTS)], expert_w[:, 2 * j * FF : 2 * (j + 1) * FF])
        unit = (jax.nn.silu(pre[:, :FF]) * pre[:, FF:]).astype(BF)
        cols_at(hidden, n.t, FF).at[pl.ds(j * SLOTS, SLOTS)][...] = unit
    hidden_onward, hidden_relay, hidden_rest = n.gather_tp(
        lambda t: cols_at(hidden, t, FF), hidden.at[:, pl.ds(0, 7 * FF)], hidden.at[:, pl.ds(0, 4 * FF)]
    )

    units_relay()
    hidden_onward()
    units_rest()
    load_dense_d.wait()
    scale = jax.nn.sigmoid(dense_mix[...])
    for g in range(NE // NT):
        for t in range(NT):
            unit_rows[t * SEQ : (t + 1) * SEQ, :] = dense_hidden[t, g * SEQ : (g + 1) * SEQ, :]
        inner = dot(order[...], unit_rows[...]).astype(BF)
        block = dot(inner, dense_d[...]) * scale
        sum_out[2 * g : 2 * g + 2] = block.astype(BF).reshape(2, NX, SEQ, WIDE)
    base_x = n.reserve(NZ)
    send_x = n.stage(sum_in.at[pl.ds(0, 3)])
    for i, dz in enumerate(FAR_ORDER):
        for dx in X_ORDER:
            x = (n.x + dx) % NX
            send_x(sum_out.at[z_at[dz], x], sum_in.at[n.x, z_at[dz]], base_x + i, x=x)

    hidden_relay()
    for rest in down_rest:
        rest()
    load_mine.wait()
    hidden_rest()
    outs = [
        dot(hidden[pl.ds(j * SLOTS, SLOTS)], down_all[j].reshape(NT * FF, WIDE)).astype(BF) for j in range(PAIR)
    ]
    spread = dot(expand[:, :SLOTS], outs[0]) + dot(expand[:, SLOTS:], outs[1])
    back_out[...] = spread.astype(BF).reshape(NE, PAD, WIDE)
    back_rest = n.swap_ep(back_out, back_in)
    back_in[pl.ds(n.e, 1)] = back_out[pl.ds(n.e, 1)]

    base_z = n.reserve(1)
    send_z = n.stage(sum2_in.at[pl.ds(0, 7)])
    for i, dz in enumerate(FAR_ORDER):
        z = z_at[dz]
        n.wait(sum_in.at[pl.ds(0, 3), z], base_x + i)
        block = sum_out[pl.ds(z, 1), n.x][0].astype(F32)
        for dx in X_ORDER:
            block = block + sum_in[(n.x + dx) % NX, pl.ds(z, 1)][0].astype(F32)
        if dz:
            sum2_out[pl.ds(z, 1)] = block.astype(BF)[None]
            send_z(sum2_out.at[z], sum2_in.at[n.z], base_z, z=z)
        else:
            sum2_in[pl.ds(n.z, 1)] = block.astype(BF)[None]
    back_rest()
    shared_rest()
    result = resid[...] + jnp.dot(
        combine[...],
        back_in[...].reshape(PADDED, WIDE).astype(F32),
        preferred_element_type=F32,
        precision=lax.Precision.HIGHEST,
    )
    for t in range(NT):
        result = result + shared_in[t].astype(F32)
    n.wait(sum2_in.at[pl.ds(0, 7)], base_z)
    for z in range(NZ):
        result = result + sum2_in[z].astype(F32)
    mixed[...] = result
    n.finish()


def closing(result, held, mixed, new_state, sem):
    copy = pltpu.make_async_copy(held, new_state, sem)
    copy.start()
    mixed[...] = result[...].astype(BF)
    copy.wait()


def local(*args):
    args = list(args)
    for i in (2, 7, 8, 10, 22):
        args[i] = args[i].reshape(1, -1)
    for i in (11, 12):
        args[i] = args[i].T
    vmem = pl.BlockSpec(memory_space=pltpu.VMEM)
    hbm = pl.BlockSpec(memory_space=pl.ANY)
    small = (2, 7, 8, 10, 11, 12, 22)
    scratch = [
        ((SEQ, WIDTH), BF),
        ((NZ, 64, 512), BF),
        ((NT, WIDE, 2 * WIDE), BF),
        ((PAIR, FF, WIDTH), BF),
        ((PAIR, NT, FF, WIDE), BF),
        ((3, SEQ, HEAD), F32),
        ((WIDTH, 2 * PAIR * FF), BF),
        ((WIDTH, 2 * FF), BF),
        ((FF, WIDTH), BF),
        ((HEAD, WIDTH), BF),
        ((WIDE, WIDE), BF),
        ((NX, SEQ, 512), BF),
        ((NX, SEQ, 512), BF),
        ((NX, SEQ, 512), BF),
        ((NX, SEQ, 512), BF),
        ((SEQ, WIDTH), BF),
        ((NT, SEQ, WIDE), BF),
        ((NE, TILE, 128), BF),
        ((NT * TILE, 128), BF),
        ((NT, TILE, 128), BF),
        ((NT, TILE, 128), BF),
        ((NT, TILE, 128), BF),
        ((NT * TILE, NT * TILE), BF),
        ((NT * TILE, NT * TILE), BF),
        ((NT * SEQ, NT * SEQ), BF),
        ((NT * SEQ, WIDE), BF),
        ((SEQ, WIDTH), F32),
        ((SEQ, WIDTH), BF),
        ((NE, PAD, WIDE), BF),
        ((NE, PAD, WIDE), BF),
        ((PAIR * SLOTS, WIDTH), BF),
        ((PAIR * SLOTS, WIDTH), BF),
        ((ROWS, WIDTH), BF),
        ((NT, ROWS, WIDE), BF),
        ((PAIR * SLOTS, NT * FF), BF),
        ((SEQ, WIDTH), BF),
        ((NT, SEQ, WIDE), BF),
        ((NZ, NX, SEQ, WIDE), BF),
        ((NX, NZ, SEQ, WIDE), BF),
        ((NZ, SEQ, WIDE), BF),
        ((NZ, SEQ, WIDE), BF),
        ((NE, PAD, WIDE), BF),
        ((NE, PAD, WIDE), BF),
        ((SEQ, HEAD), F32),
        ((SEQ, PADDED), F32),
        ((PADDED, SEQ), BF),
        ((PAIR * SLOTS, PADDED), BF),
        ((PADDED, PAIR * SLOTS), BF),
        ((SEQ, WIDE), F32),
    ]
    result, held = pl.pallas_call(
        layer,
        out_shape=[
            pltpu.VMEM((SEQ, WIDE), F32),
            pltpu.VMEM((SEQ, 1, HEAD, HEAD), F32),
        ],
        in_specs=[vmem if i in small else hbm for i in range(len(args))],
        out_specs=[vmem, vmem],
        scratch_shapes=[pltpu.VMEM(shape, kind) for shape, kind in scratch]
        + [
            pltpu.SemaphoreType.DMA((SENDS,)),
            pltpu.SemaphoreType.DMA((ARRIVALS,)),
            pltpu.SemaphoreType.DMA((LOCALS,)),
        ],
        compiler_params=pltpu.CompilerParams(collective_id=0, has_side_effects=True),
        name="layer",
    )(*args)
    return pl.pallas_call(
        closing,
        out_shape=[
            jax.ShapeDtypeStruct((SEQ, WIDE), BF),
            jax.ShapeDtypeStruct((SEQ, 1, HEAD, HEAD), F32),
        ],
        in_specs=[vmem, hbm],
        out_specs=[vmem, hbm],
        scratch_shapes=[pltpu.SemaphoreType.DMA(())],
        name="closing",
    )(pltpu.with_memory_space_constraint(result, pltpu.VMEM), pltpu.with_memory_space_constraint(held, pltpu.VMEM))


def solution(mesh):
    torus = Mesh(mesh.devices.reshape(NZ, NX, NY, NC), ("z", "x", "y", "c"))
    return jax.shard_map(
        local,
        mesh=torus,
        in_specs=(
            P(EP, None),
            P(EP, TP, None, None),
            P(),
            P(EP, TP),
            P(EP, TP),
            P(EP, TP),
            P(EP, TP),
            P(TP),
            P(TP),
            P(TP, None),
            P(),
            P(EP, None),
            P(EP, None),
            P(EP, None, TP),
            P(EP, None, TP),
            P(EP, TP, None),
            P(None, TP),
            P(None, TP),
            P(TP, None),
            P(TP, EP),
            P(TP, EP),
            P(EP, TP),
            P(TP),
        ),
        out_specs=(P(EP, TP), P(EP, TP, None, None)),
        check_vma=False,
    )
```

```python
import jax
import jax.numpy as jnp
from jax import lax
from jax.experimental import pallas as pl
from jax.experimental.pallas import tpu as pltpu
from jax.sharding import Mesh
from jax.sharding import PartitionSpec as P

EP = ("z", "x")
TP = ("y", "c")
NZ, NX, NY, NC = 8, 4, 4, 2
NE, NT = NZ * NX, NY * NC
MESH = pl.DeviceIdType.MESH
EPS = 1e-06
SEQ, WIDTH, HEAD, WIDE, TOPK = 48, 2048, 128, 256, 4
PAIR, CAP = 2, 6
SLOTS, BOTH = NE * CAP, PAIR * CAP
LINES = NE * 2 * BOTH
ROWS = SEQ * NE // NT
FF = 128
OWN = SEQ // NT
TILE = OWN * WIDTH // 128

BF, F32 = jnp.bfloat16, jnp.float32
Z_ORDER = (1, 7, 2, 6, 3, 5, 4)
Y_ORDER = (1, 3, 2)
X_ORDER = (1, 3, 2)
FAR_ORDER = (4, 3, 5, 2, 6, 1, 7, 0)
SENDS, ARRIVALS, LOCALS = 18, 67, 19
scope = jax.named_scope


def cols_at(ref, index, width):
    start = pl.multiple_of(index * width, width)
    return ref.at[(slice(None),) * (len(ref.shape) - 1) + (pl.ds(start, width),)]


def dot(left, right):
    return jnp.dot(left, right, preferred_element_type=F32)


def iota(shape, dim):
    return lax.broadcasted_iota(jnp.int32, shape, dim)


def scaled(values, gain):
    values = values.astype(F32)
    return values * lax.rsqrt(jnp.mean(values * values, axis=-1, keepdims=True) + EPS) * gain


class Links:
    def __init__(self, send_sem, recv_sem, local_sem):
        self.send_sem, self.recv_sem, self.local_sem = send_sem, recv_sem, local_sem
        self.sent = self.received = self.locals = 0
        self.z, self.x = lax.axis_index("z"), lax.axis_index("x")
        self.y, self.c = lax.axis_index("y"), lax.axis_index("c")
        self.e = self.z * NX + self.x
        self.t = self.y * NC + self.c
        self.pending = []

    def load(self, src, dst):
        copy = pltpu.make_async_copy(src, dst, self.local_sem.at[self.locals])
        self.locals += 1
        copy.start()
        return copy

    def reserve(self, number):
        first = self.received
        self.received += number
        return first

    def new_send(self):
        self.sent += 1
        return self.sent - 1

    def copy(self, src, dst, sent, slot, **device):
        return pltpu.make_async_remote_copy(
            src_ref=src,
            dst_ref=dst,
            send_sem=self.send_sem.at[sent],
            recv_sem=self.recv_sem.at[slot],
            device_id=device,
            device_id_type=MESH,
        )

    def stage(self, total):
        sent = self.new_send()
        self.pending.append(self.copy(total, total, sent, 0, c=1 - self.c))

        def send(src, dst, slot, **device):
            self.copy(src, dst, sent, slot, **device).start()

        return send

    def wait(self, dst, slot):
        self.copy(dst, dst, 0, slot, c=1 - self.c).wait_recv()

    def finish(self):
        for copy in self.pending:
            copy.wait_send()
        assert (self.sent, self.received, self.locals) == (SENDS, ARRIVALS, LOCALS)

    def greet(self):
        barrier = pltpu.get_barrier_semaphore()
        peers = []
        for dz in range(NZ):
            for dx in range(NX):
                if dz or dx:
                    peers.append(dict(z=(self.z + dz) % NZ, x=(self.x + dx) % NX))
        for dy in range(NY):
            for dc in range(NC):
                if dy or dc:
                    peers.append(dict(y=(self.y + dy) % NY, c=(self.c + dc) % NC))
        for peer in peers:
            pl.semaphore_signal(barrier, inc=1, device_id=peer, device_id_type=MESH)
        return lambda: pl.semaphore_wait(barrier, len(peers))

    def gather_tp(self, view, seven):
        base = self.reserve(10)
        send = self.stage(seven)
        up, down = (self.y + 1) % NY, (self.y + NY - 1) % NY
        far = (self.y + 2) % NY

        def half(y, i):
            block = view(y * NC + self.c)
            size = block.shape[0] // 2
            return block.at[(pl.ds(i * size, size),) + (slice(None),) * (len(block.shape) - 1)]

        for i in range(2):
            send(half(self.y, i), half(self.y, i), base + i, y=up)
            send(half(self.y, 1 - i), half(self.y, 1 - i), base + 2 + i, y=down)
        mine = view(self.t)
        send(mine, mine, base + 6, c=1 - self.c)

        def onward():
            self.wait(half(down, 0), base)
            send(half(down, 0), half(down, 0), base + 4, y=up)
            self.wait(half(up, 1), base + 2)
            send(half(up, 1), half(up, 1), base + 5, y=down)

        def relay():
            self.wait(half(down, 1), base + 1)
            block = view(down * NC + self.c)
            send(block, block, base + 7, c=1 - self.c)
            self.wait(half(up, 0), base + 3)
            block = view(up * NC + self.c)
            send(block, block, base + 8, c=1 - self.c)
            self.wait(half(far, 0), base + 4)
            self.wait(half(far, 1), base + 5)
            block = view(far * NC + self.c)
            send(block, block, base + 9, c=1 - self.c)

        def rest(only=range(4)):
            for i in only:
                self.wait(view((self.y, down, up, far)[i] * NC + 1 - self.c), base + 6 + i)

        return onward, relay, rest

    def swap_tp(self, src_view, dst_view, seven):
        base = self.reserve(1)
        send = self.stage(seven)
        mine = dst_view(self.t)
        for dy in Y_ORDER + (0,):
            for dc in range(NC):
                if dy or dc:
                    y, c = (self.y + dy) % NY, (self.c + dc) % NC
                    send(src_view(y * NC + c), mine, base, y=y, c=c)
        return lambda: self.wait(seven, base)

    def swap_ep(self, src, dst):
        slot, sent = self.reserve(1), self.new_send()
        for dz in (4, 3, 5, 2, 6, 1, 7, 0):
            for dx in (2, 1, 3, 0):
                if dz or dx:
                    z, x = (self.z + dz) % NZ, (self.x + dx) % NX
                    self.copy(src.at[z * NX + x], dst.at[self.e], sent, slot, z=z, x=x).start()
        self.pending.append(self.copy(src.at[pl.ds(0, NE - 1)], dst.at[pl.ds(0, NE - 1)], sent, slot, c=1 - self.c))
        return lambda: self.wait(dst.at[pl.ds(0, NE - 1)], slot)


def layer(
    tokens,
    state,
    norm_gain,
    w_query,
    w_forget,
    w_input,
    w_outgate,
    lower_bound,
    head_gain,
    w_output,
    ffn_gain,
    route_ids,
    route_weight,
    expert_gate,
    expert_up,
    expert_down,
    shared_gate,
    shared_up,
    shared_down,
    dense_gate,
    dense_up,
    dense_down,
    dense_mix,
    mixed,
    held,
    tok,
    wz,
    dense_w,
    down_own,
    down_all,
    gates,
    expert_w,
    shared_w,
    shared_d,
    out_w,
    dense_d,
    tok_out,
    tok_in,
    part_out,
    part_in,
    head_part,
    head_in,
    rows,
    flat,
    tok_rows,
    row_out,
    row_in,
    pack,
    unpack,
    order,
    regroup,
    dense_raw,
    resid_rows,
    slot_out,
    slot_in,
    chosen,
    chosen_in,
    dense_in,
    dense_hidden,
    hidden,
    shared_part,
    shared_in,
    sum_out,
    sum_in,
    sum2_out,
    sum2_in,
    back_out,
    back_in,
    readout,
    combine,
    dispatch,
    squeeze,
    expand,
    second,
    resid,
    send_sem,
    recv_sem,
    local_sem,
):
    n = Links(send_sem, recv_sem, local_sem)
    met = n.greet()
    own_down = cols_at(expert_down, n.t, WIDE)
    load_tok = n.load(tokens, tok)
    load_w = [
        n.load(w, wz.at[n.z, :, pl.ds(i * HEAD, HEAD)])
        for i, w in enumerate((w_query, w_forget, w_input, w_outgate))
    ]
    load_dense = [
        n.load(w, dense_w.at[n.t, :, pl.ds(i * WIDE, WIDE)]) for i, w in enumerate((dense_gate, dense_up))
    ]
    load_down = n.load(expert_down, down_own)
    load_mine = n.load(own_down, down_all.at[:, n.t])
    load_state = n.load(state, held)
    load_out = n.load(w_output, out_w)
    load_shared = [
        n.load(shared_gate, shared_w.at[:, pl.ds(0, FF)]),
        n.load(shared_up, shared_w.at[:, pl.ds(FF, FF)]),
        n.load(shared_down, shared_d),
    ]
    load_expert = [
        n.load(w.at[j], expert_w.at[:, pl.ds((2 * j + i) * FF, FF)])
        for j in range(PAIR)
        for i, w in enumerate((expert_gate, expert_up))
    ]
    load_dense_d = n.load(dense_down, dense_d)

    load_tok.wait()
    normed = scaled(tok[...], norm_gain[...]).astype(BF)
    for x in range(NX):
        for z in range(NZ):
            start = (z * NX + x) * 64
            tok_out[x, :, z * 64 : (z + 1) * 64] = normed[:, start : start + 64]
    tok_in[pl.ds(n.x, 1)] = tok_out[pl.ds(n.x, 1)]

    met()
    for copy in load_w:
        copy.wait()
    base_w = n.reserve(7)
    send_w = n.stage(wz.at[pl.ds(0, 7)])
    z_at = [(n.z + dz) % NZ for dz in range(NZ)]
    for dz, slot in ((2, 0), (6, 1), (1, 2), (7, 2)):
        send_w(wz.at[n.z], wz.at[n.z], base_w + slot, z=z_at[dz])
    base_t = n.reserve(1)
    send_t = n.stage(tok_in.at[pl.ds(0, 3)])
    for dx in X_ORDER:
        x = (n.x + dx) % NX
        send_t(tok_out.at[x], tok_in.at[n.x], base_t, x=x)
    for copy in load_dense:
        copy.wait()
    dense_onward, dense_relay, dense_rest = n.gather_tp(
        lambda t: dense_w.at[t], dense_w.at[pl.ds(0, 7)]
    )

    with scope("routes"):
        expert_row = iota((128, SEQ), 0)
        named = [route_ids[k : k + 1, :] for k in range(TOPK)]
        equal = [(expert_row == ids).astype(F32) for ids in named]
        earlier = (iota((SEQ, SEQ), 0) < iota((SEQ, SEQ), 1)).astype(BF)
        rank = dot(sum(equal).astype(BF), earlier)
        line = iota((LINES, SEQ), 0).astype(F32)
        halves = [jnp.zeros((LINES, SEQ), F32) for _ in range(2)]
        picked = jnp.zeros((LINES, SEQ), F32)
        for k in range(TOPK):
            ids = named[k]
            first = (ids // PAIR) * (2 * BOTH) + (ids % PAIR) * CAP
            place = first.astype(F32) + jnp.sum(equal[k] * rank, axis=0, keepdims=True)
            for h in range(2):
                here = line == place + h * BOTH
                halves[h] = halves[h] + jnp.where(here, route_weight[k : k + 1, :], 0.0)
                picked = picked + here.astype(F32)
        dispatch[...] = picked.astype(BF)
        for h in range(2):
            combine[h, :, :] = halves[h].T

    def row_of(place):
        inside = place % BOTH
        return (inside // CAP) * SLOTS + (place // (2 * BOTH)) * CAP + inside % CAP

    def is_second(place):
        return (place // BOTH) % 2

    across, along = iota((1, LINES), 1), iota((LINES, 1), 0)
    row = iota((PAIR * SLOTS, LINES), 0)
    for h in range(2):
        target = jnp.where(is_second(across) == h, row_of(across), -1)
        squeeze[h, :, :] = (row == target).astype(F32).astype(BF)
    expand[...] = (iota((LINES, PAIR * SLOTS), 1) == row_of(along)).astype(F32).astype(BF)
    second[...] = jnp.broadcast_to(is_second(along), (LINES, 128)).astype(F32)

    def in_lines(values):
        return jnp.where(second[...] > 0.5, values[:, 128:], values[:, :128]).astype(BF).reshape(NE, 2 * BOTH, 128)

    def packed_row(row):
        inside = row % SEQ
        return (inside // OWN) * TILE + (row // SEQ) * OWN + inside % OWN

    def ordered_row(row):
        inside = row % SEQ
        return (inside // OWN) * SEQ + (row // SEQ) * OWN + inside % OWN

    def regrouped_row(row):
        e = row // OWN
        return (e % NX) * SEQ + (e // NX) * OWN + row % OWN

    many, few = NT * TILE, NT * SEQ
    pack[...] = (iota((many, many), 0) == packed_row(iota((1, many), 1))).astype(F32).astype(BF)
    unpack[...] = (iota((many, many), 1) == packed_row(iota((many, 1), 0))).astype(F32).astype(BF)
    order[...] = (iota((few, few), 0) == ordered_row(iota((1, few), 1))).astype(F32).astype(BF)
    regroup[...] = (iota((ROWS, ROWS), 0) == regrouped_row(iota((1, ROWS), 1))).astype(F32).astype(BF)
    for k in range(WIDTH // 128):
        flat[k * SEQ : (k + 1) * SEQ, :] = tok[:, k * 128 : (k + 1) * 128]
    tok_rows[...] = dot(pack[...], flat[...]).astype(BF).reshape(NT, TILE, 128)

    for source, near, far, row, slot in ((6, 1, 2, 0, 0), (2, 7, 6, 32, 1)):
        block = wz.at[z_at[source]]
        n.wait(block, base_w + slot)
        send_w(block, block, base_w + 3 + slot, z=z_at[near])
        block = wz.at[z_at[source], pl.ds(row, 32)]
        send_w(block, block, base_w + 5 + slot, z=z_at[far])
    dense_onward()
    load_down.wait()
    down_rest = [
        n.swap_tp(lambda t: cols_at(down_own.at[0], t, WIDE), lambda t: down_all.at[0, t], down_all.at[0, pl.ds(0, 7)])
    ]
    n.wait(tok_in.at[pl.ds(0, 3)], base_t)
    n.wait(wz.at[pl.ds(0, 2)], base_w + 2)
    for slot in range(2):
        n.wait(wz.at[0], base_w + 3 + slot)
        n.wait(wz.at[0, pl.ds(0, 32)], base_w + 5 + slot)
    part = dot(tok_in[...].reshape(NX * SEQ, 512), wz[...].reshape(512, 512))
    part_out[...] = part.astype(BF).reshape(NX, SEQ, 512)
    base_p = n.reserve(1)
    send_p = n.stage(part_in.at[pl.ds(0, 3)])
    for dx in X_ORDER:
        x = (n.x + dx) % NX
        send_p(part_out.at[x], part_in.at[n.x], base_p, x=x)
    part_in[pl.ds(n.x, 1)] = part_out[pl.ds(n.x, 1)]
    n.wait(part_in.at[pl.ds(0, 3)], base_p)
    projected = part_in[0].astype(F32)
    for x in range(1, NX):
        projected = projected + part_in[x].astype(F32)
    projected = projected.astype(BF).astype(F32)
    query, forget_pre = projected[:, :HEAD], projected[:, HEAD : 2 * HEAD]
    values, out_gate = projected[:, 2 * HEAD : 3 * HEAD], projected[:, 3 * HEAD :]
    low = lower_bound[...]
    forget_sig = jax.nn.sigmoid(forget_pre)
    decay = low + (1.0 - low) * forget_sig
    keygate = (1.0 - low) * (1.0 - forget_sig)
    mixed_q = (query * decay).T
    gates[0, :, :], gates[1, :, :], gates[2, :, :] = decay, keygate, values
    load_state.wait()
    for b in range(SEQ):
        readout[b : b + 1, :] = jnp.sum(mixed_q[:, b : b + 1] * held[b, 0], axis=0, keepdims=True)
    read = readout[...] + jnp.sum(query * keygate, axis=1, keepdims=True) * values
    read = read * lax.rsqrt(jnp.mean(read * read, axis=-1, keepdims=True) + EPS)
    head_out = (read * head_gain[...] * jax.nn.silu(out_gate)).astype(BF)
    load_out.wait()
    whole = dot(head_out, out_w[...]).astype(BF)
    for k in range(WIDTH // 128):
        flat[k * SEQ : (k + 1) * SEQ, :] = whole[:, k * 128 : (k + 1) * 128]
    row_out[...] = dot(pack[...], flat[...]).astype(BF).reshape(NT, TILE, 128)
    row_rest = n.swap_tp(lambda t: row_out.at[t], lambda t: row_in.at[t], row_in.at[pl.ds(0, 7)])
    head_part[...] = whole
    head_rest = n.swap_tp(lambda t: cols_at(head_part, t, WIDE), lambda t: head_in.at[t], head_in.at[pl.ds(0, 7)])
    row_in[pl.ds(n.t, 1)] = row_out[pl.ds(n.t, 1)]
    head_in[pl.ds(n.t, 1)] = cols_at(head_part, n.t, WIDE)[...][None]
    row_rest()
    own = tok_rows[pl.ds(n.t, 1)][0].astype(F32)
    for t in range(NT):
        own = own + row_in[t].astype(F32)
    rows[pl.ds(n.e, 1)] = own.astype(BF)[None]

    base_c = n.reserve(NZ)
    send_c = n.stage(rows.at[pl.ds(0, NE - 1)])
    mine = rows.at[n.e]
    for i, dz in enumerate(Z_ORDER):
        send_c(mine, mine, base_c + i, z=z_at[dz])
    for dx in X_ORDER:
        send_c(mine, mine, base_c + 7, x=(n.x + dx) % NX)
    head_rest()
    own = cols_at(tok, n.t, WIDE)[...].astype(F32)
    for t in range(NT):
        own = own + head_in[t].astype(F32)
    resid[...] = own
    own_cols = own.astype(BF)
    slot_out[...] = in_lines(dot(dispatch[...], own_cols))
    slots_rest = n.swap_ep(slot_out, slot_in)
    slot_in[pl.ds(n.e, 1)] = slot_out[pl.ds(n.e, 1)]
    cols_at(resid_rows, n.t, WIDE)[...] = own_cols
    rows_mine = cols_at(resid_rows, n.t, WIDE)
    rows_seven = resid_rows.at[:, pl.ds(0, 7 * WIDE)]
    rows_rest = n.swap_tp(lambda t: rows_mine, lambda t: cols_at(resid_rows, t, WIDE), rows_seven)
    down_rest.append(
        n.swap_tp(lambda t: cols_at(down_own.at[1], t, WIDE), lambda t: down_all.at[1, t], down_all.at[1, pl.ds(0, 7)])
    )
    dense_relay()
    for i, dz in enumerate(Z_ORDER):
        e = z_at[(NZ - dz) % NZ] * NX + n.x
        n.wait(rows.at[e], base_c + i)
        for dx in X_ORDER:
            send_c(rows.at[e], rows.at[e], base_c + 7, x=(n.x + dx) % NX)

    gain = ffn_gain[...]
    rows_rest()
    for copy in load_shared:
        copy.wait()
    shared_x = scaled(resid_rows[...], gain).astype(BF)
    shared_pre = dot(shared_x, shared_w[...])
    shared_hidden = (jax.nn.silu(shared_pre[:, :FF]) * shared_pre[:, FF:]).astype(BF)
    shared_part[...] = dot(shared_hidden, shared_d[...]).astype(BF)
    shared_rest = n.swap_tp(lambda t: cols_at(shared_part, t, WIDE), lambda t: shared_in.at[t], shared_in.at[pl.ds(0, 7)])
    shared_in[pl.ds(n.t, 1)] = cols_at(shared_part, n.t, WIDE)[...][None]

    slots_rest()
    lines = slot_in[...].reshape(LINES, 128)
    picked_rows = jnp.concatenate([dot(squeeze[h], lines) for h in range(2)], axis=1)
    cols_at(chosen, n.t, WIDE)[...] = picked_rows.astype(BF)
    chosen_onward, chosen_relay, chosen_rest = n.gather_tp(
        lambda t: cols_at(chosen, t, WIDE), chosen.at[:, pl.ds(0, 7 * WIDE)]
    )

    n.wait(rows.at[pl.ds(0, 24)], base_c + 7)
    for g in range(NE // NT):
        group = dot(unpack[...], rows[g * NT : (g + 1) * NT].reshape(NT * TILE, 128))
        for k in range(WIDTH // 128):
            dense_raw[:, k * 128 : (k + 1) * 128] = group[k * SEQ : (k + 1) * SEQ, :]
        dense_in[g * SEQ : (g + 1) * SEQ, :] = scaled(dense_raw[...], gain).astype(BF)
    dense_rest()
    pre = dot(dense_in[...], dense_w[...].reshape(WIDTH, 2 * WIDE))
    dense_hidden[pl.ds(n.t, 1)] = (jax.nn.silu(pre[:, :WIDE]) * pre[:, WIDE:]).astype(BF)[None]
    chosen_onward()
    units_onward, units_relay, units_rest = n.gather_tp(
        lambda t: dense_hidden.at[t], dense_hidden.at[pl.ds(0, 7)]
    )

    load_dense_d.wait()
    scale = jax.nn.sigmoid(dense_mix[...])
    base_x = n.reserve(1)
    send_x = n.stage(sum_in.at[pl.ds(0, 3)])

    def emit(dy, same):
        t = ((n.y + dy) % NY) * NC + (n.c if same else 1 - n.c)
        inner = dot(regroup[...], dense_hidden[pl.ds(t, 1)][0]).astype(BF)
        block = dot(inner, dense_d[...]) * scale
        sum_out[pl.ds(t, 1)] = block.astype(BF).reshape(1, NX, SEQ, WIDE)
        for dx in X_ORDER:
            x = (n.x + dx) % NX
            send_x(sum_out.at[t, x], sum_in.at[n.x, t], base_x, x=x)

    emit(0, True)

    decay, keygate = gates[0].T, gates[1].T
    for b in range(SEQ):
        held[b, 0] = decay[:, b : b + 1] * held[b, 0] + keygate[:, b : b + 1] * gates[2, b : b + 1, :]

    units_rest([0])
    emit(0, False)
    chosen_relay()
    units_onward()
    chosen_rest()
    for copy in load_expert:
        copy.wait()
    for j in range(PAIR):
        for i in range(4):
            part = pl.ds(j * SLOTS + i * SEQ, SEQ)
            chosen_in[part] = scaled(chosen[part], gain).astype(BF)
        pre = dot(chosen_in[pl.ds(j * SLOTS, SLOTS)], expert_w[:, 2 * j * FF : 2 * (j + 1) * FF])
        unit = (jax.nn.silu(pre[:, :FF]) * pre[:, FF:]).astype(BF)
        cols_at(hidden, n.t, FF).at[pl.ds(j * SLOTS, SLOTS)][...] = unit
    hidden_onward, hidden_relay, hidden_rest = n.gather_tp(
        lambda t: cols_at(hidden, t, FF), hidden.at[:, pl.ds(0, 7 * FF)]
    )

    units_relay()
    for dy in (3, 1, 2):
        emit(dy, True)
    hidden_onward()
    for i, dy in ((1, 3), (2, 1), (3, 2)):
        units_rest([i])
        emit(dy, False)

    hidden_relay()
    for rest in down_rest:
        rest()
    load_mine.wait()
    hidden_rest()
    outs = [
        dot(hidden[pl.ds(j * SLOTS, SLOTS)], down_all[j].reshape(NT * FF, WIDE)).astype(BF) for j in range(PAIR)
    ]
    spread = dot(expand[:, :SLOTS], outs[0]) + dot(expand[:, SLOTS:], outs[1])
    back_out[...] = in_lines(spread)
    back_rest = n.swap_ep(back_out, back_in)
    back_in[pl.ds(n.e, 1)] = back_out[pl.ds(n.e, 1)]

    n.wait(sum_in.at[pl.ds(0, 3)], base_x)
    block = sum_out[:, pl.ds(n.x, 1)].reshape(NT * SEQ, WIDE).astype(F32)
    for dx in X_ORDER:
        block = block + sum_in[pl.ds((n.x + dx) % NX, 1)].reshape(NT * SEQ, WIDE).astype(F32)
    sum2_out[...] = dot(order[...], block.astype(BF)).astype(BF).reshape(NZ, SEQ, WIDE)
    base_z = n.reserve(1)
    send_z = n.stage(sum2_in.at[pl.ds(0, 7)])
    for dz in FAR_ORDER[:-1]:
        send_z(sum2_out.at[z_at[dz]], sum2_in.at[n.z], base_z, z=z_at[dz])
    sum2_in[pl.ds(n.z, 1)] = sum2_out[pl.ds(n.z, 1)]
    back_rest()
    shared_rest()
    lines = back_in[...].reshape(LINES, 128).astype(F32)
    routed = [
        jnp.dot(combine[h], lines, preferred_element_type=F32, precision=lax.Precision.HIGHEST) for h in range(2)
    ]
    result = resid[...] + jnp.concatenate(routed, axis=1)
    for t in range(NT):
        result = result + shared_in[t].astype(F32)
    n.wait(sum2_in.at[pl.ds(0, 7)], base_z)
    for z in range(NZ):
        result = result + sum2_in[z].astype(F32)
    mixed[...] = result
    n.finish()


def closing(result, held, mixed, new_state, sem):
    copy = pltpu.make_async_copy(held, new_state, sem)
    copy.start()
    mixed[...] = result[...].astype(BF)
    copy.wait()


def local(*args):
    args = list(args)
    for i in (2, 7, 8, 10, 22):
        args[i] = args[i].reshape(1, -1)
    for i in (11, 12):
        args[i] = args[i].T
    vmem = pl.BlockSpec(memory_space=pltpu.VMEM)
    hbm = pl.BlockSpec(memory_space=pl.ANY)
    small = (2, 7, 8, 10, 11, 12, 22)
    scratch = [
        ((SEQ, WIDTH), BF),
        ((NZ, 64, 512), BF),
        ((NT, WIDE, 2 * WIDE), BF),
        ((PAIR, FF, WIDTH), BF),
        ((PAIR, NT, FF, WIDE), BF),
        ((3, SEQ, HEAD), F32),
        ((WIDTH, 2 * PAIR * FF), BF),
        ((WIDTH, 2 * FF), BF),
        ((FF, WIDTH), BF),
        ((HEAD, WIDTH), BF),
        ((WIDE, WIDE), BF),
        ((NX, SEQ, 512), BF),
        ((NX, SEQ, 512), BF),
        ((NX, SEQ, 512), BF),
        ((NX, SEQ, 512), BF),
        ((SEQ, WIDTH), BF),
        ((NT, SEQ, WIDE), BF),
        ((NE, TILE, 128), BF),
        ((NT * TILE, 128), BF),
        ((NT, TILE, 128), BF),
        ((NT, TILE, 128), BF),
        ((NT, TILE, 128), BF),
        ((NT * TILE, NT * TILE), BF),
        ((NT * TILE, NT * TILE), BF),
        ((NT * SEQ, NT * SEQ), BF),
        ((ROWS, ROWS), BF),
        ((SEQ, WIDTH), F32),
        ((SEQ, WIDTH), BF),
        ((NE, 2 * BOTH, 128), BF),
        ((NE, 2 * BOTH, 128), BF),
        ((PAIR * SLOTS, WIDTH), BF),
        ((PAIR * SLOTS, WIDTH), BF),
        ((ROWS, WIDTH), BF),
        ((NT, ROWS, WIDE), BF),
        ((PAIR * SLOTS, NT * FF), BF),
        ((SEQ, WIDTH), BF),
        ((NT, SEQ, WIDE), BF),
        ((NT, NX, SEQ, WIDE), BF),
        ((NX, NT, SEQ, WIDE), BF),
        ((NZ, SEQ, WIDE), BF),
        ((NZ, SEQ, WIDE), BF),
        ((NE, 2 * BOTH, 128), BF),
        ((NE, 2 * BOTH, 128), BF),
        ((SEQ, HEAD), F32),
        ((2, SEQ, LINES), F32),
        ((LINES, SEQ), BF),
        ((2, PAIR * SLOTS, LINES), BF),
        ((LINES, PAIR * SLOTS), BF),
        ((LINES, 128), F32),
        ((SEQ, WIDE), F32),
    ]
    result, held = pl.pallas_call(
        layer,
        out_shape=[
            pltpu.VMEM((SEQ, WIDE), F32),
            pltpu.VMEM((SEQ, 1, HEAD, HEAD), F32),
        ],
        in_specs=[vmem if i in small else hbm for i in range(len(args))],
        out_specs=[vmem, vmem],
        scratch_shapes=[pltpu.VMEM(shape, kind) for shape, kind in scratch]
        + [
            pltpu.SemaphoreType.DMA((SENDS,)),
            pltpu.SemaphoreType.DMA((ARRIVALS,)),
            pltpu.SemaphoreType.DMA((LOCALS,)),
        ],
        compiler_params=pltpu.CompilerParams(collective_id=0, has_side_effects=True),
        name="layer",
    )(*args)
    return pl.pallas_call(
        closing,
        out_shape=[
            jax.ShapeDtypeStruct((SEQ, WIDE), BF),
            jax.ShapeDtypeStruct((SEQ, 1, HEAD, HEAD), F32),
        ],
        in_specs=[vmem, hbm],
        out_specs=[vmem, hbm],
        scratch_shapes=[pltpu.SemaphoreType.DMA(())],
        name="closing",
    )(pltpu.with_memory_space_constraint(result, pltpu.VMEM), pltpu.with_memory_space_constraint(held, pltpu.VMEM))


def solution(mesh):
    torus = Mesh(mesh.devices.reshape(NZ, NX, NY, NC), ("z", "x", "y", "c"))
    return jax.shard_map(
        local,
        mesh=torus,
        in_specs=(
            P(EP, None),
            P(EP, TP, None, None),
            P(),
            P(EP, TP),
            P(EP, TP),
            P(EP, TP),
            P(EP, TP),
            P(TP),
            P(TP),
            P(TP, None),
            P(),
            P(EP, None),
            P(EP, None),
            P(EP, None, TP),
            P(EP, None, TP),
            P(EP, TP, None),
            P(None, TP),
            P(None, TP),
            P(TP, None),
            P(TP, EP),
            P(TP, EP),
            P(EP, TP),
            P(TP),
        ),
        out_specs=(P(EP, TP), P(EP, TP, None, None)),
        check_vma=False,
    )
```

```python
import jax
import jax.numpy as jnp
from jax import lax
from jax.experimental import pallas as pl
from jax.experimental.pallas import tpu as pltpu
from jax.sharding import Mesh
from jax.sharding import PartitionSpec as P

EP = ("z", "x")
TP = ("y", "c")
NZ, NX, NY, NC = 8, 4, 4, 2
NE, NT = NZ * NX, NY * NC
MESH = pl.DeviceIdType.MESH
EPS = 1e-06
SEQ, WIDTH, HEAD, WIDE, TOPK = 48, 2048, 128, 256, 4
PAIR, CAP = 2, 6
SLOTS, BOTH = NE * CAP, PAIR * CAP
LINES = NE * 2 * BOTH
ROWS = SEQ * NE // NT
FF = 128
OWN = SEQ // NT
TILE = OWN * WIDTH // 128

BF, F32 = jnp.bfloat16, jnp.float32
Z_ORDER = (1, 7, 2, 6, 3, 5, 4)
Y_ORDER = (1, 3, 2)
X_ORDER = (1, 3, 2)
FAR_ORDER = (4, 3, 5, 2, 6, 1, 7, 0)
SENDS, ARRIVALS, LOCALS = 21, 70, 19
scope = jax.named_scope


def cols_at(ref, index, width):
    start = pl.multiple_of(index * width, width)
    return ref.at[(slice(None),) * (len(ref.shape) - 1) + (pl.ds(start, width),)]


def dot(left, right):
    return jnp.dot(left, right, preferred_element_type=F32)


def iota(shape, dim):
    return lax.broadcasted_iota(jnp.int32, shape, dim)


def scaled(values, gain):
    values = values.astype(F32)
    return values * lax.rsqrt(jnp.mean(values * values, axis=-1, keepdims=True) + EPS) * gain


class Links:
    def __init__(self, send_sem, recv_sem, local_sem):
        self.send_sem, self.recv_sem, self.local_sem = send_sem, recv_sem, local_sem
        self.sent = self.received = self.locals = 0
        self.z, self.x = lax.axis_index("z"), lax.axis_index("x")
        self.y, self.c = lax.axis_index("y"), lax.axis_index("c")
        self.e = self.z * NX + self.x
        self.t = self.y * NC + self.c
        self.pending = []

    def load(self, src, dst):
        copy = pltpu.make_async_copy(src, dst, self.local_sem.at[self.locals])
        self.locals += 1
        copy.start()
        return copy

    def reserve(self, number):
        first = self.received
        self.received += number
        return first

    def new_send(self):
        self.sent += 1
        return self.sent - 1

    def copy(self, src, dst, sent, slot, **device):
        return pltpu.make_async_remote_copy(
            src_ref=src,
            dst_ref=dst,
            send_sem=self.send_sem.at[sent],
            recv_sem=self.recv_sem.at[slot],
            device_id=device,
            device_id_type=MESH,
        )

    def stage(self, total):
        sent = self.new_send()
        self.pending.append(self.copy(total, total, sent, 0, c=1 - self.c))

        def send(src, dst, slot, **device):
            self.copy(src, dst, sent, slot, **device).start()

        return send

    def wait(self, dst, slot):
        self.copy(dst, dst, 0, slot, c=1 - self.c).wait_recv()

    def finish(self):
        for copy in self.pending:
            copy.wait_send()
        assert (self.sent, self.received, self.locals) == (SENDS, ARRIVALS, LOCALS)

    def greet(self):
        barrier = pltpu.get_barrier_semaphore()
        peers = []
        for dz in range(NZ):
            for dx in range(NX):
                if dz or dx:
                    peers.append(dict(z=(self.z + dz) % NZ, x=(self.x + dx) % NX))
        for dy in range(NY):
            for dc in range(NC):
                if dy or dc:
                    peers.append(dict(y=(self.y + dy) % NY, c=(self.c + dc) % NC))
        for peer in peers:
            pl.semaphore_signal(barrier, inc=1, device_id=peer, device_id_type=MESH)
        return lambda: pl.semaphore_wait(barrier, len(peers))

    def gather_tp(self, view, seven):
        base = self.reserve(10)
        send = self.stage(seven)
        up, down = (self.y + 1) % NY, (self.y + NY - 1) % NY
        far = (self.y + 2) % NY

        def half(y, i):
            block = view(y * NC + self.c)
            size = block.shape[0] // 2
            return block.at[(pl.ds(i * size, size),) + (slice(None),) * (len(block.shape) - 1)]

        for i in range(2):
            send(half(self.y, i), half(self.y, i), base + i, y=up)
            send(half(self.y, 1 - i), half(self.y, 1 - i), base + 2 + i, y=down)
        mine = view(self.t)
        send(mine, mine, base + 6, c=1 - self.c)

        def onward():
            self.wait(half(down, 0), base)
            send(half(down, 0), half(down, 0), base + 4, y=up)
            self.wait(half(up, 1), base + 2)
            send(half(up, 1), half(up, 1), base + 5, y=down)

        def relay():
            self.wait(half(down, 1), base + 1)
            block = view(down * NC + self.c)
            send(block, block, base + 7, c=1 - self.c)
            self.wait(half(up, 0), base + 3)
            block = view(up * NC + self.c)
            send(block, block, base + 8, c=1 - self.c)
            self.wait(half(far, 0), base + 4)
            self.wait(half(far, 1), base + 5)
            block = view(far * NC + self.c)
            send(block, block, base + 9, c=1 - self.c)

        def rest(only=range(4)):
            for i in only:
                self.wait(view((self.y, down, up, far)[i] * NC + 1 - self.c), base + 6 + i)

        return onward, relay, rest

    def swap_tp(self, src_view, dst_view, seven):
        base = self.reserve(1)
        send = self.stage(seven)
        mine = dst_view(self.t)
        for dy in Y_ORDER + (0,):
            for dc in range(NC):
                if dy or dc:
                    y, c = (self.y + dy) % NY, (self.c + dc) % NC
                    send(src_view(y * NC + c), mine, base, y=y, c=c)
        return lambda: self.wait(seven, base)

    def swap_ep(self, src, dst):
        slot, sent = self.reserve(1), self.new_send()
        for dz in (4, 3, 5, 2, 6, 1, 7, 0):
            for dx in (2, 1, 3, 0):
                if dz or dx:
                    z, x = (self.z + dz) % NZ, (self.x + dx) % NX
                    self.copy(src.at[z * NX + x], dst.at[self.e], sent, slot, z=z, x=x).start()
        self.pending.append(self.copy(src.at[pl.ds(0, NE - 1)], dst.at[pl.ds(0, NE - 1)], sent, slot, c=1 - self.c))
        return lambda: self.wait(dst.at[pl.ds(0, NE - 1)], slot)


def layer(
    tokens,
    state,
    norm_gain,
    w_query,
    w_forget,
    w_input,
    w_outgate,
    lower_bound,
    head_gain,
    w_output,
    ffn_gain,
    route_ids,
    route_weight,
    expert_gate,
    expert_up,
    expert_down,
    shared_gate,
    shared_up,
    shared_down,
    dense_gate,
    dense_up,
    dense_down,
    dense_mix,
    mixed,
    held,
    tok,
    wz,
    dense_w,
    down_own,
    down_all,
    gates,
    expert_w,
    shared_w,
    shared_d,
    out_w,
    dense_d,
    tok_out,
    tok_in,
    part_out,
    part_in,
    head_part,
    head_in,
    rows,
    flat,
    tok_rows,
    row_out,
    row_in,
    pack,
    unpack,
    order,
    regroup,
    dense_raw,
    resid_rows,
    slot_out,
    slot_in,
    chosen,
    chosen_in,
    dense_in,
    hidden,
    shared_part,
    shared_in,
    sum_out,
    sum_in,
    sum2_out,
    sum2_in,
    swap_out,
    swap_in,
    pad_lines,
    take_lines,
    back_out,
    back_in,
    readout,
    combine,
    dispatch,
    squeeze,
    expand,
    second,
    resid,
    send_sem,
    recv_sem,
    local_sem,
):
    n = Links(send_sem, recv_sem, local_sem)
    met = n.greet()
    own_down = cols_at(expert_down, n.t, WIDE)
    load_tok = n.load(tokens, tok)
    load_w = [
        n.load(w, wz.at[n.z, :, pl.ds(i * HEAD, HEAD)])
        for i, w in enumerate((w_query, w_forget, w_input, w_outgate))
    ]
    load_dense = [
        n.load(w, dense_w.at[n.t, :, pl.ds(i * WIDE, WIDE)]) for i, w in enumerate((dense_gate, dense_up))
    ]
    load_down = n.load(expert_down, down_own)
    load_mine = n.load(own_down, down_all.at[:, n.t])
    load_state = n.load(state, held)
    load_out = n.load(w_output, out_w)
    load_shared = [
        n.load(shared_gate, shared_w.at[:, pl.ds(0, FF)]),
        n.load(shared_up, shared_w.at[:, pl.ds(FF, FF)]),
        n.load(shared_down, shared_d),
    ]
    load_expert = [
        n.load(w.at[j], expert_w.at[:, pl.ds((2 * j + i) * FF, FF)])
        for j in range(PAIR)
        for i, w in enumerate((expert_gate, expert_up))
    ]
    load_dense_d = n.load(dense_down, cols_at(dense_d, n.t, WIDE))

    load_tok.wait()
    normed = scaled(tok[...], norm_gain[...]).astype(BF)
    for x in range(NX):
        for z in range(NZ):
            start = (z * NX + x) * 64
            tok_out[x, :, z * 64 : (z + 1) * 64] = normed[:, start : start + 64]
    tok_in[pl.ds(n.x, 1)] = tok_out[pl.ds(n.x, 1)]

    met()
    for copy in load_w:
        copy.wait()
    base_w = n.reserve(7)
    send_w = n.stage(wz.at[pl.ds(0, 7)])
    z_at = [(n.z + dz) % NZ for dz in range(NZ)]
    for dz, slot in ((2, 0), (6, 1), (1, 2), (7, 2)):
        send_w(wz.at[n.z], wz.at[n.z], base_w + slot, z=z_at[dz])
    base_t = n.reserve(1)
    send_t = n.stage(tok_in.at[pl.ds(0, 3)])
    for dx in X_ORDER:
        x = (n.x + dx) % NX
        send_t(tok_out.at[x], tok_in.at[n.x], base_t, x=x)
    for copy in load_dense:
        copy.wait()
    dense_onward, dense_relay, dense_rest = n.gather_tp(
        lambda t: dense_w.at[t], dense_w.at[pl.ds(0, 7)]
    )
    load_dense_d.wait()
    last_onward, last_relay, last_rest = n.gather_tp(
        lambda t: cols_at(dense_d, t, WIDE), dense_d.at[:, pl.ds(0, 7 * WIDE)]
    )

    with scope("routes"):
        expert_row = iota((128, SEQ), 0)
        named = [route_ids[k : k + 1, :] for k in range(TOPK)]
        equal = [(expert_row == ids).astype(F32) for ids in named]
        earlier = (iota((SEQ, SEQ), 0) < iota((SEQ, SEQ), 1)).astype(BF)
        rank = dot(sum(equal).astype(BF), earlier)
        line = iota((LINES, SEQ), 0).astype(F32)
        halves = [jnp.zeros((LINES, SEQ), F32) for _ in range(2)]
        picked = jnp.zeros((LINES, SEQ), F32)
        for k in range(TOPK):
            ids = named[k]
            first = (ids // PAIR) * (2 * BOTH) + (ids % PAIR) * CAP
            place = first.astype(F32) + jnp.sum(equal[k] * rank, axis=0, keepdims=True)
            for h in range(2):
                here = line == place + h * BOTH
                halves[h] = halves[h] + jnp.where(here, route_weight[k : k + 1, :], 0.0)
                picked = picked + here.astype(F32)
        dispatch[...] = picked.astype(BF)
        for h in range(2):
            combine[h, :, :] = halves[h].T

    def row_of(place):
        inside = place % BOTH
        return (inside // CAP) * SLOTS + (place // (2 * BOTH)) * CAP + inside % CAP

    def is_second(place):
        return (place // BOTH) % 2

    across, along = iota((1, LINES), 1), iota((LINES, 1), 0)
    row = iota((PAIR * SLOTS, LINES), 0)
    for h in range(2):
        target = jnp.where(is_second(across) == h, row_of(across), -1)
        squeeze[h, :, :] = (row == target).astype(F32).astype(BF)
    expand[...] = (iota((LINES, PAIR * SLOTS), 1) == row_of(along)).astype(F32).astype(BF)
    second[...] = jnp.broadcast_to(is_second(along), (LINES, 128)).astype(F32)

    def in_lines(values):
        return jnp.where(second[...] > 0.5, values[:, 128:], values[:, :128]).astype(BF).reshape(NE, 2 * BOTH, 128)

    def packed_row(row):
        inside = row % SEQ
        return (inside // OWN) * TILE + (row // SEQ) * OWN + inside % OWN

    def ordered_row(row):
        inside = row % SEQ
        return (inside // OWN) * SEQ + (row // SEQ) * OWN + inside % OWN

    def regrouped_row(row):
        e = row // OWN
        return (e % NX) * SEQ + (e // NX) * OWN + row % OWN

    many, few = NT * TILE, NT * SEQ
    pack[...] = (iota((many, many), 0) == packed_row(iota((1, many), 1))).astype(F32).astype(BF)
    unpack[...] = (iota((many, many), 1) == packed_row(iota((many, 1), 0))).astype(F32).astype(BF)
    order[...] = (iota((few, few), 0) == ordered_row(iota((1, few), 1))).astype(F32).astype(BF)
    line = iota((1, TILE), 1)
    pad_lines[...] = (iota((NT * 16, TILE), 0) == (line // 12) * 16 + line % 12).astype(F32).astype(BF)
    token = iota((SEQ, 1), 0)
    for h in range(2):
        source = (token // OWN) * 16 + h * OWN + token % OWN
        take_lines[h, :, :] = (iota((SEQ, NT * 16), 1) == source).astype(F32).astype(BF)
    regroup[...] = (iota((ROWS, ROWS), 0) == regrouped_row(iota((1, ROWS), 1))).astype(F32).astype(BF)
    for k in range(WIDTH // 128):
        flat[k * SEQ : (k + 1) * SEQ, :] = tok[:, k * 128 : (k + 1) * 128]
    tok_rows[...] = dot(pack[...], flat[...]).astype(BF).reshape(NT, TILE, 128)

    for source, near, far, row, slot in ((6, 1, 2, 0, 0), (2, 7, 6, 32, 1)):
        block = wz.at[z_at[source]]
        n.wait(block, base_w + slot)
        send_w(block, block, base_w + 3 + slot, z=z_at[near])
        block = wz.at[z_at[source], pl.ds(row, 32)]
        send_w(block, block, base_w + 5 + slot, z=z_at[far])
    dense_onward()
    n.wait(tok_in.at[pl.ds(0, 3)], base_t)
    n.wait(wz.at[pl.ds(0, 2)], base_w + 2)
    for slot in range(2):
        n.wait(wz.at[0], base_w + 3 + slot)
        n.wait(wz.at[0, pl.ds(0, 32)], base_w + 5 + slot)
    part = dot(tok_in[...].reshape(NX * SEQ, 512), wz[...].reshape(512, 512))
    part_out[...] = part.astype(BF).reshape(NX, SEQ, 512)
    base_p = n.reserve(1)
    send_p = n.stage(part_in.at[pl.ds(0, 3)])
    for dx in X_ORDER:
        x = (n.x + dx) % NX
        send_p(part_out.at[x], part_in.at[n.x], base_p, x=x)
    part_in[pl.ds(n.x, 1)] = part_out[pl.ds(n.x, 1)]
    n.wait(part_in.at[pl.ds(0, 3)], base_p)
    projected = part_in[0].astype(F32)
    for x in range(1, NX):
        projected = projected + part_in[x].astype(F32)
    projected = projected.astype(BF).astype(F32)
    query, forget_pre = projected[:, :HEAD], projected[:, HEAD : 2 * HEAD]
    values, out_gate = projected[:, 2 * HEAD : 3 * HEAD], projected[:, 3 * HEAD :]
    low = lower_bound[...]
    forget_sig = jax.nn.sigmoid(forget_pre)
    decay = low + (1.0 - low) * forget_sig
    keygate = (1.0 - low) * (1.0 - forget_sig)
    mixed_q = (query * decay).T
    gates[0, :, :], gates[1, :, :], gates[2, :, :] = decay, keygate, values
    load_state.wait()
    for b in range(SEQ):
        readout[b : b + 1, :] = jnp.sum(mixed_q[:, b : b + 1] * held[b, 0], axis=0, keepdims=True)
    read = readout[...] + jnp.sum(query * keygate, axis=1, keepdims=True) * values
    read = read * lax.rsqrt(jnp.mean(read * read, axis=-1, keepdims=True) + EPS)
    head_out = (read * head_gain[...] * jax.nn.silu(out_gate)).astype(BF)
    load_out.wait()
    whole = dot(head_out, out_w[...]).astype(BF)
    head_part[...] = whole
    head_rest = n.swap_tp(lambda t: cols_at(head_part, t, WIDE), lambda t: head_in.at[t], head_in.at[pl.ds(0, 7)])
    for k in range(WIDTH // 128):
        flat[k * SEQ : (k + 1) * SEQ, :] = whole[:, k * 128 : (k + 1) * 128]
    row_out[...] = dot(pack[...], flat[...]).astype(BF).reshape(NT, TILE, 128)
    row_rest = n.swap_tp(lambda t: row_out.at[t], lambda t: row_in.at[t], row_in.at[pl.ds(0, 7)])
    row_in[pl.ds(n.t, 1)] = row_out[pl.ds(n.t, 1)]
    head_in[pl.ds(n.t, 1)] = cols_at(head_part, n.t, WIDE)[...][None]
    last_onward()
    head_rest()
    own = cols_at(tok, n.t, WIDE)[...].astype(F32)
    for t in range(NT):
        own = own + head_in[t].astype(F32)
    own_cols = own.astype(BF)
    slot_out[...] = in_lines(dot(dispatch[...], own_cols))
    slots_rest = n.swap_ep(slot_out, slot_in)
    slot_in[pl.ds(n.e, 1)] = slot_out[pl.ds(n.e, 1)]
    resid[...] = own

    row_rest()
    own = tok_rows[pl.ds(n.t, 1)][0].astype(F32)
    for t in range(NT):
        own = own + row_in[t].astype(F32)
    rows[pl.ds(n.e, 1)] = own.astype(BF)[None]
    base_c = n.reserve(NZ)
    send_c = n.stage(rows.at[pl.ds(0, NE - 1)])
    mine = rows.at[n.e]
    for i, dz in enumerate(Z_ORDER):
        send_c(mine, mine, base_c + i, z=z_at[dz])
    for dx in X_ORDER:
        send_c(mine, mine, base_c + 7, x=(n.x + dx) % NX)
    cols_at(resid_rows, n.t, WIDE)[...] = own_cols
    rows_mine = cols_at(resid_rows, n.t, WIDE)
    rows_seven = resid_rows.at[:, pl.ds(0, 7 * WIDE)]
    rows_rest = n.swap_tp(lambda t: rows_mine, lambda t: cols_at(resid_rows, t, WIDE), rows_seven)
    load_down.wait()

    def swap_down(j):
        here = down_all.at[j]
        return n.swap_tp(lambda t: cols_at(down_own.at[j], t, WIDE), lambda t: here.at[t], here.at[pl.ds(0, 7)])

    down_rest = [swap_down(0)]
    dense_relay()
    last_relay()

    def pass_on(order):
        for i in order:
            e = z_at[(NZ - Z_ORDER[i]) % NZ] * NX + n.x
            n.wait(rows.at[e], base_c + i)
            for dx in X_ORDER:
                send_c(rows.at[e], rows.at[e], base_c + 7, x=(n.x + dx) % NX)

    pass_on(range(2))

    slots_rest()
    lines = slot_in[...].reshape(LINES, 128)
    picked_rows = jnp.concatenate([dot(squeeze[h], lines) for h in range(2)], axis=1)
    cols_at(chosen, n.t, WIDE)[...] = picked_rows.astype(BF)
    chosen_onward, chosen_relay, chosen_rest = n.gather_tp(
        lambda t: cols_at(chosen, t, WIDE), chosen.at[:, pl.ds(0, 7 * WIDE)]
    )
    pass_on(range(2, 7))

    gain = ffn_gain[...]
    rows_rest()
    for copy in load_shared:
        copy.wait()
    shared_x = scaled(resid_rows[...], gain).astype(BF)
    shared_pre = dot(shared_x, shared_w[...])
    shared_hidden = (jax.nn.silu(shared_pre[:, :FF]) * shared_pre[:, FF:]).astype(BF)
    shared_part[...] = dot(shared_hidden, shared_d[...]).astype(BF)
    chosen_onward()
    down_rest.append(swap_down(1))

    n.wait(rows.at[pl.ds(0, 24)], base_c + 7)
    chosen_relay()
    for g in range(NE // NT):
        group = dot(unpack[...], rows[g * NT : (g + 1) * NT].reshape(NT * TILE, 128))
        for k in range(WIDTH // 128):
            dense_raw[:, k * 128 : (k + 1) * 128] = group[k * SEQ : (k + 1) * SEQ, :]
        dense_in[g * SEQ : (g + 1) * SEQ, :] = scaled(dense_raw[...], gain).astype(BF)
    dense_rest()
    pre = dot(dense_in[...], dense_w[...].reshape(WIDTH, 2 * WIDE))
    units = (jax.nn.silu(pre[:, :WIDE]) * pre[:, WIDE:]).astype(BF)
    inner = dot(regroup[...], units).astype(BF)
    last_rest()
    base_x = n.reserve(2)
    for h in range(2):
        block = dot(inner, dense_d[:, h * 1024 : (h + 1) * 1024])
        sum_out[h, :, :, :] = block.astype(BF).reshape(NX, SEQ, 1024)
        send_x = n.stage(sum_in.at[h, pl.ds(0, 3)])
        for dx in X_ORDER:
            x = (n.x + dx) % NX
            send_x(sum_out.at[h, x], sum_in.at[h, n.x], base_x + h, x=x)
    chosen_rest()
    for copy in load_expert:
        copy.wait()
    for j in range(PAIR):
        for i in range(4):
            part = pl.ds(j * SLOTS + i * SEQ, SEQ)
            chosen_in[part] = scaled(chosen[part], gain).astype(BF)
        pre = dot(chosen_in[pl.ds(j * SLOTS, SLOTS)], expert_w[:, 2 * j * FF : 2 * (j + 1) * FF])
        unit = (jax.nn.silu(pre[:, :FF]) * pre[:, FF:]).astype(BF)
        cols_at(hidden, n.t, FF).at[pl.ds(j * SLOTS, SLOTS)][...] = unit
    hidden_onward, hidden_relay, hidden_rest = n.gather_tp(
        lambda t: cols_at(hidden, t, FF), hidden.at[:, pl.ds(0, 7 * FF)]
    )

    decay, keygate = gates[0].T, gates[1].T
    for b in range(SEQ):
        held[b, 0] = decay[:, b : b + 1] * held[b, 0] + keygate[:, b : b + 1] * gates[2, b : b + 1, :]

    base_z = n.reserve(2)

    def sum_over_x(h):
        n.wait(sum_in.at[h, pl.ds(0, 3)], base_x + h)
        block = sum_out[h, pl.ds(n.x, 1)][0].astype(F32)
        for dx in X_ORDER:
            block = block + sum_in[h, pl.ds((n.x + dx) % NX, 1)][0].astype(F32)
        block = block.astype(BF)
        for k in range(8):
            flat[k * SEQ : (k + 1) * SEQ, :] = block[:, k * 128 : (k + 1) * 128]
        sum2_out[h, :, :, :] = dot(order[...], flat[: 8 * SEQ]).astype(BF).reshape(NZ, SEQ, 128)
        send_z = n.stage(sum2_in.at[h, pl.ds(0, 7)])
        for dz in FAR_ORDER[:-1]:
            send_z(sum2_out.at[h, z_at[dz]], sum2_in.at[h, n.z], base_z + h, z=z_at[dz])
        sum2_in[h, pl.ds(n.z, 1)] = sum2_out[h, pl.ds(n.z, 1)]

    hidden_onward()
    sum_over_x(0)
    hidden_relay()
    sum_over_x(1)

    shared_rest = n.swap_tp(lambda t: cols_at(shared_part, t, WIDE), lambda t: shared_in.at[t], shared_in.at[pl.ds(0, 7)])
    shared_in[pl.ds(n.t, 1)] = cols_at(shared_part, n.t, WIDE)[...][None]
    for rest in down_rest:
        rest()
    load_mine.wait()
    hidden_rest()
    outs = [
        dot(hidden[pl.ds(j * SLOTS, SLOTS)], down_all[j].reshape(NT * FF, WIDE)).astype(BF) for j in range(PAIR)
    ]
    spread = dot(expand[:, :SLOTS], outs[0]) + dot(expand[:, SLOTS:], outs[1])
    back_out[...] = in_lines(spread)
    back_rest = n.swap_ep(back_out, back_in)
    back_in[pl.ds(n.e, 1)] = back_out[pl.ds(n.e, 1)]

    own_lines = []
    for h in range(2):
        n.wait(sum2_in.at[h, pl.ds(0, 7)], base_z + h)
        acc = sum2_in[h, 0].astype(F32)
        for z in range(1, NZ):
            acc = acc + sum2_in[h, z].astype(F32)
        own_lines.append(acc)
    own_lines = jnp.concatenate(own_lines, axis=0).astype(BF)
    swap_out[...] = dot(pad_lines[...], own_lines).astype(BF).reshape(NT, 16, 128)
    swap_rest = n.swap_tp(lambda t: swap_out.at[t], lambda t: swap_in.at[t], swap_in.at[pl.ds(0, 7)])
    swap_in[pl.ds(n.t, 1)] = swap_out[pl.ds(n.t, 1)]
    back_rest()
    shared_rest()
    lines = back_in[...].reshape(LINES, 128).astype(F32)
    routed = [
        jnp.dot(combine[h], lines, preferred_element_type=F32, precision=lax.Precision.HIGHEST) for h in range(2)
    ]
    result = resid[...] + jnp.concatenate(routed, axis=1)
    for t in range(NT):
        result = result + shared_in[t].astype(F32)
    swap_rest()
    lines = swap_in[...].reshape(NT * 16, 128)
    dense_out = jnp.concatenate([dot(take_lines[h], lines) for h in range(2)], axis=1)
    result = result + dense_out * jax.nn.sigmoid(dense_mix[...])
    mixed[...] = result
    n.finish()


def closing(result, held, mixed, new_state, sem):
    copy = pltpu.make_async_copy(held, new_state, sem)
    copy.start()
    mixed[...] = result[...].astype(BF)
    copy.wait()


def local(*args):
    args = list(args)
    for i in (2, 7, 8, 10, 22):
        args[i] = args[i].reshape(1, -1)
    for i in (11, 12):
        args[i] = args[i].T
    vmem = pl.BlockSpec(memory_space=pltpu.VMEM)
    hbm = pl.BlockSpec(memory_space=pl.ANY)
    small = (2, 7, 8, 10, 11, 12, 22)
    scratch = [
        ((SEQ, WIDTH), BF),
        ((NZ, 64, 512), BF),
        ((NT, WIDE, 2 * WIDE), BF),
        ((PAIR, FF, WIDTH), BF),
        ((PAIR, NT, FF, WIDE), BF),
        ((3, SEQ, HEAD), F32),
        ((WIDTH, 2 * PAIR * FF), BF),
        ((WIDTH, 2 * FF), BF),
        ((FF, WIDTH), BF),
        ((HEAD, WIDTH), BF),
        ((WIDE, WIDTH), BF),
        ((NX, SEQ, 512), BF),
        ((NX, SEQ, 512), BF),
        ((NX, SEQ, 512), BF),
        ((NX, SEQ, 512), BF),
        ((SEQ, WIDTH), BF),
        ((NT, SEQ, WIDE), BF),
        ((NE, TILE, 128), BF),
        ((NT * TILE, 128), BF),
        ((NT, TILE, 128), BF),
        ((NT, TILE, 128), BF),
        ((NT, TILE, 128), BF),
        ((NT * TILE, NT * TILE), BF),
        ((NT * TILE, NT * TILE), BF),
        ((NT * SEQ, NT * SEQ), BF),
        ((ROWS, ROWS), BF),
        ((SEQ, WIDTH), F32),
        ((SEQ, WIDTH), BF),
        ((NE, 2 * BOTH, 128), BF),
        ((NE, 2 * BOTH, 128), BF),
        ((PAIR * SLOTS, WIDTH), BF),
        ((PAIR * SLOTS, WIDTH), BF),
        ((ROWS, WIDTH), BF),
        ((PAIR * SLOTS, NT * FF), BF),
        ((SEQ, WIDTH), BF),
        ((NT, SEQ, WIDE), BF),
        ((2, NX, SEQ, 1024), BF),
        ((2, NX, SEQ, 1024), BF),
        ((2, NZ, SEQ, 128), BF),
        ((2, NZ, SEQ, 128), BF),
        ((NT, 16, 128), BF),
        ((NT, 16, 128), BF),
        ((NT * 16, TILE), BF),
        ((2, SEQ, NT * 16), BF),
        ((NE, 2 * BOTH, 128), BF),
        ((NE, 2 * BOTH, 128), BF),
        ((SEQ, HEAD), F32),
        ((2, SEQ, LINES), F32),
        ((LINES, SEQ), BF),
        ((2, PAIR * SLOTS, LINES), BF),
        ((LINES, PAIR * SLOTS), BF),
        ((LINES, 128), F32),
        ((SEQ, WIDE), F32),
    ]
    result, held = pl.pallas_call(
        layer,
        out_shape=[
            pltpu.VMEM((SEQ, WIDE), F32),
            pltpu.VMEM((SEQ, 1, HEAD, HEAD), F32),
        ],
        in_specs=[vmem if i in small else hbm for i in range(len(args))],
        out_specs=[vmem, vmem],
        scratch_shapes=[pltpu.VMEM(shape, kind) for shape, kind in scratch]
        + [
            pltpu.SemaphoreType.DMA((SENDS,)),
            pltpu.SemaphoreType.DMA((ARRIVALS,)),
            pltpu.SemaphoreType.DMA((LOCALS,)),
        ],
        compiler_params=pltpu.CompilerParams(collective_id=0, has_side_effects=True),
        name="layer",
    )(*args)
    return pl.pallas_call(
        closing,
        out_shape=[
            jax.ShapeDtypeStruct((SEQ, WIDE), BF),
            jax.ShapeDtypeStruct((SEQ, 1, HEAD, HEAD), F32),
        ],
        in_specs=[vmem, hbm],
        out_specs=[vmem, hbm],
        scratch_shapes=[pltpu.SemaphoreType.DMA(())],
        name="closing",
    )(pltpu.with_memory_space_constraint(result, pltpu.VMEM), pltpu.with_memory_space_constraint(held, pltpu.VMEM))


def solution(mesh):
    torus = Mesh(mesh.devices.reshape(NZ, NX, NY, NC), ("z", "x", "y", "c"))
    return jax.shard_map(
        local,
        mesh=torus,
        in_specs=(
            P(EP, None),
            P(EP, TP, None, None),
            P(),
            P(EP, TP),
            P(EP, TP),
            P(EP, TP),
            P(EP, TP),
            P(TP),
            P(TP),
            P(TP, None),
            P(),
            P(EP, None),
            P(EP, None),
            P(EP, None, TP),
            P(EP, None, TP),
            P(EP, TP, None),
            P(None, TP),
            P(None, TP),
            P(TP, None),
            P(TP, EP),
            P(TP, EP),
            P(EP, TP),
            P(TP),
        ),
        out_specs=(P(EP, TP), P(EP, TP, None, None)),
        check_vma=False,
    )
```

```python
import jax
import jax.numpy as jnp
from jax import lax
from jax.experimental import pallas as pl
from jax.experimental.pallas import tpu as pltpu
from jax.sharding import Mesh
from jax.sharding import PartitionSpec as P

EP = ("z", "x")
TP = ("y", "c")
NZ, NX, NY, NC = 8, 4, 4, 2
NE, NT = NZ * NX, NY * NC
MESH = pl.DeviceIdType.MESH
EPS = 1e-06
SEQ, WIDTH, HEAD, WIDE, TOPK = 48, 2048, 128, 256, 4
PAIR, CAP = 2, 6
SLOTS, BOTH = NE * CAP, PAIR * CAP
LINES = NE * 2 * BOTH
ROWS = SEQ * NE // NT
FF = 128
OWN = SEQ // NT
TILE = OWN * WIDTH // 128

BF, F32 = jnp.bfloat16, jnp.float32
Z_ORDER = (1, 7, 2, 6, 3, 5, 4)
Y_ORDER = (1, 3, 2)
X_ORDER = (1, 3, 2)
FAR_ORDER = (4, 3, 5, 2, 6, 1, 7, 0)
SENDS, ARRIVALS, LOCALS = 25, 74, 19
scope = jax.named_scope


def cols_at(ref, index, width):
    start = pl.multiple_of(index * width, width)
    return ref.at[(slice(None),) * (len(ref.shape) - 1) + (pl.ds(start, width),)]


def dot(left, right):
    return jnp.dot(left, right, preferred_element_type=F32)


def iota(shape, dim):
    return lax.broadcasted_iota(jnp.int32, shape, dim)


def scaled(values, gain):
    values = values.astype(F32)
    return values * lax.rsqrt(jnp.mean(values * values, axis=-1, keepdims=True) + EPS) * gain


class Links:
    def __init__(self, send_sem, recv_sem, local_sem):
        self.send_sem, self.recv_sem, self.local_sem = send_sem, recv_sem, local_sem
        self.sent = self.received = self.locals = 0
        self.z, self.x = lax.axis_index("z"), lax.axis_index("x")
        self.y, self.c = lax.axis_index("y"), lax.axis_index("c")
        self.e = self.z * NX + self.x
        self.t = self.y * NC + self.c
        self.pending = []

    def load(self, src, dst):
        copy = pltpu.make_async_copy(src, dst, self.local_sem.at[self.locals])
        self.locals += 1
        copy.start()
        return copy

    def reserve(self, number):
        first = self.received
        self.received += number
        return first

    def new_send(self):
        self.sent += 1
        return self.sent - 1

    def copy(self, src, dst, sent, slot, **device):
        return pltpu.make_async_remote_copy(
            src_ref=src,
            dst_ref=dst,
            send_sem=self.send_sem.at[sent],
            recv_sem=self.recv_sem.at[slot],
            device_id=device,
            device_id_type=MESH,
        )

    def stage(self, total):
        sent = self.new_send()
        self.pending.append(self.copy(total, total, sent, 0, c=1 - self.c))

        def send(src, dst, slot, **device):
            self.copy(src, dst, sent, slot, **device).start()

        return send

    def wait(self, dst, slot):
        self.copy(dst, dst, 0, slot, c=1 - self.c).wait_recv()

    def finish(self):
        for copy in self.pending:
            copy.wait_send()
        assert (self.sent, self.received, self.locals) == (SENDS, ARRIVALS, LOCALS)

    def greet(self):
        barrier = pltpu.get_barrier_semaphore()
        peers = []
        for dz in FAR_ORDER:
            for dx in (2, 1, 3, 0):
                if dz or dx:
                    peers.append(dict(z=(self.z + dz) % NZ, x=(self.x + dx) % NX))
        for dy in (2, 1, 3, 0):
            for dc in range(NC):
                if dy or dc:
                    peers.append(dict(y=(self.y + dy) % NY, c=(self.c + dc) % NC))
        for peer in peers:
            pl.semaphore_signal(barrier, inc=1, device_id=peer, device_id_type=MESH)
        return lambda: pl.semaphore_wait(barrier, len(peers))

    def gather_tp(self, view, seven):
        base = self.reserve(10)
        send = self.stage(seven)
        up, down = (self.y + 1) % NY, (self.y + NY - 1) % NY
        far = (self.y + 2) % NY

        def half(y, i):
            block = view(y * NC + self.c)
            size = block.shape[0] // 2
            return block.at[(pl.ds(i * size, size),) + (slice(None),) * (len(block.shape) - 1)]

        for i in range(2):
            send(half(self.y, i), half(self.y, i), base + i, y=up)
            send(half(self.y, 1 - i), half(self.y, 1 - i), base + 2 + i, y=down)
        mine = view(self.t)
        send(mine, mine, base + 6, c=1 - self.c)

        def onward():
            self.wait(half(down, 0), base)
            send(half(down, 0), half(down, 0), base + 4, y=up)
            self.wait(half(up, 1), base + 2)
            send(half(up, 1), half(up, 1), base + 5, y=down)

        def relay():
            self.wait(half(down, 1), base + 1)
            block = view(down * NC + self.c)
            send(block, block, base + 7, c=1 - self.c)
            self.wait(half(up, 0), base + 3)
            block = view(up * NC + self.c)
            send(block, block, base + 8, c=1 - self.c)
            self.wait(half(far, 0), base + 4)
            self.wait(half(far, 1), base + 5)
            block = view(far * NC + self.c)
            send(block, block, base + 9, c=1 - self.c)

        def rest(only=range(4)):
            for i in only:
                self.wait(view((self.y, down, up, far)[i] * NC + 1 - self.c), base + 6 + i)

        return onward, relay, rest

    def swap_tp(self, src_view, dst_view, seven):
        base = self.reserve(1)
        send = self.stage(seven)
        mine = dst_view(self.t)
        for dy in Y_ORDER + (0,):
            for dc in range(NC):
                if dy or dc:
                    y, c = (self.y + dy) % NY, (self.c + dc) % NC
                    send(src_view(y * NC + c), mine, base, y=y, c=c)
        return lambda: self.wait(seven, base)

    def swap_ep(self, src, dst):
        slot, sent = self.reserve(1), self.new_send()
        for dz in (4, 3, 5, 2, 6, 1, 7, 0):
            for dx in (2, 1, 3, 0):
                if dz or dx:
                    z, x = (self.z + dz) % NZ, (self.x + dx) % NX
                    self.copy(src.at[z * NX + x], dst.at[self.e], sent, slot, z=z, x=x).start()
        self.pending.append(self.copy(src.at[pl.ds(0, NE - 1)], dst.at[pl.ds(0, NE - 1)], sent, slot, c=1 - self.c))
        return lambda: self.wait(dst.at[pl.ds(0, NE - 1)], slot)


def layer(
    tokens,
    state,
    norm_gain,
    w_query,
    w_forget,
    w_input,
    w_outgate,
    lower_bound,
    head_gain,
    w_output,
    ffn_gain,
    route_ids,
    route_weight,
    expert_gate,
    expert_up,
    expert_down,
    shared_gate,
    shared_up,
    shared_down,
    dense_gate,
    dense_up,
    dense_down,
    dense_mix,
    mixed,
    held,
    tok,
    wz,
    dense_w,
    down_own,
    down_all,
    gates,
    expert_w,
    shared_w,
    shared_d,
    out_w,
    dense_d,
    tok_out,
    tok_in,
    part_out,
    part_in,
    head_part,
    head_in,
    rows,
    flat,
    tok_rows,
    row_out,
    row_in,
    pack,
    unpack,
    regroup,
    dense_raw,
    resid_rows,
    slot_out,
    slot_in,
    chosen,
    chosen_in,
    dense_in,
    hidden,
    shared_part,
    shared_in,
    sum_out,
    sum_in,
    sum2_out,
    sum2_in,
    zq_out,
    zq_in,
    xq_out,
    xq_in,
    quarter,
    swap_out,
    swap_in,
    pad_lines,
    take_lines,
    back_out,
    back_in,
    readout,
    combine,
    dispatch,
    squeeze,
    expand,
    second,
    resid,
    send_sem,
    recv_sem,
    local_sem,
):
    n = Links(send_sem, recv_sem, local_sem)
    met = n.greet()
    own_down = cols_at(expert_down, n.t, WIDE)
    load_tok = n.load(tokens, tok)
    load_w = [
        n.load(w, wz.at[n.z, :, pl.ds(i * HEAD, HEAD)])
        for i, w in enumerate((w_query, w_forget, w_input, w_outgate))
    ]
    load_dense = [
        n.load(w, dense_w.at[n.t, :, pl.ds(i * WIDE, WIDE)]) for i, w in enumerate((dense_gate, dense_up))
    ]
    load_down = n.load(expert_down, down_own)
    load_mine = n.load(own_down, down_all.at[:, n.t])
    load_state = n.load(state, held)
    load_out = n.load(w_output, out_w)
    load_shared = [
        n.load(shared_gate, shared_w.at[:, pl.ds(0, FF)]),
        n.load(shared_up, shared_w.at[:, pl.ds(FF, FF)]),
        n.load(shared_down, shared_d),
    ]
    load_expert = [
        n.load(w.at[j], expert_w.at[:, pl.ds((2 * j + i) * FF, FF)])
        for j in range(PAIR)
        for i, w in enumerate((expert_gate, expert_up))
    ]
    load_dense_d = n.load(dense_down, cols_at(dense_d, n.t, WIDE))

    load_tok.wait()
    normed = scaled(tok[...], norm_gain[...]).astype(BF)
    for x in range(NX):
        for z in range(NZ):
            start = (z * NX + x) * 64
            tok_out[x, :, z * 64 : (z + 1) * 64] = normed[:, start : start + 64]
    tok_in[pl.ds(n.x, 1)] = tok_out[pl.ds(n.x, 1)]

    met()
    for copy in load_w:
        copy.wait()
    base_w = n.reserve(7)
    send_w = n.stage(wz.at[pl.ds(0, 7)])
    z_at = [(n.z + dz) % NZ for dz in range(NZ)]
    for dz, slot in ((2, 0), (6, 1), (1, 2), (7, 2)):
        send_w(wz.at[n.z], wz.at[n.z], base_w + slot, z=z_at[dz])
    base_t = n.reserve(1)
    send_t = n.stage(tok_in.at[pl.ds(0, 3)])
    for dx in X_ORDER:
        x = (n.x + dx) % NX
        send_t(tok_out.at[x], tok_in.at[n.x], base_t, x=x)
    for copy in load_dense:
        copy.wait()
    dense_onward, dense_relay, dense_rest = n.gather_tp(
        lambda t: dense_w.at[t], dense_w.at[pl.ds(0, 7)]
    )
    load_dense_d.wait()
    last_onward, last_relay, last_rest = n.gather_tp(
        lambda t: cols_at(dense_d, t, WIDE), dense_d.at[:, pl.ds(0, 7 * WIDE)]
    )

    with scope("routes"):
        expert_row = iota((128, SEQ), 0)
        named = [route_ids[k : k + 1, :] for k in range(TOPK)]
        equal = [(expert_row == ids).astype(F32) for ids in named]
        earlier = (iota((SEQ, SEQ), 0) < iota((SEQ, SEQ), 1)).astype(BF)
        rank = dot(sum(equal).astype(BF), earlier)
        line = iota((LINES, SEQ), 0).astype(F32)
        halves = [jnp.zeros((LINES, SEQ), F32) for _ in range(2)]
        picked = jnp.zeros((LINES, SEQ), F32)
        for k in range(TOPK):
            ids = named[k]
            first = (ids // PAIR) * (2 * BOTH) + (ids % PAIR) * CAP
            place = first.astype(F32) + jnp.sum(equal[k] * rank, axis=0, keepdims=True)
            for h in range(2):
                here = line == place + h * BOTH
                halves[h] = halves[h] + jnp.where(here, route_weight[k : k + 1, :], 0.0)
                picked = picked + here.astype(F32)
        dispatch[...] = picked.astype(BF)
        for h in range(2):
            rest = halves[h].T
            for i in range(3):
                piece = rest.astype(BF)
                combine[h, i * SEQ : (i + 1) * SEQ, :] = piece
                rest = rest - piece.astype(F32)

    def row_of(place):
        inside = place % BOTH
        return (inside // CAP) * SLOTS + (place // (2 * BOTH)) * CAP + inside % CAP

    def is_second(place):
        return (place // BOTH) % 2

    across, along = iota((1, LINES), 1), iota((LINES, 1), 0)
    row = iota((PAIR * SLOTS, LINES), 0)
    for h in range(2):
        target = jnp.where(is_second(across) == h, row_of(across), -1)
        squeeze[h, :, :] = (row == target).astype(F32).astype(BF)
    expand[...] = (iota((LINES, PAIR * SLOTS), 1) == row_of(along)).astype(F32).astype(BF)
    second[...] = jnp.broadcast_to(is_second(along), (LINES, 128)).astype(F32)

    def in_lines(values):
        return jnp.where(second[...] > 0.5, values[:, 128:], values[:, :128]).astype(BF).reshape(NE, 2 * BOTH, 128)

    def packed_row(row):
        inside = row % SEQ
        return (inside // OWN) * TILE + (row // SEQ) * OWN + inside % OWN

    def quarter_row(row):
        inside = row % SEQ
        return (inside // OWN) * 4 * OWN + (row // SEQ) * OWN + inside % OWN

    def regrouped_row(row):
        e = row // OWN
        return (e % NX) * SEQ + (e // NX) * OWN + row % OWN

    many = NT * TILE
    pack[...] = (iota((many, many), 0) == packed_row(iota((1, many), 1))).astype(F32).astype(BF)
    unpack[...] = (iota((many, many), 1) == packed_row(iota((many, 1), 0))).astype(F32).astype(BF)
    quarter[...] = (iota((ROWS, ROWS), 0) == quarter_row(iota((1, ROWS), 1))).astype(F32).astype(BF)
    line = iota((1, TILE), 1)
    pad_lines[...] = (iota((NT * 16, TILE), 0) == (line // 12) * 16 + line % 12).astype(F32).astype(BF)
    token = iota((SEQ, 1), 0)
    for h in range(2):
        source = (token // OWN) * 16 + h * OWN + token % OWN
        take_lines[h, :, :] = (iota((SEQ, NT * 16), 1) == source).astype(F32).astype(BF)
    regroup[...] = (iota((ROWS, ROWS), 0) == regrouped_row(iota((1, ROWS), 1))).astype(F32).astype(BF)
    for k in range(WIDTH // 128):
        flat[k * SEQ : (k + 1) * SEQ, :] = tok[:, k * 128 : (k + 1) * 128]
    tok_rows[...] = dot(pack[...], flat[...]).astype(BF).reshape(NT, TILE, 128)

    for source, near, far, row, slot in ((6, 1, 2, 0, 0), (2, 7, 6, 32, 1)):
        block = wz.at[z_at[source]]
        n.wait(block, base_w + slot)
        send_w(block, block, base_w + 3 + slot, z=z_at[near])
        block = wz.at[z_at[source], pl.ds(row, 32)]
        send_w(block, block, base_w + 5 + slot, z=z_at[far])
    dense_onward()
    n.wait(tok_in.at[pl.ds(0, 3)], base_t)
    n.wait(wz.at[pl.ds(0, 2)], base_w + 2)
    for slot in range(2):
        n.wait(wz.at[0], base_w + 3 + slot)
        n.wait(wz.at[0, pl.ds(0, 32)], base_w + 5 + slot)
    part = dot(tok_in[...].reshape(NX * SEQ, 512), wz[...].reshape(512, 512))
    part_out[...] = part.astype(BF).reshape(NX, SEQ, 512)
    base_p = n.reserve(1)
    send_p = n.stage(part_in.at[pl.ds(0, 3)])
    for dx in X_ORDER:
        x = (n.x + dx) % NX
        send_p(part_out.at[x], part_in.at[n.x], base_p, x=x)
    part_in[pl.ds(n.x, 1)] = part_out[pl.ds(n.x, 1)]
    n.wait(part_in.at[pl.ds(0, 3)], base_p)
    projected = part_in[0].astype(F32)
    for x in range(1, NX):
        projected = projected + part_in[x].astype(F32)
    projected = projected.astype(BF).astype(F32)
    query, forget_pre = projected[:, :HEAD], projected[:, HEAD : 2 * HEAD]
    values, out_gate = projected[:, 2 * HEAD : 3 * HEAD], projected[:, 3 * HEAD :]
    low = lower_bound[...]
    forget_sig = jax.nn.sigmoid(forget_pre)
    decay = low + (1.0 - low) * forget_sig
    keygate = (1.0 - low) * (1.0 - forget_sig)
    mixed_q = (query * decay).T
    gates[0, :, :], gates[1, :, :], gates[2, :, :] = decay, keygate, values
    load_state.wait()
    for b in range(SEQ):
        readout[b : b + 1, :] = jnp.sum(mixed_q[:, b : b + 1] * held[b, 0], axis=0, keepdims=True)
    read = readout[...] + jnp.sum(query * keygate, axis=1, keepdims=True) * values
    read = read * lax.rsqrt(jnp.mean(read * read, axis=-1, keepdims=True) + EPS)
    head_out = (read * head_gain[...] * jax.nn.silu(out_gate)).astype(BF)
    load_out.wait()
    whole = dot(head_out, out_w[...]).astype(BF)
    head_part[...] = whole
    head_rest = n.swap_tp(lambda t: cols_at(head_part, t, WIDE), lambda t: head_in.at[t], head_in.at[pl.ds(0, 7)])
    for k in range(WIDTH // 128):
        flat[k * SEQ : (k + 1) * SEQ, :] = whole[:, k * 128 : (k + 1) * 128]
    row_out[...] = dot(pack[...], flat[...]).astype(BF).reshape(NT, TILE, 128)
    row_rest = n.swap_tp(lambda t: row_out.at[t], lambda t: row_in.at[t], row_in.at[pl.ds(0, 7)])
    row_in[pl.ds(n.t, 1)] = row_out[pl.ds(n.t, 1)]
    head_in[pl.ds(n.t, 1)] = cols_at(head_part, n.t, WIDE)[...][None]
    last_onward()
    head_rest()
    own = cols_at(tok, n.t, WIDE)[...].astype(F32)
    for t in range(NT):
        own = own + head_in[t].astype(F32)
    own_cols = own.astype(BF)
    slot_out[...] = in_lines(dot(dispatch[...], own_cols))
    slots_rest = n.swap_ep(slot_out, slot_in)
    slot_in[pl.ds(n.e, 1)] = slot_out[pl.ds(n.e, 1)]
    resid[...] = own

    row_rest()
    own = tok_rows[pl.ds(n.t, 1)][0].astype(F32)
    for t in range(NT):
        own = own + row_in[t].astype(F32)
    rows[pl.ds(n.e, 1)] = own.astype(BF)[None]
    base_c = n.reserve(NZ)
    send_c = n.stage(rows.at[pl.ds(0, NE - 1)])
    mine = rows.at[n.e]
    for i, dz in enumerate(Z_ORDER):
        send_c(mine, mine, base_c + i, z=z_at[dz])
    for dx in X_ORDER:
        send_c(mine, mine, base_c + 7, x=(n.x + dx) % NX)
    cols_at(resid_rows, n.t, WIDE)[...] = own_cols
    rows_mine = cols_at(resid_rows, n.t, WIDE)
    rows_seven = resid_rows.at[:, pl.ds(0, 7 * WIDE)]
    rows_rest = n.swap_tp(lambda t: rows_mine, lambda t: cols_at(resid_rows, t, WIDE), rows_seven)
    load_down.wait()

    def swap_down(j):
        here = down_all.at[j]
        return n.swap_tp(lambda t: cols_at(down_own.at[j], t, WIDE), lambda t: here.at[t], here.at[pl.ds(0, 7)])

    down_rest = [swap_down(0)]
    dense_relay()
    last_relay()

    def pass_on(order):
        for i in order:
            e = z_at[(NZ - Z_ORDER[i]) % NZ] * NX + n.x
            n.wait(rows.at[e], base_c + i)
            for dx in X_ORDER:
                send_c(rows.at[e], rows.at[e], base_c + 7, x=(n.x + dx) % NX)

    pass_on(range(2))

    slots_rest()
    lines = slot_in[...].reshape(LINES, 128)
    picked_rows = jnp.concatenate([dot(squeeze[h], lines) for h in range(2)], axis=1)
    cols_at(chosen, n.t, WIDE)[...] = picked_rows.astype(BF)
    chosen_onward, chosen_relay, chosen_rest = n.gather_tp(
        lambda t: cols_at(chosen, t, WIDE), chosen.at[:, pl.ds(0, 7 * WIDE)]
    )
    pass_on(range(2, 7))

    gain = ffn_gain[...]
    rows_rest()
    for copy in load_shared:
        copy.wait()
    shared_x = scaled(resid_rows[...], gain).astype(BF)
    shared_pre = dot(shared_x, shared_w[...])
    shared_hidden = (jax.nn.silu(shared_pre[:, :FF]) * shared_pre[:, FF:]).astype(BF)
    shared_part[...] = dot(shared_hidden, shared_d[...]).astype(BF)
    chosen_onward()
    down_rest.append(swap_down(1))

    chosen_relay()
    chosen_rest()
    for copy in load_expert:
        copy.wait()
    for j in range(PAIR):
        for i in range(4):
            part = pl.ds(j * SLOTS + i * SEQ, SEQ)
            chosen_in[part] = scaled(chosen[part], gain).astype(BF)
        pre = dot(chosen_in[pl.ds(j * SLOTS, SLOTS)], expert_w[:, 2 * j * FF : 2 * (j + 1) * FF])
        unit = (jax.nn.silu(pre[:, :FF]) * pre[:, FF:]).astype(BF)
        cols_at(hidden, n.t, FF).at[pl.ds(j * SLOTS, SLOTS)][...] = unit
    hidden_onward, hidden_relay, hidden_rest = n.gather_tp(
        lambda t: cols_at(hidden, t, FF), hidden.at[:, pl.ds(0, 7 * FF)]
    )

    n.wait(rows.at[pl.ds(0, 24)], base_c + 7)
    for g in range(NE // NT):
        group = dot(unpack[...], rows[g * NT : (g + 1) * NT].reshape(NT * TILE, 128))
        for k in range(WIDTH // 128):
            dense_raw[:, k * 128 : (k + 1) * 128] = group[k * SEQ : (k + 1) * SEQ, :]
        dense_in[g * SEQ : (g + 1) * SEQ, :] = scaled(dense_raw[...], gain).astype(BF)
    dense_rest()
    pre = dot(dense_in[...], dense_w[...].reshape(WIDTH, 2 * WIDE))
    units = (jax.nn.silu(pre[:, :WIDE]) * pre[:, WIDE:]).astype(BF)
    inner = dot(regroup[...], units).astype(BF)
    last_rest()
    def to_lines(block):
        for k in range(4):
            flat[k * SEQ : (k + 1) * SEQ, :] = block[:, k * 128 : (k + 1) * 128]
        return dot(quarter[...], flat[:ROWS]).astype(BF).reshape(NZ, 4 * OWN, 128)

    block = dot(inner, dense_d[:, 3 * 512 :]).astype(BF)
    for x in range(NX):
        zq_out[:, x] = to_lines(block[x * SEQ : (x + 1) * SEQ])
    base_zq = n.reserve(1)
    send_zq = n.stage(zq_in.at[pl.ds(0, 7)])
    for dz in FAR_ORDER[:-1]:
        send_zq(zq_out.at[z_at[dz]], zq_in.at[n.z], base_zq, z=z_at[dz])
    zq_in[pl.ds(n.z, 1)] = zq_out[pl.ds(n.z, 1)]
    base_x = n.reserve(3)
    for q in range(3):
        block = dot(inner, dense_d[:, q * 512 : (q + 1) * 512])
        sum_out[q, :, :, :] = block.astype(BF).reshape(NX, SEQ, 512)
        send_x = n.stage(sum_in.at[q, pl.ds(0, 3)])
        for dx in X_ORDER:
            x = (n.x + dx) % NX
            send_x(sum_out.at[q, x], sum_in.at[q, n.x], base_x + q, x=x)

    base_z = n.reserve(3)

    def sum_over_x(q):
        n.wait(sum_in.at[q, pl.ds(0, 3)], base_x + q)
        block = sum_out[q, pl.ds(n.x, 1)][0].astype(F32)
        for dx in X_ORDER:
            block = block + sum_in[q, pl.ds((n.x + dx) % NX, 1)][0].astype(F32)
        sum2_out[q, :, :, :] = to_lines(block.astype(BF))
        send_z = n.stage(sum2_in.at[q, pl.ds(0, 7)])
        for dz in FAR_ORDER[:-1]:
            send_z(sum2_out.at[q, z_at[dz]], sum2_in.at[q, n.z], base_z + q, z=z_at[dz])
        sum2_in[q, pl.ds(n.z, 1)] = sum2_out[q, pl.ds(n.z, 1)]

    hidden_onward()
    hidden_relay()
    sum_over_x(0)
    sum_over_x(1)
    n.wait(zq_in.at[pl.ds(0, 7)], base_zq)
    acc = zq_in[0].astype(F32)
    for z in range(1, NZ):
        acc = acc + zq_in[z].astype(F32)
    xq_out[...] = acc.astype(BF)
    base_xq = n.reserve(1)
    send_xq = n.stage(xq_in.at[pl.ds(0, 3)])
    for dx in X_ORDER:
        x = (n.x + dx) % NX
        send_xq(xq_out.at[x], xq_in.at[n.x], base_xq, x=x)
    xq_in[pl.ds(n.x, 1)] = xq_out[pl.ds(n.x, 1)]
    sum_over_x(2)

    shared_rest = n.swap_tp(lambda t: cols_at(shared_part, t, WIDE), lambda t: shared_in.at[t], shared_in.at[pl.ds(0, 7)])
    shared_in[pl.ds(n.t, 1)] = cols_at(shared_part, n.t, WIDE)[...][None]
    for rest in down_rest:
        rest()
    load_mine.wait()
    hidden_rest()
    outs = [
        dot(hidden[pl.ds(j * SLOTS, SLOTS)], down_all[j].reshape(NT * FF, WIDE)).astype(BF) for j in range(PAIR)
    ]
    spread = dot(expand[:, :SLOTS], outs[0]) + dot(expand[:, SLOTS:], outs[1])
    back_out[...] = in_lines(spread)
    back_rest = n.swap_ep(back_out, back_in)
    back_in[pl.ds(n.e, 1)] = back_out[pl.ds(n.e, 1)]

    decay, keygate = gates[0].T, gates[1].T
    for b in range(SEQ):
        held[b, 0] = decay[:, b : b + 1] * held[b, 0] + keygate[:, b : b + 1] * gates[2, b : b + 1, :]

    own_lines = []
    for q in range(3):
        n.wait(sum2_in.at[q, pl.ds(0, 7)], base_z + q)
        acc = sum2_in[q, 0].astype(F32)
        for z in range(1, NZ):
            acc = acc + sum2_in[q, z].astype(F32)
        own_lines.append(acc)
    n.wait(xq_in.at[pl.ds(0, 3)], base_xq)
    acc = xq_in[0].astype(F32)
    for x in range(1, NX):
        acc = acc + xq_in[x].astype(F32)
    own_lines.append(acc)
    own_lines = jnp.concatenate(own_lines, axis=0).astype(BF)
    swap_out[...] = dot(pad_lines[...], own_lines).astype(BF).reshape(NT, 16, 128)
    swap_rest = n.swap_tp(lambda t: swap_out.at[t], lambda t: swap_in.at[t], swap_in.at[pl.ds(0, 7)])
    swap_in[pl.ds(n.t, 1)] = swap_out[pl.ds(n.t, 1)]
    shared_rest()
    result = resid[...]
    for t in range(NT):
        result = result + shared_in[t].astype(F32)
    swap_rest()
    lines = swap_in[...].reshape(NT * 16, 128)
    dense_out = jnp.concatenate([dot(take_lines[h], lines) for h in range(2)], axis=1)
    result = result + dense_out * jax.nn.sigmoid(dense_mix[...])
    back_rest()
    lines = back_in[...].reshape(LINES, 128)
    both = dot(combine[...].reshape(6 * SEQ, LINES), lines)
    parts = [both[i * SEQ : (i + 1) * SEQ] for i in range(6)]
    routed = [parts[3 * h] + (parts[3 * h + 1] + parts[3 * h + 2]) for h in range(2)]
    result = result + jnp.concatenate(routed, axis=1)
    mixed[...] = result
    n.finish()


def closing(result, held, mixed, new_state, sem):
    copy = pltpu.make_async_copy(held, new_state, sem)
    copy.start()
    mixed[...] = result[...].astype(BF)
    copy.wait()


def local(*args):
    args = list(args)
    for i in (2, 7, 8, 10, 22):
        args[i] = args[i].reshape(1, -1)
    for i in (11, 12):
        args[i] = args[i].T
    vmem = pl.BlockSpec(memory_space=pltpu.VMEM)
    hbm = pl.BlockSpec(memory_space=pl.ANY)
    small = (2, 7, 8, 10, 11, 12, 22)
    scratch = [
        ((SEQ, WIDTH), BF),
        ((NZ, 64, 512), BF),
        ((NT, WIDE, 2 * WIDE), BF),
        ((PAIR, FF, WIDTH), BF),
        ((PAIR, NT, FF, WIDE), BF),
        ((3, SEQ, HEAD), F32),
        ((WIDTH, 2 * PAIR * FF), BF),
        ((WIDTH, 2 * FF), BF),
        ((FF, WIDTH), BF),
        ((HEAD, WIDTH), BF),
        ((WIDE, WIDTH), BF),
        ((NX, SEQ, 512), BF),
        ((NX, SEQ, 512), BF),
        ((NX, SEQ, 512), BF),
        ((NX, SEQ, 512), BF),
        ((SEQ, WIDTH), BF),
        ((NT, SEQ, WIDE), BF),
        ((NE, TILE, 128), BF),
        ((NT * TILE, 128), BF),
        ((NT, TILE, 128), BF),
        ((NT, TILE, 128), BF),
        ((NT, TILE, 128), BF),
        ((NT * TILE, NT * TILE), BF),
        ((NT * TILE, NT * TILE), BF),
        ((ROWS, ROWS), BF),
        ((SEQ, WIDTH), F32),
        ((SEQ, WIDTH), BF),
        ((NE, 2 * BOTH, 128), BF),
        ((NE, 2 * BOTH, 128), BF),
        ((PAIR * SLOTS, WIDTH), BF),
        ((PAIR * SLOTS, WIDTH), BF),
        ((ROWS, WIDTH), BF),
        ((PAIR * SLOTS, NT * FF), BF),
        ((SEQ, WIDTH), BF),
        ((NT, SEQ, WIDE), BF),
        ((3, NX, SEQ, 512), BF),
        ((3, NX, SEQ, 512), BF),
        ((3, NZ, 4 * OWN, 128), BF),
        ((3, NZ, 4 * OWN, 128), BF),
        ((NZ, NX, 4 * OWN, 128), BF),
        ((NZ, NX, 4 * OWN, 128), BF),
        ((NX, 4 * OWN, 128), BF),
        ((NX, 4 * OWN, 128), BF),
        ((ROWS, ROWS), BF),
        ((NT, 16, 128), BF),
        ((NT, 16, 128), BF),
        ((NT * 16, TILE), BF),
        ((2, SEQ, NT * 16), BF),
        ((NE, 2 * BOTH, 128), BF),
        ((NE, 2 * BOTH, 128), BF),
        ((SEQ, HEAD), F32),
        ((2, 3 * SEQ, LINES), BF),
        ((LINES, SEQ), BF),
        ((2, PAIR * SLOTS, LINES), BF),
        ((LINES, PAIR * SLOTS), BF),
        ((LINES, 128), F32),
        ((SEQ, WIDE), F32),
    ]
    result, held = pl.pallas_call(
        layer,
        out_shape=[
            pltpu.VMEM((SEQ, WIDE), F32),
            pltpu.VMEM((SEQ, 1, HEAD, HEAD), F32),
        ],
        in_specs=[vmem if i in small else hbm for i in range(len(args))],
        out_specs=[vmem, vmem],
        scratch_shapes=[pltpu.VMEM(shape, kind) for shape, kind in scratch]
        + [
            pltpu.SemaphoreType.DMA((SENDS,)),
            pltpu.SemaphoreType.DMA((ARRIVALS,)),
            pltpu.SemaphoreType.DMA((LOCALS,)),
        ],
        compiler_params=pltpu.CompilerParams(collective_id=0, has_side_effects=True),
        name="layer",
    )(*args)
    return pl.pallas_call(
        closing,
        out_shape=[
            jax.ShapeDtypeStruct((SEQ, WIDE), BF),
            jax.ShapeDtypeStruct((SEQ, 1, HEAD, HEAD), F32),
        ],
        in_specs=[vmem, hbm],
        out_specs=[vmem, hbm],
        scratch_shapes=[pltpu.SemaphoreType.DMA(())],
        name="closing",
    )(pltpu.with_memory_space_constraint(result, pltpu.VMEM), pltpu.with_memory_space_constraint(held, pltpu.VMEM))


def solution(mesh):
    torus = Mesh(mesh.devices.reshape(NZ, NX, NY, NC), ("z", "x", "y", "c"))
    return jax.shard_map(
        local,
        mesh=torus,
        in_specs=(
            P(EP, None),
            P(EP, TP, None, None),
            P(),
            P(EP, TP),
            P(EP, TP),
            P(EP, TP),
            P(EP, TP),
            P(TP),
            P(TP),
            P(TP, None),
            P(),
            P(EP, None),
            P(EP, None),
            P(EP, None, TP),
            P(EP, None, TP),
            P(EP, TP, None),
            P(None, TP),
            P(None, TP),
            P(TP, None),
            P(TP, EP),
            P(TP, EP),
            P(EP, TP),
            P(TP),
        ),
        out_specs=(P(EP, TP), P(EP, TP, None, None)),
        check_vma=False,
    )
```

```python
import jax
import jax.numpy as jnp
from jax import lax
from jax.experimental import pallas as pl
from jax.experimental.pallas import tpu as pltpu
from jax.sharding import Mesh
from jax.sharding import PartitionSpec as P

EP = ("z", "x")
TP = ("y", "c")
NZ, NX, NY, NC = 8, 4, 4, 2
NE, NT = NZ * NX, NY * NC
MESH = pl.DeviceIdType.MESH
EPS = 1e-06
SEQ, WIDTH, HEAD, WIDE, TOPK = 48, 2048, 128, 256, 4
PAIR, CAP = 2, 6
SLOTS, BOTH = NE * CAP, PAIR * CAP
LINES = NE * 2 * BOTH
ROWS = SEQ * NE // NT
FF = 128
OWN = SEQ // NT
TILE = OWN * WIDTH // 128

BF, F32 = jnp.bfloat16, jnp.float32
Z_ORDER = (1, 7, 2, 6, 3, 5, 4)
Y_ORDER = (1, 3, 2)
X_ORDER = (1, 3, 2)
FAR_ORDER = (4, 3, 5, 2, 6, 1, 7, 0)
SENDS, ARRIVALS, LOCALS = 25, 74, 19
scope = jax.named_scope


def cols_at(ref, index, width):
    start = pl.multiple_of(index * width, width)
    return ref.at[(slice(None),) * (len(ref.shape) - 1) + (pl.ds(start, width),)]


def dot(left, right):
    return jnp.dot(left, right, preferred_element_type=F32)


def iota(shape, dim):
    return lax.broadcasted_iota(jnp.int32, shape, dim)


def scaled(values, gain):
    values = values.astype(F32)
    return values * lax.rsqrt(jnp.mean(values * values, axis=-1, keepdims=True) + EPS) * gain


class Links:
    def __init__(self, send_sem, recv_sem, local_sem):
        self.send_sem, self.recv_sem, self.local_sem = send_sem, recv_sem, local_sem
        self.sent = self.received = self.locals = 0
        self.z, self.x = lax.axis_index("z"), lax.axis_index("x")
        self.y, self.c = lax.axis_index("y"), lax.axis_index("c")
        self.e = self.z * NX + self.x
        self.t = self.y * NC + self.c
        self.pending = []

    def load(self, src, dst):
        copy = pltpu.make_async_copy(src, dst, self.local_sem.at[self.locals])
        self.locals += 1
        copy.start()
        return copy

    def reserve(self, number):
        first = self.received
        self.received += number
        return first

    def new_send(self):
        self.sent += 1
        return self.sent - 1

    def copy(self, src, dst, sent, slot, **device):
        return pltpu.make_async_remote_copy(
            src_ref=src,
            dst_ref=dst,
            send_sem=self.send_sem.at[sent],
            recv_sem=self.recv_sem.at[slot],
            device_id=device,
            device_id_type=MESH,
        )

    def stage(self, total):
        sent = self.new_send()
        self.pending.append(self.copy(total, total, sent, 0, c=1 - self.c))

        def send(src, dst, slot, **device):
            self.copy(src, dst, sent, slot, **device).start()

        return send

    def wait(self, dst, slot):
        self.copy(dst, dst, 0, slot, c=1 - self.c).wait_recv()

    def finish(self):
        for copy in self.pending:
            copy.wait_send()
        assert (self.sent, self.received, self.locals) == (SENDS, ARRIVALS, LOCALS)

    def greet(self):
        barrier = pltpu.get_barrier_semaphore()
        peers = []
        for dz in FAR_ORDER:
            for dx in (2, 1, 3, 0):
                if dz or dx:
                    peers.append(dict(z=(self.z + dz) % NZ, x=(self.x + dx) % NX))
        for dy in (2, 1, 3, 0):
            for dc in range(NC):
                if dy or dc:
                    peers.append(dict(y=(self.y + dy) % NY, c=(self.c + dc) % NC))
        for peer in peers:
            pl.semaphore_signal(barrier, inc=1, device_id=peer, device_id_type=MESH)
        return lambda: pl.semaphore_wait(barrier, len(peers))

    def gather_tp(self, view, seven):
        base = self.reserve(10)
        send = self.stage(seven)
        up, down = (self.y + 1) % NY, (self.y + NY - 1) % NY
        far = (self.y + 2) % NY

        def half(y, i):
            block = view(y * NC + self.c)
            size = block.shape[0] // 2
            return block.at[(pl.ds(i * size, size),) + (slice(None),) * (len(block.shape) - 1)]

        for i in range(2):
            send(half(self.y, i), half(self.y, i), base + i, y=up)
            send(half(self.y, 1 - i), half(self.y, 1 - i), base + 2 + i, y=down)
        mine = view(self.t)
        send(mine, mine, base + 6, c=1 - self.c)

        def onward():
            self.wait(half(down, 0), base)
            send(half(down, 0), half(down, 0), base + 4, y=up)
            self.wait(half(up, 1), base + 2)
            send(half(up, 1), half(up, 1), base + 5, y=down)

        def relay():
            self.wait(half(down, 1), base + 1)
            block = view(down * NC + self.c)
            send(block, block, base + 7, c=1 - self.c)
            self.wait(half(up, 0), base + 3)
            block = view(up * NC + self.c)
            send(block, block, base + 8, c=1 - self.c)
            self.wait(half(far, 0), base + 4)
            self.wait(half(far, 1), base + 5)
            block = view(far * NC + self.c)
            send(block, block, base + 9, c=1 - self.c)

        def rest(only=range(4)):
            for i in only:
                self.wait(view((self.y, down, up, far)[i] * NC + 1 - self.c), base + 6 + i)

        return onward, relay, rest

    def swap_tp(self, src_view, dst_view, seven):
        base = self.reserve(1)
        send = self.stage(seven)
        mine = dst_view(self.t)
        for dy in Y_ORDER + (0,):
            for dc in range(NC):
                if dy or dc:
                    y, c = (self.y + dy) % NY, (self.c + dc) % NC
                    send(src_view(y * NC + c), mine, base, y=y, c=c)
        return lambda: self.wait(seven, base)

    def swap_ep(self, src, dst):
        slot, sent = self.reserve(1), self.new_send()
        for dz in (4, 3, 5, 2, 6, 1, 7, 0):
            for dx in (2, 1, 3, 0):
                if dz or dx:
                    z, x = (self.z + dz) % NZ, (self.x + dx) % NX
                    self.copy(src.at[z * NX + x], dst.at[self.e], sent, slot, z=z, x=x).start()
        self.pending.append(self.copy(src.at[pl.ds(0, NE - 1)], dst.at[pl.ds(0, NE - 1)], sent, slot, c=1 - self.c))
        return lambda: self.wait(dst.at[pl.ds(0, NE - 1)], slot)


def layer(
    tokens,
    state,
    norm_gain,
    w_query,
    w_forget,
    w_input,
    w_outgate,
    lower_bound,
    head_gain,
    w_output,
    ffn_gain,
    route_ids,
    route_weight,
    expert_gate,
    expert_up,
    expert_down,
    shared_gate,
    shared_up,
    shared_down,
    dense_gate,
    dense_up,
    dense_down,
    dense_mix,
    mixed,
    held,
    tok,
    wz,
    dense_w,
    down_own,
    down_all,
    gates,
    expert_w,
    shared_w,
    shared_d,
    out_w,
    dense_d,
    tok_out,
    tok_in,
    part_out,
    part_in,
    head_part,
    head_in,
    rows,
    flat,
    tok_rows,
    row_out,
    row_in,
    pack,
    unpack,
    regroup,
    dense_raw,
    resid_rows,
    slot_out,
    slot_in,
    chosen,
    chosen_in,
    dense_in,
    hidden,
    shared_part,
    shared_in,
    sum_out,
    sum_in,
    sum2_out,
    sum2_in,
    zq_out,
    zq_in,
    xq_out,
    xq_in,
    quarter,
    swap_out,
    swap_in,
    pad_lines,
    take_lines,
    back_out,
    back_in,
    readout,
    combine,
    dispatch,
    squeeze,
    expand,
    second,
    resid,
    send_sem,
    recv_sem,
    local_sem,
):
    n = Links(send_sem, recv_sem, local_sem)
    met = n.greet()
    own_down = cols_at(expert_down, n.t, WIDE)
    load_tok = n.load(tokens, tok)
    load_w = [
        n.load(w, wz.at[n.z, :, pl.ds(i * HEAD, HEAD)])
        for i, w in enumerate((w_query, w_forget, w_input, w_outgate))
    ]
    load_dense = [
        n.load(w, dense_w.at[n.t, :, pl.ds(i * WIDE, WIDE)]) for i, w in enumerate((dense_gate, dense_up))
    ]
    load_down = n.load(expert_down, down_own)
    load_mine = n.load(own_down, down_all.at[:, n.t])
    load_state = n.load(state, held)
    load_out = n.load(w_output, out_w)
    load_shared = [
        n.load(shared_gate, shared_w.at[:, pl.ds(0, FF)]),
        n.load(shared_up, shared_w.at[:, pl.ds(FF, FF)]),
        n.load(shared_down, shared_d),
    ]
    load_expert = [
        n.load(w.at[j], expert_w.at[:, pl.ds((2 * j + i) * FF, FF)])
        for j in range(PAIR)
        for i, w in enumerate((expert_gate, expert_up))
    ]
    load_dense_d = n.load(dense_down, cols_at(dense_d, n.t, WIDE))

    load_tok.wait()
    normed = scaled(tok[...], norm_gain[...]).astype(BF)
    for x in range(NX):
        for z in range(NZ):
            start = (z * NX + x) * 64
            tok_out[x, :, z * 64 : (z + 1) * 64] = normed[:, start : start + 64]
    tok_in[pl.ds(n.x, 1)] = tok_out[pl.ds(n.x, 1)]

    met()
    for copy in load_w:
        copy.wait()
    base_w = n.reserve(7)
    send_w = n.stage(wz.at[pl.ds(0, 7)])
    z_at = [(n.z + dz) % NZ for dz in range(NZ)]
    for dz, slot in ((2, 0), (6, 1), (1, 2), (7, 2)):
        send_w(wz.at[n.z], wz.at[n.z], base_w + slot, z=z_at[dz])
    base_t = n.reserve(1)
    send_t = n.stage(tok_in.at[pl.ds(0, 3)])
    for dx in X_ORDER:
        x = (n.x + dx) % NX
        send_t(tok_out.at[x], tok_in.at[n.x], base_t, x=x)
    for copy in load_dense:
        copy.wait()
    dense_onward, dense_relay, dense_rest = n.gather_tp(
        lambda t: dense_w.at[t], dense_w.at[pl.ds(0, 7)]
    )
    load_dense_d.wait()
    last_onward, last_relay, last_rest = n.gather_tp(
        lambda t: cols_at(dense_d, t, WIDE), dense_d.at[:, pl.ds(0, 7 * WIDE)]
    )

    with scope("routes"):
        expert_row = iota((128, SEQ), 0)
        named = [route_ids[k : k + 1, :] for k in range(TOPK)]
        equal = [(expert_row == ids).astype(F32) for ids in named]
        earlier = (iota((SEQ, SEQ), 0) < iota((SEQ, SEQ), 1)).astype(BF)
        rank = dot(sum(equal).astype(BF), earlier)
        line = iota((LINES, SEQ), 0).astype(F32)
        halves = [jnp.zeros((LINES, SEQ), F32) for _ in range(2)]
        picked = jnp.zeros((LINES, SEQ), F32)
        for k in range(TOPK):
            ids = named[k]
            first = (ids // PAIR) * (2 * BOTH) + (ids % PAIR) * CAP
            place = first.astype(F32) + jnp.sum(equal[k] * rank, axis=0, keepdims=True)
            for h in range(2):
                here = line == place + h * BOTH
                halves[h] = halves[h] + jnp.where(here, route_weight[k : k + 1, :], 0.0)
                picked = picked + here.astype(F32)
        dispatch[...] = picked.astype(BF)
        for h in range(2):
            rest = halves[h].T
            for i in range(3):
                piece = rest.astype(BF)
                combine[h, i * SEQ : (i + 1) * SEQ, :] = piece
                rest = rest - piece.astype(F32)

    def row_of(place):
        inside = place % BOTH
        return (inside // CAP) * SLOTS + (place // (2 * BOTH)) * CAP + inside % CAP

    def is_second(place):
        return (place // BOTH) % 2

    across, along = iota((1, LINES), 1), iota((LINES, 1), 0)
    row = iota((PAIR * SLOTS, LINES), 0)
    for h in range(2):
        target = jnp.where(is_second(across) == h, row_of(across), -1)
        squeeze[h, :, :] = (row == target).astype(F32).astype(BF)
    expand[...] = (iota((LINES, PAIR * SLOTS), 1) == row_of(along)).astype(F32).astype(BF)
    second[...] = jnp.broadcast_to(is_second(along), (LINES, 128)).astype(F32)

    def in_lines(values):
        return jnp.where(second[...] > 0.5, values[:, 128:], values[:, :128]).astype(BF).reshape(NE, 2 * BOTH, 128)

    def packed_row(row):
        inside = row % SEQ
        return (inside // OWN) * TILE + (row // SEQ) * OWN + inside % OWN

    def quarter_row(row):
        inside = row % SEQ
        return (inside // OWN) * 4 * OWN + (row // SEQ) * OWN + inside % OWN

    def regrouped_row(row):
        e = row // OWN
        return (e % NX) * SEQ + (e // NX) * OWN + row % OWN

    many = NT * TILE
    pack[...] = (iota((many, many), 0) == packed_row(iota((1, many), 1))).astype(F32).astype(BF)
    unpack[...] = (iota((many, many), 1) == packed_row(iota((many, 1), 0))).astype(F32).astype(BF)
    quarter[...] = (iota((ROWS, ROWS), 0) == quarter_row(iota((1, ROWS), 1))).astype(F32).astype(BF)
    line = iota((1, TILE), 1)
    pad_lines[...] = (iota((NT * 16, TILE), 0) == (line // 12) * 16 + line % 12).astype(F32).astype(BF)
    token = iota((SEQ, 1), 0)
    for h in range(2):
        source = (token // OWN) * 16 + h * OWN + token % OWN
        take_lines[h, :, :] = (iota((SEQ, NT * 16), 1) == source).astype(F32).astype(BF)
    regroup[...] = (iota((ROWS, ROWS), 0) == regrouped_row(iota((1, ROWS), 1))).astype(F32).astype(BF)
    for k in range(WIDTH // 128):
        flat[k * SEQ : (k + 1) * SEQ, :] = tok[:, k * 128 : (k + 1) * 128]
    tok_rows[...] = dot(pack[...], flat[...]).astype(BF).reshape(NT, TILE, 128)

    for source, near, far, row, slot in ((6, 1, 2, 0, 0), (2, 7, 6, 32, 1)):
        block = wz.at[z_at[source]]
        n.wait(block, base_w + slot)
        send_w(block, block, base_w + 3 + slot, z=z_at[near])
        block = wz.at[z_at[source], pl.ds(row, 32)]
        send_w(block, block, base_w + 5 + slot, z=z_at[far])
    dense_onward()
    n.wait(tok_in.at[pl.ds(0, 3)], base_t)
    n.wait(wz.at[pl.ds(0, 2)], base_w + 2)
    for slot in range(2):
        n.wait(wz.at[0], base_w + 3 + slot)
        n.wait(wz.at[0, pl.ds(0, 32)], base_w + 5 + slot)
    part = dot(tok_in[...].reshape(NX * SEQ, 512), wz[...].reshape(512, 512))
    part_out[...] = part.astype(BF).reshape(NX, SEQ, 512)
    base_p = n.reserve(1)
    send_p = n.stage(part_in.at[pl.ds(0, 3)])
    for dx in X_ORDER:
        x = (n.x + dx) % NX
        send_p(part_out.at[x], part_in.at[n.x], base_p, x=x)
    part_in[pl.ds(n.x, 1)] = part_out[pl.ds(n.x, 1)]
    n.wait(part_in.at[pl.ds(0, 3)], base_p)
    projected = part_in[0].astype(F32)
    for x in range(1, NX):
        projected = projected + part_in[x].astype(F32)
    projected = projected.astype(BF).astype(F32)
    query, forget_pre = projected[:, :HEAD], projected[:, HEAD : 2 * HEAD]
    values, out_gate = projected[:, 2 * HEAD : 3 * HEAD], projected[:, 3 * HEAD :]
    low = lower_bound[...]
    forget_sig = jax.nn.sigmoid(forget_pre)
    decay = low + (1.0 - low) * forget_sig
    keygate = (1.0 - low) * (1.0 - forget_sig)
    mixed_q = (query * decay).T
    gates[0, :, :], gates[1, :, :], gates[2, :, :] = decay, keygate, values
    load_state.wait()
    for b in range(SEQ):
        readout[b : b + 1, :] = jnp.sum(mixed_q[:, b : b + 1] * held[b, 0], axis=0, keepdims=True)
    read = readout[...] + jnp.sum(query * keygate, axis=1, keepdims=True) * values
    read = read * lax.rsqrt(jnp.mean(read * read, axis=-1, keepdims=True) + EPS)
    head_out = (read * head_gain[...] * jax.nn.silu(out_gate)).astype(BF)
    load_out.wait()
    whole = dot(head_out, out_w[...]).astype(BF)
    head_part[...] = whole
    head_rest = n.swap_tp(lambda t: cols_at(head_part, t, WIDE), lambda t: head_in.at[t], head_in.at[pl.ds(0, 7)])
    for k in range(WIDTH // 128):
        flat[k * SEQ : (k + 1) * SEQ, :] = whole[:, k * 128 : (k + 1) * 128]
    row_out[...] = dot(pack[...], flat[...]).astype(BF).reshape(NT, TILE, 128)
    row_rest = n.swap_tp(lambda t: row_out.at[t], lambda t: row_in.at[t], row_in.at[pl.ds(0, 7)])
    row_in[pl.ds(n.t, 1)] = row_out[pl.ds(n.t, 1)]
    head_in[pl.ds(n.t, 1)] = cols_at(head_part, n.t, WIDE)[...][None]
    last_onward()
    head_rest()
    own = cols_at(tok, n.t, WIDE)[...].astype(F32)
    for t in range(NT):
        own = own + head_in[t].astype(F32)
    own_cols = own.astype(BF)
    slot_out[...] = in_lines(dot(dispatch[...], own_cols))
    slots_rest = n.swap_ep(slot_out, slot_in)
    slot_in[pl.ds(n.e, 1)] = slot_out[pl.ds(n.e, 1)]
    resid[...] = own

    row_rest()
    own = tok_rows[pl.ds(n.t, 1)][0].astype(F32)
    for t in range(NT):
        own = own + row_in[t].astype(F32)
    rows[pl.ds(n.e, 1)] = own.astype(BF)[None]
    base_c = n.reserve(NZ)
    send_c = n.stage(rows.at[pl.ds(0, NE - 1)])
    mine = rows.at[n.e]
    for i, dz in enumerate(Z_ORDER):
        send_c(mine, mine, base_c + i, z=z_at[dz])
    for dx in X_ORDER:
        send_c(mine, mine, base_c + 7, x=(n.x + dx) % NX)
    cols_at(resid_rows, n.t, WIDE)[...] = own_cols
    rows_mine = cols_at(resid_rows, n.t, WIDE)
    rows_seven = resid_rows.at[:, pl.ds(0, 7 * WIDE)]
    rows_rest = n.swap_tp(lambda t: rows_mine, lambda t: cols_at(resid_rows, t, WIDE), rows_seven)
    load_down.wait()

    def swap_down(j):
        here = down_all.at[j]
        return n.swap_tp(lambda t: cols_at(down_own.at[j], t, WIDE), lambda t: here.at[t], here.at[pl.ds(0, 7)])

    down_rest = [swap_down(0)]
    dense_relay()
    last_relay()

    def pass_on(order):
        for i in order:
            e = z_at[(NZ - Z_ORDER[i]) % NZ] * NX + n.x
            n.wait(rows.at[e], base_c + i)
            for dx in X_ORDER:
                send_c(rows.at[e], rows.at[e], base_c + 7, x=(n.x + dx) % NX)

    pass_on(range(2))

    slots_rest()
    lines = slot_in[...].reshape(LINES, 128)
    both = dot(squeeze[...].reshape(2 * PAIR * SLOTS, LINES), lines)
    picked_rows = jnp.concatenate([both[: PAIR * SLOTS], both[PAIR * SLOTS :]], axis=1)
    cols_at(chosen, n.t, WIDE)[...] = picked_rows.astype(BF)
    chosen_onward, chosen_relay, chosen_rest = n.gather_tp(
        lambda t: cols_at(chosen, t, WIDE), chosen.at[:, pl.ds(0, 7 * WIDE)]
    )
    pass_on(range(2, 7))

    gain = ffn_gain[...]
    rows_rest()
    for copy in load_shared:
        copy.wait()
    shared_x = scaled(resid_rows[...], gain).astype(BF)
    shared_pre = dot(shared_x, shared_w[...])
    shared_hidden = (jax.nn.silu(shared_pre[:, :FF]) * shared_pre[:, FF:]).astype(BF)
    shared_part[...] = dot(shared_hidden, shared_d[...]).astype(BF)
    chosen_onward()
    down_rest.append(swap_down(1))

    chosen_relay()
    chosen_rest()
    for copy in load_expert:
        copy.wait()
    for j in range(PAIR):
        for i in range(4):
            part = pl.ds(j * SLOTS + i * SEQ, SEQ)
            chosen_in[part] = scaled(chosen[part], gain).astype(BF)
        pre = dot(chosen_in[pl.ds(j * SLOTS, SLOTS)], expert_w[:, 2 * j * FF : 2 * (j + 1) * FF])
        unit = (jax.nn.silu(pre[:, :FF]) * pre[:, FF:]).astype(BF)
        cols_at(hidden, n.t, FF).at[pl.ds(j * SLOTS, SLOTS)][...] = unit
    hidden_onward, hidden_relay, hidden_rest = n.gather_tp(
        lambda t: cols_at(hidden, t, FF), hidden.at[:, pl.ds(0, 7 * FF)]
    )

    n.wait(rows.at[pl.ds(0, 24)], base_c + 7)
    for g in range(NE // NT):
        group = dot(unpack[...], rows[g * NT : (g + 1) * NT].reshape(NT * TILE, 128))
        for k in range(WIDTH // 128):
            dense_raw[:, k * 128 : (k + 1) * 128] = group[k * SEQ : (k + 1) * SEQ, :]
        dense_in[g * SEQ : (g + 1) * SEQ, :] = scaled(dense_raw[...], gain).astype(BF)
    dense_rest()
    pre = dot(dense_in[...], dense_w[...].reshape(WIDTH, 2 * WIDE))
    units = (jax.nn.silu(pre[:, :WIDE]) * pre[:, WIDE:]).astype(BF)
    inner = dot(regroup[...], units).astype(BF)
    last_rest()
    def to_lines(block):
        for k in range(4):
            flat[k * SEQ : (k + 1) * SEQ, :] = block[:, k * 128 : (k + 1) * 128]
        return dot(quarter[...], flat[:ROWS]).astype(BF).reshape(NZ, 4 * OWN, 128)

    block = dot(inner, dense_d[:, 3 * 512 :]).astype(BF)
    for x in range(NX):
        zq_out[:, x] = to_lines(block[x * SEQ : (x + 1) * SEQ])
    base_zq = n.reserve(1)
    send_zq = n.stage(zq_in.at[pl.ds(0, 7)])
    for dz in FAR_ORDER[:-1]:
        send_zq(zq_out.at[z_at[dz]], zq_in.at[n.z], base_zq, z=z_at[dz])
    zq_in[pl.ds(n.z, 1)] = zq_out[pl.ds(n.z, 1)]
    base_x = n.reserve(3)
    for q in range(3):
        block = dot(inner, dense_d[:, q * 512 : (q + 1) * 512])
        sum_out[q, :, :, :] = block.astype(BF).reshape(NX, SEQ, 512)
        send_x = n.stage(sum_in.at[q, pl.ds(0, 3)])
        for dx in X_ORDER:
            x = (n.x + dx) % NX
            send_x(sum_out.at[q, x], sum_in.at[q, n.x], base_x + q, x=x)

    base_z = n.reserve(3)

    def sum_over_x(q):
        n.wait(sum_in.at[q, pl.ds(0, 3)], base_x + q)
        block = sum_out[q, pl.ds(n.x, 1)][0].astype(F32)
        for dx in X_ORDER:
            block = block + sum_in[q, pl.ds((n.x + dx) % NX, 1)][0].astype(F32)
        sum2_out[q, :, :, :] = to_lines(block.astype(BF))
        send_z = n.stage(sum2_in.at[q, pl.ds(0, 7)])
        for dz in FAR_ORDER[:-1]:
            send_z(sum2_out.at[q, z_at[dz]], sum2_in.at[q, n.z], base_z + q, z=z_at[dz])
        sum2_in[q, pl.ds(n.z, 1)] = sum2_out[q, pl.ds(n.z, 1)]

    hidden_onward()
    hidden_relay()
    sum_over_x(0)
    sum_over_x(1)
    n.wait(zq_in.at[pl.ds(0, 7)], base_zq)
    acc = zq_in[0].astype(F32)
    for z in range(1, NZ):
        acc = acc + zq_in[z].astype(F32)
    xq_out[...] = acc.astype(BF)
    base_xq = n.reserve(1)
    send_xq = n.stage(xq_in.at[pl.ds(0, 3)])
    for dx in X_ORDER:
        x = (n.x + dx) % NX
        send_xq(xq_out.at[x], xq_in.at[n.x], base_xq, x=x)
    xq_in[pl.ds(n.x, 1)] = xq_out[pl.ds(n.x, 1)]
    shared_rest = n.swap_tp(lambda t: cols_at(shared_part, t, WIDE), lambda t: shared_in.at[t], shared_in.at[pl.ds(0, 7)])
    shared_in[pl.ds(n.t, 1)] = cols_at(shared_part, n.t, WIDE)[...][None]
    for rest in down_rest:
        rest()
    load_mine.wait()
    hidden_rest()
    outs = [
        dot(hidden[pl.ds(j * SLOTS, SLOTS)], down_all[j].reshape(NT * FF, WIDE)).astype(BF) for j in range(PAIR)
    ]
    spread = dot(expand[:, :SLOTS], outs[0]) + dot(expand[:, SLOTS:], outs[1])
    back_out[...] = in_lines(spread)
    sum_over_x(2)
    back_rest = n.swap_ep(back_out, back_in)
    back_in[pl.ds(n.e, 1)] = back_out[pl.ds(n.e, 1)]

    decay, keygate = gates[0].T, gates[1].T
    for b in range(SEQ):
        held[b, 0] = decay[:, b : b + 1] * held[b, 0] + keygate[:, b : b + 1] * gates[2, b : b + 1, :]

    own_lines = []
    for q in range(3):
        n.wait(sum2_in.at[q, pl.ds(0, 7)], base_z + q)
        acc = sum2_in[q, 0].astype(F32)
        for z in range(1, NZ):
            acc = acc + sum2_in[q, z].astype(F32)
        own_lines.append(acc)
    n.wait(xq_in.at[pl.ds(0, 3)], base_xq)
    acc = xq_in[0].astype(F32)
    for x in range(1, NX):
        acc = acc + xq_in[x].astype(F32)
    own_lines.append(acc)
    own_lines = jnp.concatenate(own_lines, axis=0).astype(BF)
    swap_out[...] = dot(pad_lines[...], own_lines).astype(BF).reshape(NT, 16, 128)
    swap_rest = n.swap_tp(lambda t: swap_out.at[t], lambda t: swap_in.at[t], swap_in.at[pl.ds(0, 7)])
    swap_in[pl.ds(n.t, 1)] = swap_out[pl.ds(n.t, 1)]
    shared_rest()
    result = resid[...]
    for t in range(NT):
        result = result + shared_in[t].astype(F32)
    swap_rest()
    lines = swap_in[...].reshape(NT * 16, 128)
    dense_out = jnp.concatenate([dot(take_lines[h], lines) for h in range(2)], axis=1)
    result = result + dense_out * jax.nn.sigmoid(dense_mix[...])
    back_rest()
    lines = back_in[...].reshape(LINES, 128)
    both = dot(combine[...].reshape(6 * SEQ, LINES), lines)
    parts = [both[i * SEQ : (i + 1) * SEQ] for i in range(6)]
    routed = [parts[3 * h] + (parts[3 * h + 1] + parts[3 * h + 2]) for h in range(2)]
    result = result + jnp.concatenate(routed, axis=1)
    mixed[...] = result
    n.finish()


def closing(result, held, mixed, new_state, sem):
    copy = pltpu.make_async_copy(held, new_state, sem)
    copy.start()
    mixed[...] = result[...].astype(BF)
    copy.wait()


def local(*args):
    args = list(args)
    for i in (2, 7, 8, 10, 22):
        args[i] = args[i].reshape(1, -1)
    for i in (11, 12):
        args[i] = args[i].T
    vmem = pl.BlockSpec(memory_space=pltpu.VMEM)
    hbm = pl.BlockSpec(memory_space=pl.ANY)
    small = (2, 7, 8, 10, 11, 12, 22)
    scratch = [
        ((SEQ, WIDTH), BF),
        ((NZ, 64, 512), BF),
        ((NT, WIDE, 2 * WIDE), BF),
        ((PAIR, FF, WIDTH), BF),
        ((PAIR, NT, FF, WIDE), BF),
        ((3, SEQ, HEAD), F32),
        ((WIDTH, 2 * PAIR * FF), BF),
        ((WIDTH, 2 * FF), BF),
        ((FF, WIDTH), BF),
        ((HEAD, WIDTH), BF),
        ((WIDE, WIDTH), BF),
        ((NX, SEQ, 512), BF),
        ((NX, SEQ, 512), BF),
        ((NX, SEQ, 512), BF),
        ((NX, SEQ, 512), BF),
        ((SEQ, WIDTH), BF),
        ((NT, SEQ, WIDE), BF),
        ((NE, TILE, 128), BF),
        ((NT * TILE, 128), BF),
        ((NT, TILE, 128), BF),
        ((NT, TILE, 128), BF),
        ((NT, TILE, 128), BF),
        ((NT * TILE, NT * TILE), BF),
        ((NT * TILE, NT * TILE), BF),
        ((ROWS, ROWS), BF),
        ((SEQ, WIDTH), F32),
        ((SEQ, WIDTH), BF),
        ((NE, 2 * BOTH, 128), BF),
        ((NE, 2 * BOTH, 128), BF),
        ((PAIR * SLOTS, WIDTH), BF),
        ((PAIR * SLOTS, WIDTH), BF),
        ((ROWS, WIDTH), BF),
        ((PAIR * SLOTS, NT * FF), BF),
        ((SEQ, WIDTH), BF),
        ((NT, SEQ, WIDE), BF),
        ((3, NX, SEQ, 512), BF),
        ((3, NX, SEQ, 512), BF),
        ((3, NZ, 4 * OWN, 128), BF),
        ((3, NZ, 4 * OWN, 128), BF),
        ((NZ, NX, 4 * OWN, 128), BF),
        ((NZ, NX, 4 * OWN, 128), BF),
        ((NX, 4 * OWN, 128), BF),
        ((NX, 4 * OWN, 128), BF),
        ((ROWS, ROWS), BF),
        ((NT, 16, 128), BF),
        ((NT, 16, 128), BF),
        ((NT * 16, TILE), BF),
        ((2, SEQ, NT * 16), BF),
        ((NE, 2 * BOTH, 128), BF),
        ((NE, 2 * BOTH, 128), BF),
        ((SEQ, HEAD), F32),
        ((2, 3 * SEQ, LINES), BF),
        ((LINES, SEQ), BF),
        ((2, PAIR * SLOTS, LINES), BF),
        ((LINES, PAIR * SLOTS), BF),
        ((LINES, 128), F32),
        ((SEQ, WIDE), F32),
    ]
    result, held = pl.pallas_call(
        layer,
        out_shape=[
            pltpu.VMEM((SEQ, WIDE), F32),
            pltpu.VMEM((SEQ, 1, HEAD, HEAD), F32),
        ],
        in_specs=[vmem if i in small else hbm for i in range(len(args))],
        out_specs=[vmem, vmem],
        scratch_shapes=[pltpu.VMEM(shape, kind) for shape, kind in scratch]
        + [
            pltpu.SemaphoreType.DMA((SENDS,)),
            pltpu.SemaphoreType.DMA((ARRIVALS,)),
            pltpu.SemaphoreType.DMA((LOCALS,)),
        ],
        compiler_params=pltpu.CompilerParams(collective_id=0, has_side_effects=True),
        name="layer",
    )(*args)
    return pl.pallas_call(
        closing,
        out_shape=[
            jax.ShapeDtypeStruct((SEQ, WIDE), BF),
            jax.ShapeDtypeStruct((SEQ, 1, HEAD, HEAD), F32),
        ],
        in_specs=[vmem, hbm],
        out_specs=[vmem, hbm],
        scratch_shapes=[pltpu.SemaphoreType.DMA(())],
        name="closing",
    )(pltpu.with_memory_space_constraint(result, pltpu.VMEM), pltpu.with_memory_space_constraint(held, pltpu.VMEM))


def solution(mesh):
    torus = Mesh(mesh.devices.reshape(NZ, NX, NY, NC), ("z", "x", "y", "c"))
    return jax.shard_map(
        local,
        mesh=torus,
        in_specs=(
            P(EP, None),
            P(EP, TP, None, None),
            P(),
            P(EP, TP),
            P(EP, TP),
            P(EP, TP),
            P(EP, TP),
            P(TP),
            P(TP),
            P(TP, None),
            P(),
            P(EP, None),
            P(EP, None),
            P(EP, None, TP),
            P(EP, None, TP),
            P(EP, TP, None),
            P(None, TP),
            P(None, TP),
            P(TP, None),
            P(TP, EP),
            P(TP, EP),
            P(EP, TP),
            P(TP),
        ),
        out_specs=(P(EP, TP), P(EP, TP, None, None)),
        check_vma=False,
    )
```
